256 devices in a mesh: grp: 2 (over y), ep: 32 (over z, core), tp: 4 (over x).
Axes of the slice: x: 4, y: 2, z: 16, core: 2. Of those that a mesh axis runs over, the one named last changes fastest.
The devices are a block of a 4x16x16 slice.
Arguments:
- query_vectors: bfloat16 [32768, 2048], P(('grp', 'ep'), 'tp'), parts along dimension 0, may hold values from -6 to 6
- attend_lookup_vectors: bfloat16 [32768, 2048], P(('grp', 'ep'), 'tp'), parts along dimension 0, may hold values from -6 to 6
- attend_content_vectors: bfloat16 [32768, 2048], P(('grp', 'ep'), 'tp'), parts along dimension 0, may hold values from -6 to 6
- forget_speed_dependent: bfloat16 [32768, 2048], P(('grp', 'ep'), 'tp'), parts along dimension 0, may hold values from -3 to 3
- amend_speed_dependent: bfloat16 [32768, 2048], P(('grp', 'ep'), 'tp'), parts along dimension 0, may hold values from -6 to 6
- result_switch_preactivation: bfloat16 [32768, 2048], P(('grp', 'ep'), 'tp'), parts along dimension 0, may hold values from -6 to 6
- feature_forget_baseline: float32 [2048], P('tp'), may hold values from -13 to -3
- amend_speed_baseline: float32 [2048], P('tp'), may hold values from -9 to 3
- sudden_forget_extra: float32 [32768, 32], P(('grp', 'ep'), 'tp'), parts along dimension 0, may hold values from -1 to 0
- group_scaling_factor: float32 [2048], P('tp'), may hold values from 0.1 to 1.9
- result_mapping_matrix: bfloat16 [2048, 2048], P('tp'), may hold values from -0.125 to 0.125
- specialist_tokens_activations: bfloat16 [32768, 2048], P(('grp', 'ep', 'tp')), parts along dimension 0, may hold values from -6 to 6
- specialist_scaling_factor: float32 [2048], replicated, may hold values from 0.1 to 1.9
- selected_specialists: int32 [32768, 2], P(('grp', 'ep', 'tp')), parts along dimension 0, may hold values from 0 to 31, all different within a row; in each aligned block of 128 rows (0 to 127, 128 to 255, ...) at most 12 rows name the same one
- selection_mixing_factors: float32 [32768, 2], P(('grp', 'ep', 'tp')), parts along dimension 0, may hold values from 0.3 to 1.5
- dispatched_switch_matrix: bfloat16 [32, 2048, 1024], P('ep', None, 'tp'), may hold values from -0.125 to 0.125
- dispatched_raising_matrix: bfloat16 [32, 2048, 1024], P('ep', None, 'tp'), may hold values from -0.125 to 0.125
- dispatched_lowering_matrix: bfloat16 [32, 1024, 2048], P('ep', 'tp'), may hold values from -0.1875 to 0.1875
- common_switch_matrix: bfloat16 [2048, 512], P(None, 'tp'), may hold values from -0.125 to 0.125
- common_raising_matrix: bfloat16 [2048, 512], P(None, 'tp'), may hold values from -0.125 to 0.125
- common_lowering_matrix: bfloat16 [512, 2048], P('tp'), may hold values from -0.25 to 0.25
Outputs:
- attend_result_matrix: bfloat16 [32768, 2048], P(('grp', 'ep', 'tp')), parts along dimension 0
- moe_out: bfloat16 [32768, 2048], P(('grp', 'ep', 'tp')), parts along dimension 0
The draws below stay inside these ranges and needn't reach their ends.
There are 2 independent parts, one for each index of `grp`. The reference program is written for one: setup_inputs(seed, part) draws one part's arguments, and reference() takes and returns one part's arrays. A program takes and returns all parts, laid end to end along the dimension named above; an argument that names none is the same for every part. Nothing has to cross between parts.
Inputs may be any that keep to these rules, and one draw needn't show every extreme that they name: `selected_specialists`: each row names 2 different experts. Among the rows of one device no expert is named more than 12 times, and in every draw some device names some expert exactly 12 times.
All inputs are finite; a program needn't handle non-finite values.
Results may differ from the reference program's by a relative error of at most 0.023.
Values may be sent and summed in bfloat16 or wider, within the bound.
A program may use at most 128 MiB of HBM per device.

```python
import math
import jax
import jax.numpy as jnp
import numpy as np
from jax import lax

D = 2048
ATTEND_GROUPS = 32
ATTEND_SIZE = 64
FF = 1024
SFF = 512
TOP = 2
TOK_A = 512
TOK_B = 128
TOKENS_A = 16384
TOKENS_B = 16384
EXPERTS = 32
CAP = 12
N_TP = 4


def slow_heads(key):
    chance = 0.5
    return jax.random.uniform(jax.random.fold_in(key, 101), (ATTEND_GROUPS,), jnp.float32) < chance


def draw_feature_forget_baseline(key, part):
    slow_mask = slow_heads(key)
    spread = jax.random.uniform(jax.random.fold_in(key, 202), (ATTEND_GROUPS, ATTEND_SIZE), jnp.float32)
    slow_log = jnp.log(0.05 / TOKENS_A) + spread * jnp.log(8.0)
    fast_log = jnp.log(0.01) + spread * jnp.log(100.0 / 30.0)
    return jnp.where(slow_mask[:, None], slow_log, fast_log).reshape(ATTEND_GROUPS * ATTEND_SIZE).astype(jnp.float32)


def draw_amend_speed_baseline(key, part):
    slow_mask = slow_heads(key)
    noise = jnp.clip(jax.random.normal(jax.random.fold_in(key, 303), (ATTEND_GROUPS, ATTEND_SIZE), jnp.float32), -3.0, 3.0)
    return jnp.where(slow_mask[:, None], -7.0 + 0.5 * noise, noise).reshape(ATTEND_GROUPS * ATTEND_SIZE).astype(jnp.float32)


def draw_forget_speed_dependent(key, part):
    block_count = TOKENS_A // TOK_A
    offsets = jax.random.uniform(jax.random.fold_in(key, 1), (block_count,), jnp.float32, -0.7, 0.7)
    noise = jnp.clip(0.6 * jax.random.normal(jax.random.fold_in(key, 2), (TOKENS_A, ATTEND_GROUPS * ATTEND_SIZE), jnp.float32), -2.0, 2.0)
    return (noise + jnp.repeat(offsets, TOK_A)[:, None]).astype(jnp.bfloat16)


def draw_sudden_forget_extra(key, part):
    where_at = jax.random.randint(jax.random.fold_in(key, 1), (2, 1, ATTEND_GROUPS), 0, TOKENS_A)
    losses = jax.random.uniform(jax.random.fold_in(key, 2), (2, 1, ATTEND_GROUPS), jnp.float32, jnp.log(0.6), jnp.log(0.8))
    row_ids = jnp.arange(TOKENS_A, dtype=jnp.int32)[None, :, None]
    return jnp.sum(jnp.where(row_ids == where_at, losses, 0.0), axis=0).astype(jnp.float32)


def block_levels(own_key, dims, pieces, low, high):
    level = 1.0
    for axis_at, parts in pieces:
        steps = jax.random.uniform(jax.random.fold_in(jax.random.fold_in(own_key, 6), axis_at), (parts,), jnp.float32, low / len(pieces), high / len(pieces))
        level = level * jnp.repeat(jnp.exp(steps), dims[axis_at] // parts).reshape((-1,) + (1,) * (len(dims) - 1 - axis_at))
    return level


def routed_block(rng, own, number, rows, count, top, reach, lean):
    ranking = jax.random.permutation(rng, count)
    heavy_load, common = load_shares(count, rows * top, reach, lean, True), load_shares(count, rows * top, reach, lean, False)
    places = jnp.arange(count)

    def named(sizes, offset_by):
        used = int((sizes > 0).sum())
        fixed = max(1, used // 4)
        shifted = fixed + (places - fixed + offset_by * (used - fixed)) % max(1, count - fixed)
        return jnp.zeros((count,), jnp.int32).at[ranking[jnp.where(places < fixed, places, shifted)]].set(jnp.asarray(sizes, jnp.int32))

    sizes = jnp.where(number % 4 == 0, named(heavy_load, number // 4), named(common, number - number // 4 - 1))
    mixed = jax.random.permutation(jax.random.fold_in(own, 3), count)
    source_of, receiver = mixed[0:count // 2 * 2:2], mixed[1:count // 2 * 2:2]
    room = jnp.minimum(sizes[source_of] - 1, reach - sizes[receiver]) // 2
    room = jnp.where((source_of == ranking[0]) | (receiver == ranking[0]) | (sizes[receiver] == 0), 0, jnp.maximum(room, 0))
    shifted = jax.random.randint(jax.random.fold_in(own, 4), (count // 2,), 0, 1 << 20) % (room + 1)
    sizes = sizes.at[source_of].add(-shifted).at[receiver].add(shifted)
    items = jnp.searchsorted(jnp.cumsum(sizes), jnp.arange(rows * top), side="right").astype(jnp.int32)
    table = items.reshape(top, rows).T
    table = table[jax.random.permutation(jax.random.fold_in(own, 1), rows)]
    offset_by = jax.random.randint(jax.random.fold_in(own, 2), (rows, 1), 0, top)
    return jnp.take_along_axis(table, (jnp.arange(top)[None, :] + offset_by) % top, axis=1)


def load_shares(number_of, total, bound, skew, full):
    loads = [(1 << 20) // math.isqrt(standing ** skew) + 1 for standing in range(1, number_of + 1)]
    largest = bound if full else min(bound, max(-(-total // number_of), total * loads[0] // sum(loads)))
    least = 1 if total - largest >= number_of - 1 else 0
    given, rest = [largest] + [least] * (number_of - 1), total - largest - least * (number_of - 1)
    while rest > 0:
        candidates = [i for i in range(1, number_of) if given[i] < largest] or [i for i in range(1, number_of) if given[i] < bound]
        mass, left = sum([loads[i] for i in candidates]), rest
        for i in candidates:
            extra = min(bound - given[i], max(1, left * loads[i] // mass), rest)
            given[i] = given[i] + extra
            rest = rest - extra
    return np.array(given)


def centred(rng, dims, width, reach, shards=(), kind=jnp.bfloat16):
    level = block_levels(rng, dims, shards, -0.22, 0.18) if shards else 1.0
    result = jax.random.normal(rng, dims, jnp.float32) * width * level
    return jnp.minimum(jnp.maximum(result, -reach), reach).astype(kind)


def setup_inputs(seed: int = 0, part: int = 0) -> dict:
    arg_keys = jax.random.split(jax.random.key(seed), 22)
    part_splits = jax.random.split(jax.random.fold_in(arg_keys[21], part), 22)
    query_vectors = centred(part_splits[0], (TOKENS_A, ATTEND_GROUPS * ATTEND_SIZE), 1.0, 6.0, ((0, 32), (1, 4)))
    attend_lookup_vectors = centred(part_splits[1], (TOKENS_A, ATTEND_GROUPS * ATTEND_SIZE), 1.0, 6.0, ((0, 32), (1, 4)))
    attend_content_vectors = centred(part_splits[2], (TOKENS_A, ATTEND_GROUPS * ATTEND_SIZE), 1.0, 6.0, ((0, 32), (1, 4)))
    forget_speed_dependent = draw_forget_speed_dependent(jax.random.fold_in(jax.random.fold_in(arg_keys[21], part), 71), part)
    amend_speed_dependent = centred(part_splits[4], (TOKENS_A, ATTEND_GROUPS * ATTEND_SIZE), 1.0, 6.0, ((0, 32), (1, 4)))
    result_switch_preactivation = centred(part_splits[5], (TOKENS_A, ATTEND_GROUPS * ATTEND_SIZE), 1.0, 6.0, ((0, 32), (1, 4)))
    feature_forget_baseline = draw_feature_forget_baseline(jax.random.fold_in(arg_keys[21], 71), part)
    amend_speed_baseline = draw_amend_speed_baseline(jax.random.fold_in(arg_keys[21], 71), part)
    sudden_forget_extra = draw_sudden_forget_extra(jax.random.fold_in(jax.random.fold_in(arg_keys[21], part), 71), part)
    group_scaling_factor = jnp.clip(1.0 + 0.18 * jax.random.normal(arg_keys[9], (ATTEND_GROUPS * ATTEND_SIZE,), jnp.float32), 0.1, 1.9)
    result_mapping_matrix = centred(arg_keys[10], (ATTEND_GROUPS * ATTEND_SIZE, D), (ATTEND_GROUPS * ATTEND_SIZE) ** -0.5, 0.125, ((0, 4),))
    specialist_tokens_activations = centred(part_splits[11], (TOKENS_B, D), 1.0, 6.0, ((0, 128),))
    specialist_scaling_factor = jnp.clip(1.0 + 0.18 * jax.random.normal(arg_keys[12], (D,), jnp.float32), 0.1, 1.9)
    selected_specialists_keys = jax.random.split(jax.random.fold_in(part_splits[13], 1), TOKENS_B // TOK_B)
    selected_specialists_turns = jax.random.permutation(jax.random.fold_in(part_splits[13], 3), TOKENS_B // TOK_B)
    selected_specialists = jax.vmap(lambda own, number: routed_block(jax.random.fold_in(part_splits[13], 2), own, number, TOK_B, EXPERTS, TOP, CAP, 2))(selected_specialists_keys, selected_specialists_turns).reshape((TOKENS_B, TOP))
    selection_mixing_factors = jnp.clip(jnp.exp(math.log(1.5) - 1.60943787 * jax.random.uniform(part_splits[14], (TOKENS_B, TOP), jnp.float32) ** block_levels(part_splits[14], (TOKENS_B, TOP), ((0, 128),), -0.2, 0.2)), 0.3, 1.5)
    dispatched_switch_matrix = centred(arg_keys[15], (EXPERTS, D, FF), D ** -0.5, 0.125, ((0, 32), (2, 4)))
    dispatched_raising_matrix = centred(arg_keys[16], (EXPERTS, D, FF), D ** -0.5, 0.125, ((0, 32), (2, 4)))
    dispatched_lowering_matrix = centred(arg_keys[17], (EXPERTS, FF, D), FF ** -0.5, 0.1875, ((0, 32), (1, 4)))
    common_switch_matrix = centred(arg_keys[18], (D, SFF), D ** -0.5, 0.125, ((1, 4),))
    common_raising_matrix = centred(arg_keys[19], (D, SFF), D ** -0.5, 0.125, ((1, 4),))
    common_lowering_matrix = centred(arg_keys[20], (SFF, D), SFF ** -0.5, 0.25, ((0, 4),))
    return dict(query_vectors=query_vectors, attend_lookup_vectors=attend_lookup_vectors, attend_content_vectors=attend_content_vectors, forget_speed_dependent=forget_speed_dependent, amend_speed_dependent=amend_speed_dependent, result_switch_preactivation=result_switch_preactivation, feature_forget_baseline=feature_forget_baseline, amend_speed_baseline=amend_speed_baseline, sudden_forget_extra=sudden_forget_extra, group_scaling_factor=group_scaling_factor, result_mapping_matrix=result_mapping_matrix, specialist_tokens_activations=specialist_tokens_activations, specialist_scaling_factor=specialist_scaling_factor, selected_specialists=selected_specialists, selection_mixing_factors=selection_mixing_factors, dispatched_switch_matrix=dispatched_switch_matrix, dispatched_raising_matrix=dispatched_raising_matrix, dispatched_lowering_matrix=dispatched_lowering_matrix, common_switch_matrix=common_switch_matrix, common_raising_matrix=common_raising_matrix, common_lowering_matrix=common_lowering_matrix)


highest = lax.Precision.HIGHEST

def split_sum(hidden, weight, blocks):
    width_dev = hidden.shape[1] // blocks
    summed = jnp.zeros((hidden.shape[0], weight.shape[1]), jnp.float32)
    for block_id in range(blocks):
        lower = block_id * width_dev
        partial_value = jnp.dot(hidden[:, lower:lower + width_dev], weight[lower:lower + width_dev], preferred_element_type=jnp.float32)
        summed = summed + lax.optimization_barrier(partial_value.astype(jnp.bfloat16)).astype(jnp.float32)
    return summed

def swiglu_rows(rows, gate_w, up_w):
    gate_vals = jnp.dot(rows, gate_w, preferred_element_type=jnp.float32)
    up_vals = jnp.dot(rows, up_w, preferred_element_type=jnp.float32)
    return (jax.nn.silu(gate_vals) * up_vals).astype(jnp.bfloat16)

def simple_attend_verify(query_vectors, attend_lookup_vectors, attend_content_vectors, forget_speed_dependent, amend_speed_dependent, result_switch_preactivation, feature_forget_baseline, amend_speed_baseline, sudden_forget_extra, group_scaling_factor, result_mapping_matrix):
    tokens = query_vectors.shape[0]

    def split_among_groups(array_in):
        return array_in.astype(jnp.float32).reshape(tokens, ATTEND_GROUPS, ATTEND_SIZE)
    forget_exponent_log = -jnp.exp(feature_forget_baseline.reshape(ATTEND_GROUPS, ATTEND_SIZE) + split_among_groups(forget_speed_dependent)) + sudden_forget_extra[:, :, None]
    learn_rate = jax.nn.sigmoid(amend_speed_baseline.reshape(ATTEND_GROUPS, ATTEND_SIZE) + split_among_groups(amend_speed_dependent))
    key_heads = split_among_groups(attend_lookup_vectors)
    unit_key = key_heads * lax.rsqrt(lax.optimization_barrier(jnp.sum(key_heads * key_heads, -1, keepdims=True)) + 1e-06)

    def advance(memory, inputs):
        recept_now, decay_now, write_now, value_now, unit_now, erase_now = inputs
        removed = jnp.einsum('hvk,hk->hv', memory, -unit_now, precision=highest)
        memory = memory * decay_now[:, None, :] + removed[:, :, None] * erase_now[:, None, :] + value_now[:, :, None] * write_now[:, None, :]
        return (memory, jnp.einsum('hvk,hk->hv', memory, recept_now, precision=highest))
    memory_zero = jnp.zeros((ATTEND_GROUPS, ATTEND_SIZE, ATTEND_SIZE), jnp.float32)
    memory_end, recur = lax.scan(advance, memory_zero, (split_among_groups(query_vectors), jnp.exp(forget_exponent_log), key_heads * learn_rate, split_among_groups(attend_content_vectors), unit_key, unit_key * learn_rate))
    head_mean = lax.optimization_barrier(jnp.mean(recur, -1, keepdims=True))
    centered = recur - head_mean
    head_var = lax.optimization_barrier(jnp.mean(centered * centered, -1, keepdims=True))
    normed = centered * lax.rsqrt(head_var + 0.00064) * group_scaling_factor.reshape(ATTEND_GROUPS, ATTEND_SIZE)
    mixed_rows = (normed * jax.nn.sigmoid(split_among_groups(result_switch_preactivation))).reshape(tokens, ATTEND_GROUPS * ATTEND_SIZE)
    mixed_rows = mixed_rows.astype(jnp.bfloat16)
    return split_sum(mixed_rows, result_mapping_matrix, N_TP).astype(jnp.bfloat16)

def moe_reference(specialist_tokens_activations, specialist_scaling_factor, selected_specialists, selection_mixing_factors, dispatched_switch_matrix, dispatched_raising_matrix, dispatched_lowering_matrix, common_switch_matrix, common_raising_matrix, common_lowering_matrix):
    floats = specialist_tokens_activations.astype(jnp.float32)
    normed = floats * lax.rsqrt(lax.optimization_barrier(jnp.mean(floats * floats, -1, keepdims=True)) + 1e-06) * specialist_scaling_factor
    normed = normed.astype(jnp.bfloat16)
    top_count = selected_specialists.shape[1]
    block_count = TOKENS_B // TOK_B
    flat_block = selected_specialists.reshape(block_count, TOK_B * top_count)
    one_hot = (flat_block[:, :, None] == jnp.arange(EXPERTS, dtype=jnp.int32)[None, None, :]).astype(jnp.int32)
    slot_rank = lax.optimization_barrier(jnp.sum((jnp.cumsum(one_hot, axis=1) - 1) * one_hot, axis=-1))
    position = (jnp.arange(block_count, dtype=jnp.int32)[:, None] * CAP + slot_rank).reshape(-1)
    flat_ids = flat_block.reshape(-1)
    weights_flat = selection_mixing_factors.reshape(-1)
    repeated = jnp.repeat(normed, top_count, axis=0)
    buffer_rows = block_count * CAP

    def per_expert(summed, operands):
        gate_w, up_w, down_w, expert_id = operands
        chosen = flat_ids == expert_id
        target = jnp.where(chosen, position, buffer_rows)
        buffer = jnp.zeros((buffer_rows, D), jnp.bfloat16).at[target].set(repeated, mode='drop')
        hidden = swiglu_rows(buffer, gate_w, up_w)
        expert_out = split_sum(hidden, down_w, N_TP).astype(jnp.bfloat16)
        picked = jnp.take(expert_out, jnp.minimum(position, buffer_rows - 1), axis=0).astype(jnp.float32)
        contrib = jnp.where(chosen[:, None], picked * weights_flat[:, None], 0.0)
        return (summed + lax.optimization_barrier(jnp.sum(contrib.reshape(TOKENS_B, top_count, D), axis=1)), None)
    routed, _ = lax.scan(per_expert, jnp.zeros((TOKENS_B, D), jnp.float32), (dispatched_switch_matrix, dispatched_raising_matrix, dispatched_lowering_matrix, jnp.arange(EXPERTS, dtype=jnp.int32)))
    shared_hidden = swiglu_rows(normed, common_switch_matrix, common_raising_matrix)
    shared_sum = split_sum(shared_hidden, common_lowering_matrix, N_TP)
    return (routed + shared_sum).astype(jnp.bfloat16)

def reference(query_vectors, attend_lookup_vectors, attend_content_vectors, forget_speed_dependent, amend_speed_dependent, result_switch_preactivation, feature_forget_baseline, amend_speed_baseline, sudden_forget_extra, group_scaling_factor, result_mapping_matrix, specialist_tokens_activations, specialist_scaling_factor, selected_specialists, selection_mixing_factors, dispatched_switch_matrix, dispatched_raising_matrix, dispatched_lowering_matrix, common_switch_matrix, common_raising_matrix, common_lowering_matrix):
    attend_result_matrix = simple_attend_verify(query_vectors, attend_lookup_vectors, attend_content_vectors, forget_speed_dependent, amend_speed_dependent, result_switch_preactivation, feature_forget_baseline, amend_speed_baseline, sudden_forget_extra, group_scaling_factor, result_mapping_matrix)
    moe_out = moe_reference(specialist_tokens_activations, specialist_scaling_factor, selected_specialists, selection_mixing_factors, dispatched_switch_matrix, dispatched_raising_matrix, dispatched_lowering_matrix, common_switch_matrix, common_raising_matrix, common_lowering_matrix)
    return (attend_result_matrix, moe_out)
```

```python
import functools

import jax
import jax.numpy as jnp
from jax import lax
from jax.experimental import pallas as pl
from jax.experimental.pallas import tpu as pltpu
from jax.sharding import PartitionSpec as P

F32 = jnp.float32
BF16 = jnp.bfloat16
SPAN = 64
MESH = pl.DeviceIdType.MESH


def dot(a, b):
    return jnp.dot(a, b, preferred_element_type=F32)


def dot_nt(a, b):
    return lax.dot_general(a, b, (((1,), (1,)), ((), ())), preferred_element_type=F32)


def dot_tn(a, b):
    return lax.dot_general(a, b, (((0,), (0,)), ((), ())), preferred_element_type=F32)


def split(x, parts):
    out = []
    for _ in range(parts - 1):
        out.append(x.astype(BF16))
        x = x - out[-1].astype(F32)
    out.append(x.astype(BF16))
    return out


def iota(shape, dim):
    return lax.broadcasted_iota(jnp.int32, shape, dim)


def local_mixer(
    q_ref, k_ref, v_ref, f_ref, a_ref, fb_ref, ab_ref, x_ref, omap_ref, oloc_ref, pay_ref
):
    rows, lanes = q_ref.shape
    half = lanes // 2
    spans = rows // SPAN
    groups = x_ref.shape[1]
    pair = pl.program_id(0)
    low = iota((SPAN, lanes), 1) < half
    col = jnp.where(low, iota((SPAN, lanes), 1), iota((SPAN, lanes), 1) - half)
    row = iota((SPAN, lanes), 0)
    strict = row > col
    inclusive = row >= col
    tri = (iota((SPAN, SPAN), 0) >= iota((SPAN, SPAN), 1)).astype(BF16)
    tri3 = jnp.concatenate([tri] * 3, axis=1)
    same = ((iota((lanes, lanes), 0) < half) == (iota((lanes, lanes), 1) < half)).astype(BF16)
    same2 = jnp.concatenate([same] * 2, axis=0)
    spread = (
        iota((groups, lanes), 0) == 2 * pair + (iota((groups, lanes), 1) >= half).astype(jnp.int32)
    ).astype(BF16)
    spread3 = jnp.concatenate([spread] * 3, axis=0)
    below = iota((lanes, lanes), 0) < half
    left = iota((lanes, lanes), 1) < half

    def stack(x):
        return jnp.concatenate([jnp.where(low, x, 0.0), jnp.where(low, 0.0, x)], axis=0).astype(
            BF16
        )

    fb = fb_ref[...]
    ab = ab_ref[...]
    extra = dot(jnp.concatenate(split(x_ref[...], 3), axis=1), spread3)

    spans_in = []
    for c in range(spans):
        at = slice(c * SPAN, (c + 1) * SPAN)
        decay = -jnp.exp(fb + f_ref[at, :].astype(F32)) + extra[at, :]
        rate = jax.nn.sigmoid(ab + a_ref[at, :].astype(F32))
        key = k_ref[at, :].astype(F32)
        sq = dot(jnp.concatenate(split(key * key, 2), axis=1), same2)
        unit = key * lax.rsqrt(sq + 1e-06)
        cum = dot(tri3, jnp.concatenate(split(decay, 3), axis=0))
        mid = cum[SPAN // 2 : SPAN // 2 + 1, :]
        last = cum[SPAN - 1 : SPAN, :]
        left_erase = -unit * jnp.exp(cum - decay - mid)
        left_read = q_ref[at, :].astype(F32) * jnp.exp(cum - mid)
        right = jnp.exp(mid - cum) * rate
        right_erase = unit * right
        right_write = key * right
        grow = jnp.exp(mid)
        tail = jnp.exp(last - mid)
        lefts = jnp.concatenate([left_erase, left_read], axis=0).astype(BF16)
        rights = jnp.concatenate([stack(right_erase), stack(right_write)], axis=0)
        pairs = dot_nt(lefts, rights)
        a_mat = jnp.where(strict, pairs[:SPAN, :lanes], 0.0)
        erase_write = jnp.where(strict, pairs[:SPAN, lanes:], 0.0)
        read_erase = jnp.where(inclusive, pairs[SPAN:, :lanes], 0.0)
        read_write = jnp.where(inclusive, pairs[SPAN:, lanes:], 0.0)
        value = v_ref[at, :].astype(F32)
        writes = dot(
            jnp.concatenate([erase_write, read_write], axis=0).astype(BF16), stack(value)
        )
        ends = jnp.concatenate([right_erase * tail, right_write * tail], axis=0).astype(BF16)
        spans_in.append(
            dict(
                a=a_mat,
                first=stack(left_erase * grow),
                read=left_read * grow,
                re=read_erase.astype(BF16),
                ew=stack(writes[:SPAN]),
                rw=writes[SPAN:],
                ends=ends,
                value=v_ref[at, :],
                last=jnp.exp(last),
            )
        )

    eye = (row == col).astype(F32)
    block = 1
    inverse = None
    while block < SPAN:
        in_block = (row // (2 * block) == col // (2 * block)) & (
            (row // block) % 2 == 1
        ) & ((col // block) % 2 == 0)
        steps = [jnp.where(in_block, s["a"], 0.0) for s in spans_in]
        if inverse is None:
            inverse = [eye + step for step in steps]
        else:
            inner = [
                dot(step.astype(BF16), stack(x)) for step, x in zip(steps, inverse)
            ]
            inverse = [x + dot(x.astype(BF16), stack(y)) for x, y in zip(inverse, inner)]
        block *= 2

    state = jnp.concatenate([eye, jnp.zeros_like(eye)], axis=0)
    for c, s in enumerate(spans_in):
        at = slice(c * SPAN, (c + 1) * SPAN)
        solved = dot(inverse[c].astype(BF16), jnp.concatenate([s["first"], s["ew"]], axis=1))
        w, y = (solved[:, :lanes], solved[:, lanes:])
        seen = dot(s["re"], jnp.concatenate([stack(w), stack(y)], axis=1))
        read = s["read"] + seen[:, :lanes]
        added = s["rw"] + seen[:, lanes:]
        value = s["value"]
        erased = dot_tn(w.astype(BF16), s["ends"][:SPAN])
        erased = jnp.where(below == left, erased, 0.0).astype(BF16)
        offset = dot_tn(jnp.concatenate([y.astype(BF16), value], axis=0), s["ends"])
        offset = jnp.where(low, offset[:half], offset[half:])
        both = jnp.concatenate([stack(state[:SPAN]), stack(state[SPAN:])], axis=0)
        reads = dot_nt(read.astype(BF16), both)
        omap_ref[at, :] = reads[:, :lanes].astype(BF16)
        oloc_ref[at, :] = added + reads[:, lanes:]
        state = (
            state * s["last"]
            + dot(state.astype(BF16), erased)
            + jnp.concatenate([jnp.zeros_like(offset), offset], axis=0)
        )
    jump, offset = (state[:SPAN], state[SPAN:])
    quarter = SPAN // 4
    eighth = SPAN // 8
    half_low = low[: SPAN // 2]
    jump_turned = pltpu.roll(jump, half, 1)
    offset_turned = pltpu.roll(offset, half, 1)
    empty = jnp.zeros((eighth, lanes), F32)
    for h in range(2):
        top = (jump, jump_turned)[h][: SPAN // 2]
        bottom = (jump_turned, jump)[h][SPAN // 2 :]
        packed = jnp.where(half_low, top, bottom)
        for j in range(4):
            top = (offset, offset_turned)[h][j * quarter : j * quarter + eighth]
            bottom = (offset_turned, offset)[h][j * quarter + eighth : (j + 1) * quarter]
            piece = jnp.where(low[:eighth], top, bottom)
            pay_ref[4 * h + j] = jnp.concatenate([packed, piece, empty], axis=0).astype(BF16)


def run_local_mixer(q, k, v, f, a, fb, ab, extra):
    rows, width = q.shape
    groups = extra.shape[1]
    lanes = 2 * (width // groups)
    tall = pl.BlockSpec((rows, lanes), lambda i: (0, i))
    flat = pl.BlockSpec((1, lanes), lambda i: (0, i))
    return pl.pallas_call(
        local_mixer,
        grid=(width // lanes,),
        in_specs=[tall] * 5 + [flat] * 2 + [pl.BlockSpec((rows, groups), lambda i: (0, 0))],
        out_specs=(tall, tall, pl.BlockSpec((8, 48, lanes), lambda i: (i, 0, 0))),
        out_shape=(
            jax.ShapeDtypeStruct((rows, width), BF16),
            jax.ShapeDtypeStruct((rows, width), F32),
            jax.ShapeDtypeStruct((4 * groups, 48, lanes), BF16),
        ),
        compiler_params=pltpu.CompilerParams(vmem_limit_bytes=48 * 1024 * 1024),
        cost_estimate=pl.CostEstimate(
            flops=10_000_000_000, bytes_accessed=6_000_000, transcendentals=1_500_000
        ),
        name="local_mixer",
    )(q, k, v, f, a, fb.reshape(1, -1), ab.reshape(1, -1), extra)


def fold_states(pay_ref, out_ref, arrived, sent, send_sem, recv_sem, back_sem, home_sem, own_sem):
    count = pay_ref.shape[0]
    lanes = pay_ref.shape[2]
    half = lanes // 2
    me = lax.axis_index("ep")
    barrier = pltpu.get_barrier_semaphore()

    def greet(d, carry):
        pl.semaphore_signal(
            barrier, inc=1, device_id={"ep": lax.rem(me + d, count)}, device_id_type=MESH
        )
        return carry

    lax.fori_loop(1, count, greet, 0)
    pl.semaphore_wait(barrier, count - 1)

    def outward(d):
        to = lax.rem(me + d, count)
        return pltpu.make_async_remote_copy(
            src_ref=pay_ref.at[to],
            dst_ref=arrived.at[me],
            send_sem=send_sem.at[d],
            recv_sem=recv_sem.at[me],
            device_id={"ep": to},
            device_id_type=MESH,
        )

    def inward(e):
        return pltpu.make_async_remote_copy(
            src_ref=pay_ref.at[e],
            dst_ref=arrived.at[e],
            send_sem=send_sem.at[0],
            recv_sem=recv_sem.at[e],
            device_id={"ep": e},
            device_id_type=MESH,
        )

    def go(d, carry):
        outward(d).start()
        return carry

    lax.fori_loop(1, count, go, 0)
    own = pltpu.make_async_copy(pay_ref.at[me], arrived.at[me], own_sem.at[0])
    own.start()
    own.wait()

    def homeward(e):
        return pltpu.make_async_remote_copy(
            src_ref=sent.at[e],
            dst_ref=out_ref.at[me],
            send_sem=back_sem.at[e],
            recv_sem=home_sem.at[me],
            device_id={"ep": e},
            device_id_type=MESH,
        )

    low = iota((lanes // 4, lanes), 1) < half

    def step(e, state):
        sent[e] = state

        @pl.when(e != me)
        def _():
            inward(e).wait_recv()

        @pl.when((e > 0) & (e - 1 != me))
        def _():
            homeward(e - 1).start()

        block = arrived[e].astype(F32)
        jump, offset = (block[: lanes // 4], block[lanes // 4 : lanes // 4 + 8])
        turned = pltpu.roll(jump, half, 1)
        spread = jnp.concatenate(
            [
                jnp.where(low, jump, 0.0),
                jnp.where(low, turned, 0.0),
                jnp.where(low, 0.0, turned),
                jnp.where(low, 0.0, jump),
            ],
            axis=0,
        ).astype(BF16)
        moved = dot(jnp.concatenate(split(state, 2), axis=0), spread)
        return moved[:8] + moved[8:] + offset

    lax.fori_loop(0, count, step, jnp.zeros((8, lanes), F32))

    @pl.when(me != count - 1)
    def _():
        homeward(count - 1).start()

    own = pltpu.make_async_copy(sent.at[me], out_ref.at[me], own_sem.at[1])
    own.start()
    own.wait()

    def finish(d, carry):
        outward(d).wait_send()
        return carry

    lax.fori_loop(1, count, finish, 0)

    def drain(d, carry):
        e = lax.rem(me + d, count)
        homeward(e).wait_send()
        pltpu.make_async_remote_copy(
            src_ref=sent.at[e],
            dst_ref=out_ref.at[e],
            send_sem=back_sem.at[e],
            recv_sem=home_sem.at[e],
            device_id={"ep": e},
            device_id_type=MESH,
        ).wait_recv()
        return carry

    lax.fori_loop(1, count, drain, 0)


def run_fold_states(pay):
    count, _, lanes = pay.shape
    vmem = pl.BlockSpec(memory_space=pltpu.VMEM)
    return pl.pallas_call(
        fold_states,
        in_specs=[vmem],
        out_specs=vmem,
        out_shape=jax.ShapeDtypeStruct((count, 8, lanes), F32),
        scratch_shapes=[
            pltpu.VMEM(pay.shape, BF16),
            pltpu.VMEM((count, 8, lanes), F32),
            pltpu.SemaphoreType.DMA((count,)),
            pltpu.SemaphoreType.DMA((count,)),
            pltpu.SemaphoreType.DMA((count,)),
            pltpu.SemaphoreType.DMA((count,)),
            pltpu.SemaphoreType.DMA((2,)),
        ],
        compiler_params=pltpu.CompilerParams(
            collective_id=0, has_side_effects=True, vmem_limit_bytes=16 * 1024 * 1024
        ),
        cost_estimate=pl.CostEstimate(
            flops=20_000_000_000, bytes_accessed=3_000_000, transcendentals=0
        ),
        name="fold_states",
    )(pay)


def finish_mixer(omap_ref, oloc_ref, state_ref, gate_ref, gain_ref, out_ref):
    rows, lanes = omap_ref.shape
    half = lanes // 2
    low = iota((8, lanes), 1) < half
    zero = jnp.zeros((8, lanes), F32)
    tiles = []
    for h in range(2):
        for j in range(4):
            block = state_ref[4 * h + j]
            turned = pltpu.roll(block, half, 1)
            if h == 0:
                tiles += [jnp.where(low, block, zero), jnp.where(low, turned, zero)]
            else:
                tiles += [jnp.where(low, zero, turned), jnp.where(low, zero, block)]
    state = jnp.concatenate(tiles, axis=0).astype(BF16)
    same = jnp.where(
        (iota((lanes, lanes), 0) < half) == (iota((lanes, lanes), 1) < half), 1.0 / half, 0.0
    ).astype(BF16)
    same2 = jnp.concatenate([same] * 2, axis=0)
    head_out = oloc_ref[...] + dot_nt(omap_ref[...], state)
    mean = dot(jnp.concatenate(split(head_out, 2), axis=1), same2)
    centered = head_out - mean
    var = dot(jnp.concatenate(split(centered * centered, 2), axis=1), same2)
    normed = centered * lax.rsqrt(var + 0.00064) * gain_ref[...]
    out_ref[...] = (normed * jax.nn.sigmoid(gate_ref[...].astype(F32))).astype(BF16)


def run_finish_mixer(omap, oloc, states, gate, gain):
    rows, width = omap.shape
    lanes = states.shape[2]
    tall = pl.BlockSpec((rows, lanes), lambda i: (0, i))
    return pl.pallas_call(
        finish_mixer,
        grid=(width // lanes,),
        in_specs=[
            tall,
            tall,
            pl.BlockSpec((8, 8, lanes), lambda i: (i, 0, 0)),
            tall,
            pl.BlockSpec((1, lanes), lambda i: (0, i)),
        ],
        out_specs=tall,
        out_shape=jax.ShapeDtypeStruct((rows, width), BF16),
        compiler_params=pltpu.CompilerParams(vmem_limit_bytes=32 * 1024 * 1024),
        cost_estimate=pl.CostEstimate(
            flops=1_000_000_000, bytes_accessed=3_000_000, transcendentals=300_000
        ),
        name="finish_mixer",
    )(omap, oloc, states, gate, gain.reshape(1, -1))


def swiglu(rows, gate_w, up_w):
    return (jax.nn.silu(dot(rows, gate_w)) * dot(rows, up_w)).astype(BF16)


def on_device(
    query_vectors,
    attend_lookup_vectors,
    attend_content_vectors,
    forget_speed_dependent,
    amend_speed_dependent,
    result_switch_preactivation,
    feature_forget_baseline,
    amend_speed_baseline,
    sudden_forget_extra,
    group_scaling_factor,
    result_mapping_matrix,
    specialist_tokens_activations,
    specialist_scaling_factor,
    selected_specialists,
    selection_mixing_factors,
    dispatched_switch_matrix,
    dispatched_raising_matrix,
    dispatched_lowering_matrix,
    common_switch_matrix,
    common_raising_matrix,
    common_lowering_matrix,
):
    floats = specialist_tokens_activations.astype(F32)
    normed = (
        floats
        * lax.rsqrt(jnp.mean(floats * floats, -1, keepdims=True) + 1e-06)
        * specialist_scaling_factor
    ).astype(BF16)
    tok_rows, top_count = selected_specialists.shape
    model_width = specialist_tokens_activations.shape[1]
    experts = lax.axis_size("ep")
    tp_size = lax.axis_size("tp")
    capacity = 3 * tok_rows * top_count // (2 * experts)
    slots = experts * capacity
    gates = lax.all_gather(dispatched_switch_matrix[0], "tp")
    ups = lax.all_gather(dispatched_raising_matrix[0], "tp")
    downs = lax.all_gather(dispatched_lowering_matrix[0], "tp")
    flat_ids = selected_specialists.reshape(-1)
    one_hot = (flat_ids[:, None] == jnp.arange(experts, dtype=jnp.int32)[None, :]).astype(jnp.int32)
    slot_rank = jnp.sum((jnp.cumsum(one_hot, axis=0) - 1) * one_hot, axis=1)
    position = flat_ids * capacity + slot_rank
    placing = (position[:, None] == jnp.arange(slots, dtype=jnp.int32)[None, :]).reshape(
        tok_rows, top_count, slots
    )
    outgoing = jnp.einsum(
        "te,td->ed", jnp.sum(placing.astype(BF16), axis=1), normed, preferred_element_type=F32
    ).astype(BF16)
    weight = jnp.sum(jnp.where(placing, selection_mixing_factors[:, :, None], 0.0), axis=1)
    received = lax.all_to_all(
        outgoing.reshape(experts, capacity, model_width),
        "ep",
        split_axis=0,
        concat_axis=0,
        tiled=True,
    ).reshape(slots, model_width)

    omap, oloc, pay = run_local_mixer(
        query_vectors,
        attend_lookup_vectors,
        attend_content_vectors,
        forget_speed_dependent,
        amend_speed_dependent,
        feature_forget_baseline,
        amend_speed_baseline,
        sudden_forget_extra,
    )
    states = run_fold_states(pay)
    mixed_rows = run_finish_mixer(
        omap, oloc, states, result_switch_preactivation, group_scaling_factor
    )

    hidden = jnp.concatenate(
        [swiglu(received, gates[r], ups[r]) for r in range(tp_size)], axis=1
    )
    expert_rows = dot(hidden, downs.reshape(hidden.shape[1], model_width)).astype(BF16)
    expert_out = lax.all_to_all(
        expert_rows.reshape(experts, capacity, model_width),
        "ep",
        split_axis=0,
        concat_axis=0,
        tiled=True,
    ).reshape(slots, model_width)
    high = weight.astype(BF16)
    low = (weight - high.astype(F32)).astype(BF16)
    routed = dot(high, expert_out) + dot(low, expert_out)

    shared_hidden = swiglu(
        lax.all_gather(normed, "tp", axis=0, tiled=True),
        common_switch_matrix,
        common_raising_matrix,
    )
    shared_sum = lax.psum_scatter(
        dot(shared_hidden, common_lowering_matrix).astype(BF16),
        "tp",
        scatter_dimension=0,
        tiled=True,
    )
    attend = lax.psum_scatter(
        dot(mixed_rows, result_mapping_matrix).astype(BF16),
        "tp",
        scatter_dimension=0,
        tiled=True,
    )
    return (attend, (routed + shared_sum.astype(F32)).astype(BF16))


def solution(mesh):
    rows = P(("grp", "ep"), "tp")
    tokens = P(("grp", "ep", "tp"), None)
    placed = (
        (rows,) * 6
        + (P("tp"), P("tp"), rows, P("tp"), P("tp", None), tokens, P(), tokens, tokens)
        + (P("ep", None, "tp"), P("ep", None, "tp"), P("ep", "tp", None))
        + (P(None, "tp"), P(None, "tp"), P("tp", None))
    )
    return jax.shard_map(
        on_device, mesh=mesh, in_specs=placed, out_specs=(tokens, tokens), check_vma=False
    )
```

```python
import functools

import jax
import jax.numpy as jnp
from jax import lax
from jax.experimental import pallas as pl
from jax.experimental.pallas import tpu as pltpu
from jax.sharding import PartitionSpec as P

F32 = jnp.float32
BF16 = jnp.bfloat16
SPAN = 64
MESH = pl.DeviceIdType.MESH


def dot(a, b):
    return jnp.dot(a, b, preferred_element_type=F32)


def dot_nt(a, b):
    return lax.dot_general(a, b, (((1,), (1,)), ((), ())), preferred_element_type=F32)


def dot_tn(a, b):
    return lax.dot_general(a, b, (((0,), (0,)), ((), ())), preferred_element_type=F32)


def split(x, parts):
    out = []
    for _ in range(parts - 1):
        out.append(x.astype(BF16))
        x = x - out[-1].astype(F32)
    out.append(x.astype(BF16))
    return out


def iota(shape, dim):
    return lax.broadcasted_iota(jnp.int32, shape, dim)


def local_mixer(
    pair, q_ref, k_ref, v_ref, f_ref, a_ref, fb_ref, ab_ref, x_ref, omap_ref, oloc_ref, pay_ref
):
    rows = q_ref.shape[0]
    groups = x_ref.shape[0]
    half = q_ref.shape[1] // groups
    lanes = 2 * half
    spans = rows // SPAN
    here = pl.ds(pl.multiple_of(pair * lanes, lanes), lanes)
    low = iota((SPAN, lanes), 1) < half
    col = jnp.where(low, iota((SPAN, lanes), 1), iota((SPAN, lanes), 1) - half)
    row = iota((SPAN, lanes), 0)
    strict = row > col
    inclusive = row >= col
    tri = (iota((SPAN, SPAN), 0) >= iota((SPAN, SPAN), 1)).astype(BF16)
    tri3 = jnp.concatenate([tri] * 3, axis=1)
    same = ((iota((lanes, lanes), 0) < half) == (iota((lanes, lanes), 1) < half)).astype(BF16)
    same2 = jnp.concatenate([same] * 2, axis=0)
    spread = (
        iota((groups, lanes), 0) == 2 * pair + (iota((groups, lanes), 1) >= half).astype(jnp.int32)
    ).astype(F32)
    spread3 = jnp.concatenate([spread] * 3, axis=0).astype(BF16)
    below = iota((lanes, lanes), 0) < half
    left = iota((lanes, lanes), 1) < half

    def stack(x):
        return jnp.concatenate([jnp.where(low, x, 0.0), jnp.where(low, 0.0, x)], axis=0).astype(
            BF16
        )

    fb = fb_ref[:, here]
    ab = ab_ref[:, here]
    parts = [part.astype(F32) for part in split(x_ref[...], 3)]
    extra = dot_tn(jnp.concatenate(parts, axis=0).astype(BF16), spread3)

    spans_in = []
    for c in range(spans):
        at = slice(c * SPAN, (c + 1) * SPAN)
        decay = -jnp.exp(fb + f_ref[at, here].astype(F32)) + extra[at, :]
        rate = jax.nn.sigmoid(ab + a_ref[at, here].astype(F32))
        key = k_ref[at, here].astype(F32)
        sq = dot(jnp.concatenate(split(key * key, 2), axis=1), same2)
        unit = key * lax.rsqrt(sq + 1e-06)
        cum = dot(tri3, jnp.concatenate(split(decay, 3), axis=0))
        mid = cum[SPAN // 2 : SPAN // 2 + 1, :]
        last = cum[SPAN - 1 : SPAN, :]
        left_erase = -unit * jnp.exp(cum - decay - mid)
        left_read = q_ref[at, here].astype(F32) * jnp.exp(cum - mid)
        right = jnp.exp(mid - cum) * rate
        right_erase = unit * right
        right_write = key * right
        grow = jnp.exp(mid)
        tail = jnp.exp(last - mid)
        lefts = jnp.concatenate([left_erase, left_read], axis=0).astype(BF16)
        rights = jnp.concatenate([stack(right_erase), stack(right_write)], axis=0)
        pairs = dot_nt(lefts, rights)
        a_mat = jnp.where(strict, pairs[:SPAN, :lanes], 0.0)
        erase_write = jnp.where(strict, pairs[:SPAN, lanes:], 0.0)
        read_erase = jnp.where(inclusive, pairs[SPAN:, :lanes], 0.0)
        read_write = jnp.where(inclusive, pairs[SPAN:, lanes:], 0.0)
        value = v_ref[at, here].astype(F32)
        writes = dot(
            jnp.concatenate([erase_write, read_write], axis=0).astype(BF16), stack(value)
        )
        ends = jnp.concatenate([right_erase * tail, right_write * tail], axis=0).astype(BF16)
        spans_in.append(
            dict(
                a=a_mat,
                first=stack(left_erase * grow),
                read=left_read * grow,
                re=read_erase.astype(BF16),
                ew=stack(writes[:SPAN]),
                rw=writes[SPAN:],
                ends=ends,
                value=v_ref[at, here],
                last=jnp.exp(last),
            )
        )

    eye = (row == col).astype(F32)
    block = 1
    inverse = None
    while block < SPAN:
        in_block = (row // (2 * block) == col // (2 * block)) & (
            (row // block) % 2 == 1
        ) & ((col // block) % 2 == 0)
        steps = [jnp.where(in_block, s["a"], 0.0) for s in spans_in]
        if inverse is None:
            inverse = [eye + step for step in steps]
        else:
            inner = [
                dot(step.astype(BF16), stack(x)) for step, x in zip(steps, inverse)
            ]
            inverse = [x + dot(x.astype(BF16), stack(y)) for x, y in zip(inverse, inner)]
        block *= 2

    state = jnp.concatenate([eye, jnp.zeros_like(eye)], axis=0)
    for c, s in enumerate(spans_in):
        at = slice(c * SPAN, (c + 1) * SPAN)
        solved = dot(inverse[c].astype(BF16), jnp.concatenate([s["first"], s["ew"]], axis=1))
        w, y = (solved[:, :lanes], solved[:, lanes:])
        seen = dot(s["re"], jnp.concatenate([stack(w), stack(y)], axis=1))
        read = s["read"] + seen[:, :lanes]
        added = s["rw"] + seen[:, lanes:]
        value = s["value"]
        erased = dot_tn(w.astype(BF16), s["ends"][:SPAN])
        erased = jnp.where(below == left, erased, 0.0).astype(BF16)
        offset = dot_tn(jnp.concatenate([y.astype(BF16), value], axis=0), s["ends"])
        offset = jnp.where(low, offset[:half], offset[half:])
        both = jnp.concatenate([stack(state[:SPAN]), stack(state[SPAN:])], axis=0)
        reads = dot_nt(read.astype(BF16), both)
        omap_ref[at, here] = reads[:, :lanes].astype(BF16)
        oloc_ref[at, here] = added + reads[:, lanes:]
        state = (
            state * s["last"]
            + dot(state.astype(BF16), erased)
            + jnp.concatenate([jnp.zeros_like(offset), offset], axis=0)
        )
    jump, offset = (state[:SPAN], state[SPAN:])
    quarter = SPAN // 4
    eighth = SPAN // 8
    half_low = low[: SPAN // 2]
    jump_turned = pltpu.roll(jump, half, 1)
    offset_turned = pltpu.roll(offset, half, 1)
    empty = jnp.zeros((eighth, lanes), F32)
    for h in range(2):
        top = (jump, jump_turned)[h][: SPAN // 2]
        bottom = (jump_turned, jump)[h][SPAN // 2 :]
        packed = jnp.where(half_low, top, bottom)
        for j in range(4):
            top = (offset, offset_turned)[h][j * quarter : j * quarter + eighth]
            bottom = (offset_turned, offset)[h][j * quarter + eighth : (j + 1) * quarter]
            piece = jnp.where(low[:eighth], top, bottom)
            pay_ref[8 * pair + 4 * h + j] = jnp.concatenate([packed, piece, empty], axis=0).astype(
                BF16
            )


def fold_step(state, arrived):
    lanes = state.shape[1]
    half = lanes // 2
    low = iota((lanes // 4, lanes), 1) < half
    block = arrived.astype(F32)
    jump, offset = (block[: lanes // 4], block[lanes // 4 : lanes // 4 + 8])
    turned = pltpu.roll(jump, half, 1)
    spread = jnp.concatenate(
        [
            jnp.where(low, jump, 0.0),
            jnp.where(low, turned, 0.0),
            jnp.where(low, 0.0, turned),
            jnp.where(low, 0.0, jump),
        ],
        axis=0,
    ).astype(BF16)
    parts = [part.astype(F32) for part in split(state, 2)]
    moved = dot(jnp.concatenate(parts, axis=0).astype(BF16), spread)
    return moved[:8] + moved[8:] + offset


def finish_mixer(pair, omap_ref, oloc_ref, state_ref, gate_ref, gain_ref, out_ref):
    lanes = state_ref.shape[2]
    half = lanes // 2
    here = pl.ds(pl.multiple_of(pair * lanes, lanes), lanes)
    low = iota((8, lanes), 1) < half
    zero = jnp.zeros((8, lanes), F32)
    tiles = []
    for h in range(2):
        for j in range(4):
            block = state_ref[8 * pair + 4 * h + j]
            turned = pltpu.roll(block, half, 1)
            if h == 0:
                tiles += [jnp.where(low, block, zero), jnp.where(low, turned, zero)]
            else:
                tiles += [jnp.where(low, zero, turned), jnp.where(low, zero, block)]
    state = jnp.concatenate(tiles, axis=0).astype(BF16)
    same = jnp.where(
        (iota((lanes, lanes), 0) < half) == (iota((lanes, lanes), 1) < half), 1.0 / half, 0.0
    ).astype(BF16)
    same2 = jnp.concatenate([same] * 2, axis=0)
    head_out = oloc_ref[:, here] + dot_nt(omap_ref[:, here], state)
    mean = dot(jnp.concatenate(split(head_out, 2), axis=1), same2)
    centered = head_out - mean
    var = dot(jnp.concatenate(split(centered * centered, 2), axis=1), same2)
    normed = centered * lax.rsqrt(var + 0.00064) * gain_ref[:, here]
    out_ref[:, here] = (normed * jax.nn.sigmoid(gate_ref[:, here].astype(F32))).astype(BF16)


def slot_hits(ids, experts, capacity):
    tokens = ids.shape[1]
    ids = ids.astype(F32)
    expert = iota((experts, tokens), 0).astype(F32)
    hot = [(expert == ids[j : j + 1]).astype(F32) for j in range(2)]
    earlier = (iota((tokens, tokens), 0) < iota((tokens, tokens), 1)).astype(F32).astype(BF16)
    before = dot((hot[0] + hot[1]).astype(BF16), earlier)
    place = [
        ids[j : j + 1] * capacity + jnp.sum(hot[j] * before, axis=0, keepdims=True)
        for j in range(2)
    ]
    at = iota((16 * experts, tokens), 0)
    base = (capacity * (at // 16) + at % 4).astype(F32)
    quarter = (at // 4) % 4
    groups = [[base + 4 * g == place[j] for j in range(2)] for g in range(capacity // 4)]
    return groups, quarter


def everything(
    capacity,
    q_in,
    k_in,
    v_in,
    f_in,
    a_in,
    g_in,
    fb_ref,
    ab_ref,
    x_ref,
    gain_ref,
    wout_in,
    tok_ref,
    scale_ref,
    ids_ref,
    mix_ref,
    gate_in,
    up_in,
    down_in,
    cgate_in,
    cup_in,
    cdown_in,
    attend_ref,
    moe_ref,
    q_ref,
    k_ref,
    v_ref,
    f_ref,
    a_ref,
    g_ref,
    wout_ref,
    wg_ref,
    wu_ref,
    wd_ref,
    cgu_ref,
    cd_ref,
    omap_ref,
    oloc_ref,
    pay_ref,
    arrived,
    sent,
    states,
    mixed_ref,
    out_buf,
    in_buf,
    ret_buf,
    back_buf,
    xbuf,
    yacc,
    hbuf,
    normed_own,
    ngather,
    part_a,
    part_b,
    relay_a,
    relay_b,
    sums_a,
    sums_b,
    load_sem,
    own_sem,
    out_send,
    out_recv,
    pay_send,
    pay_recv,
    home_send,
    home_recv,
    ret_send,
    ret_recv,
    ring_send,
    ring_recv,
    rs_send,
    rs_recv,
):
    experts = out_buf.shape[0]
    tps = ngather.shape[0]
    tokens, width = tok_ref.shape
    quarter_width = width // 4
    groups = capacity // 4
    pairs = omap_ref.shape[1] // sent.shape[2]
    ep = lax.axis_index("ep")
    tp = lax.axis_index("tp")
    right, left, across = (lax.rem(tp + 1, tps), lax.rem(tp + 3, tps), lax.rem(tp + 2, tps))

    barrier = pltpu.get_barrier_semaphore()

    def greet(d, carry):
        pl.semaphore_signal(
            barrier, inc=1, device_id={"ep": lax.rem(ep + d, experts)}, device_id_type=MESH
        )
        return carry

    lax.fori_loop(1, experts, greet, 0)
    for near in (right, left):
        pl.semaphore_signal(barrier, inc=1, device_id={"tp": near}, device_id_type=MESH)

    half_lanes = cgate_in.shape[1]
    hid = gate_in.shape[1]
    loads = [
        pltpu.make_async_copy(a, b, load_sem.at[i])
        for i, (a, b) in enumerate(
            [
                (q_in, q_ref),
                (k_in, k_ref),
                (v_in, v_ref),
                (f_in, f_ref),
                (a_in, a_ref),
                (g_in, g_ref),
                (wout_in, wout_ref),
                (gate_in, wg_ref.at[0]),
                (up_in, wu_ref.at[0]),
                (down_in, wd_ref.at[pl.ds(0, hid)]),
                (cgate_in, cgu_ref.at[:, pl.ds(0, half_lanes)]),
                (cup_in, cgu_ref.at[:, pl.ds(half_lanes, half_lanes)]),
                (cdown_in, cd_ref),
            ]
        )
    ]
    for load in loads:
        load.start()

    def remote(src, dst, send, recv, axis, to):
        return pltpu.make_async_remote_copy(
            src_ref=src,
            dst_ref=dst,
            send_sem=send,
            recv_sem=recv,
            device_id={axis: to},
            device_id_type=MESH,
        )

    floats = tok_ref[...].astype(F32)
    normed = (
        floats
        * lax.rsqrt(jnp.mean(floats * floats, -1, keepdims=True) + 1e-06)
        * scale_ref[...]
    ).astype(BF16)
    normed_own[...] = normed
    hits, quarter = slot_hits(ids_ref[...], experts, capacity)
    stacked = jnp.concatenate(
        [normed[:, c * quarter_width : (c + 1) * quarter_width] for c in range(4)], axis=0
    )
    for g in range(groups):
        either = hits[g][0] | hits[g][1]
        placing = jnp.concatenate(
            [(either & (quarter == c)).astype(F32).astype(BF16) for c in range(4)], axis=1
        )
        out_buf[:, :, g * quarter_width : (g + 1) * quarter_width] = (
            dot(placing, stacked).astype(BF16).reshape(experts, 16, quarter_width)
        )

    pl.semaphore_wait(barrier, experts - 1 + 2)

    def peer(d):
        return lax.rem(ep + d, experts)

    def outward(d):
        to = peer(d)
        return remote(out_buf.at[to], in_buf.at[ep], out_send.at[d], out_recv.at[ep], "ep", to)

    def inward(d):
        e = peer(d)
        return remote(out_buf.at[e], in_buf.at[e], out_send.at[d], out_recv.at[e], "ep", e)

    def spray(make):
        def go(i, carry):
            d = experts // 2 - i
            make(d).start()
            make(experts - d).start()
            return carry

        make(experts // 2).start()
        lax.fori_loop(1, experts // 2, go, 0)

    def drain(make, recv):
        def go(d, carry):
            if recv:
                make(d).wait_recv()
            else:
                make(d).wait_send()
            return carry

        lax.fori_loop(1, experts, go, 0)

    spray(outward)

    class Ring:
        def __init__(self, index, own, slot):
            n = own.shape[0]
            top, bottom = (pl.ds(0, n // 2), pl.ds(n // 2, n // 2))
            s = [ring_send.at[4 * index + i] for i in range(4)]
            r = [ring_recv.at[4 * index + i] for i in range(4)]
            self.near = [
                remote(own, slot(1, pl.ds(0, n)), s[0], r[0], "tp", right),
                remote(own, slot(2, pl.ds(0, n)), s[1], r[1], "tp", left),
            ]
            self.far = [
                remote(slot(1, top), slot(3, top), s[2], r[2], "tp", right),
                remote(slot(2, bottom), slot(3, bottom), s[3], r[3], "tp", left),
            ]

        def start(self):
            for copy in self.near:
                copy.start()

        def forward(self):
            for copy, onward in zip(self.near, self.far):
                copy.wait_recv()
                onward.start()

        def arrive(self):
            for copy in self.far:
                copy.wait_recv()

        def finish(self):
            for copy in self.near + self.far:
                copy.wait_send()

    gate_ring = Ring(0, gate_in, lambda s, rows: wg_ref.at[s, rows])
    up_ring = Ring(1, up_in, lambda s, rows: wu_ref.at[s, rows])
    down_ring = Ring(
        2, down_in, lambda s, rows: wd_ref.at[pl.ds(s * hid + rows.start, rows.size)]
    )
    normed_ring = Ring(3, normed_own, lambda s, rows: ngather.at[s, rows])
    weight_rings = (gate_ring, up_ring, down_ring)
    for ring in weight_rings:
        ring.start()

    own_out = pltpu.make_async_copy(out_buf.at[ep], in_buf.at[ep], own_sem.at[0])
    own_out.start()
    own_normed = pltpu.make_async_copy(normed_own, ngather.at[0], own_sem.at[1])
    own_normed.start()

    for load in loads[:5]:
        load.wait()

    def mix(pair, carry):
        local_mixer(
            pair,
            q_ref,
            k_ref,
            v_ref,
            f_ref,
            a_ref,
            fb_ref,
            ab_ref,
            x_ref,
            omap_ref,
            oloc_ref,
            pay_ref,
        )
        return carry

    lax.fori_loop(0, pairs, mix, 0)

    def pay_out(d):
        to = peer(d)
        return remote(pay_ref.at[to], arrived.at[ep], pay_send.at[d], pay_recv.at[ep], "ep", to)

    def pay_in(e):
        return remote(pay_ref.at[e], arrived.at[e], pay_send.at[0], pay_recv.at[e], "ep", e)

    spray(pay_out)
    own_pay = pltpu.make_async_copy(pay_ref.at[ep], arrived.at[ep], own_sem.at[2])
    own_pay.start()

    for ring in weight_rings:
        ring.forward()
    normed_ring.start()

    own_out.wait()
    drain(inward, True)
    block_rows = 4 * experts
    at_row = iota((block_rows, 16 * experts), 0)
    at_col = iota((block_rows, 16 * experts), 1)
    for c in range(4):
        pick = (at_col == 16 * (at_row // 4) + 4 * c + at_row % 4).astype(F32).astype(BF16)
        for g in range(groups):
            block = in_buf[:, :, g * quarter_width : (g + 1) * quarter_width].reshape(
                16 * experts, quarter_width
            )
            xbuf[
                g * block_rows : (g + 1) * block_rows,
                c * quarter_width : (c + 1) * quarter_width,
            ] = dot(pick, block).astype(BF16)

    for load in loads[7:10]:
        load.wait()

    def hidden(s):
        rows = xbuf[...]
        return (jax.nn.silu(dot(rows, wg_ref[s])) * dot(rows, wu_ref[s])).astype(BF16)

    for s in range(3):
        hbuf[:, s * hid : (s + 1) * hid] = hidden(s)
    yacc[...] = dot(hbuf[...], wd_ref[: 3 * hid])

    own_pay.wait()

    def homeward(e):
        return remote(sent.at[e], states.at[ep], home_send.at[e], home_recv.at[ep], "ep", e)

    def home(e):
        return remote(sent.at[e], states.at[e], home_send.at[e], home_recv.at[e], "ep", e)

    def step(e, state):
        sent[e] = state

        @pl.when(e != ep)
        def _():
            pay_in(e).wait_recv()

        @pl.when((e > 0) & (e - 1 != ep))
        def _():
            homeward(e - 1).start()

        return fold_step(state, arrived[e])

    lax.fori_loop(0, experts, step, jnp.zeros(sent.shape[1:], F32))

    @pl.when(ep != experts - 1)
    def _():
        homeward(experts - 1).start()

    own_state = pltpu.make_async_copy(sent.at[ep], states.at[ep], own_sem.at[3])
    own_state.start()

    for ring in weight_rings:
        ring.arrive()
    total = yacc[...] + dot(hidden(3), wd_ref[3 * hid :])
    yacc[...] = total
    at_row = iota((16 * experts, block_rows), 0)
    at_col = iota((16 * experts, block_rows), 1)
    put = jnp.concatenate(
        [
            (at_row == 16 * (at_col // 4) + 4 * c + at_col % 4).astype(F32).astype(BF16)
            for c in range(4)
        ],
        axis=1,
    )
    for g in range(groups):
        rows = yacc[g * block_rows : (g + 1) * block_rows, :].astype(BF16)
        rows = jnp.concatenate(
            [rows[:, c * quarter_width : (c + 1) * quarter_width] for c in range(4)], axis=0
        )
        ret_buf[:, :, g * quarter_width : (g + 1) * quarter_width] = (
            dot(put, rows).astype(BF16).reshape(experts, 16, quarter_width)
        )

    def ret_out(d):
        to = peer(d)
        return remote(ret_buf.at[to], back_buf.at[ep], ret_send.at[d], ret_recv.at[ep], "ep", to)

    def ret_in(d):
        e = peer(d)
        return remote(ret_buf.at[e], back_buf.at[e], ret_send.at[d], ret_recv.at[e], "ep", e)

    spray(ret_out)
    own_ret = pltpu.make_async_copy(ret_buf.at[ep], back_buf.at[ep], own_sem.at[4])
    own_ret.start()

    def homecoming(d, carry):
        home(peer(d)).wait_recv()
        return carry

    lax.fori_loop(1, experts, homecoming, 0)
    own_state.wait()
    for load in loads[5:7]:
        load.wait()

    def finish(pair, carry):
        finish_mixer(pair, omap_ref, oloc_ref, states, g_ref, gain_ref, mixed_ref)
        return carry

    lax.fori_loop(0, pairs, finish, 0)

    class Scatter:
        def __init__(self, index, part, relay, sums):
            n = part.shape[1]
            top, bottom = (pl.ds(0, n // 2), pl.ds(n // 2, n // 2))
            s = [rs_send.at[6 * index + i] for i in range(6)]
            r = [rs_recv.at[6 * index + i] for i in range(6)]
            self.part, self.sums = (part, sums)
            self.near = [
                remote(part.at[3, top], relay.at[0], s[0], r[0], "tp", right),
                remote(part.at[3, bottom], relay.at[1], s[1], r[1], "tp", left),
                remote(part.at[2], sums.at[1], s[2], r[2], "tp", right),
                remote(part.at[1], sums.at[2], s[3], r[3], "tp", left),
            ]
            self.far = [
                remote(relay.at[0], sums.at[3, top], s[4], r[4], "tp", right),
                remote(relay.at[1], sums.at[3, bottom], s[5], r[5], "tp", left),
            ]

        def start(self):
            for copy in self.near:
                copy.start()

        def forward(self):
            for copy, onward in zip(self.near[:2], self.far):
                copy.wait_recv()
                onward.start()

        def total(self):
            for copy in self.near[2:] + self.far:
                copy.wait_recv()
            out = self.part[0].astype(F32)
            for s in range(1, 4):
                out = out + self.sums[s].astype(F32)
            return out

        def finish(self):
            for copy in self.near + self.far:
                copy.wait_send()

    scatter_a = Scatter(0, part_a, relay_a, sums_a)
    scatter_b = Scatter(1, part_b, relay_b, sums_b)
    mixer_rows = part_a.shape[1]
    for s, owner in enumerate((tp, left, right, across)):
        mine = pl.ds(pl.multiple_of(owner * mixer_rows, mixer_rows), mixer_rows)
        part_a[s] = dot(mixed_ref[mine, :], wout_ref[...]).astype(BF16)
    scatter_a.start()

    normed_ring.forward()
    own_normed.wait()
    for load in loads[10:13]:
        load.wait()
    normed_ring.arrive()
    scatter_a.forward()
    both = dot(ngather[...].reshape(tps * tokens, width), cgu_ref[...])
    inner = (jax.nn.silu(both[:, :half_lanes]) * both[:, half_lanes:]).astype(BF16)
    for s in range(4):
        part_b[s] = dot(inner[s * tokens : (s + 1) * tokens], cd_ref[...]).astype(BF16)
    scatter_b.start()
    scatter_b.forward()
    attend_ref[...] = scatter_a.total().astype(BF16)
    moe_sum = scatter_b.total()
    yacc[:tokens, :] = moe_sum

    hits, quarter = slot_hits(ids_ref[...], experts, capacity)
    own_ret.wait()
    drain(ret_in, True)
    for c in range(4):
        block = yacc[:tokens, c * quarter_width : (c + 1) * quarter_width]
        for g in range(groups):
            weight = jnp.where(hits[g][0], mix_ref[0:1, :], 0.0) + jnp.where(
                hits[g][1], mix_ref[1:2, :], 0.0
            )
            weight = jnp.where(quarter == c, weight, 0.0)
            values = back_buf[:, :, g * quarter_width : (g + 1) * quarter_width].reshape(
                16 * experts, quarter_width
            )
            for part in split(weight, 2):
                block = block + dot_tn(part, values)
        moe_ref[:, c * quarter_width : (c + 1) * quarter_width] = block.astype(BF16)

    drain(outward, False)
    drain(pay_out, False)
    drain(ret_out, False)

    def homegoing(d, carry):
        homeward(peer(d)).wait_send()
        return carry

    lax.fori_loop(1, experts, homegoing, 0)
    for item in weight_rings + (normed_ring, scatter_a, scatter_b):
        item.finish()


def on_device(
    query_vectors,
    attend_lookup_vectors,
    attend_content_vectors,
    forget_speed_dependent,
    amend_speed_dependent,
    result_switch_preactivation,
    feature_forget_baseline,
    amend_speed_baseline,
    sudden_forget_extra,
    group_scaling_factor,
    result_mapping_matrix,
    specialist_tokens_activations,
    specialist_scaling_factor,
    selected_specialists,
    selection_mixing_factors,
    dispatched_switch_matrix,
    dispatched_raising_matrix,
    dispatched_lowering_matrix,
    common_switch_matrix,
    common_raising_matrix,
    common_lowering_matrix,
):
    tokens, top_count = selected_specialists.shape
    width = specialist_tokens_activations.shape[1]
    rows, mix_width = query_vectors.shape
    groups = sudden_forget_extra.shape[1]
    lanes = 2 * (mix_width // groups)
    experts = lax.axis_size("ep")
    tps = lax.axis_size("tp")
    capacity = 3 * tokens * top_count // (2 * experts)
    hid = dispatched_switch_matrix.shape[2]
    shared = common_switch_matrix.shape[1]
    slab = (experts, 16, capacity * width // 16)
    vmem = pl.BlockSpec(memory_space=pltpu.VMEM)
    hbm = pl.BlockSpec(memory_space=pl.ANY)
    V = pltpu.VMEM
    dma = pltpu.SemaphoreType.DMA
    mixer_rows = rows // tps
    return pl.pallas_call(
        functools.partial(everything, capacity),
        in_specs=[hbm] * 6 + [vmem] * 4 + [hbm] + [vmem] * 4 + [hbm] * 6,
        out_specs=(vmem, vmem),
        out_shape=(
            jax.ShapeDtypeStruct((mixer_rows, width), BF16),
            jax.ShapeDtypeStruct((tokens, width), BF16),
        ),
        scratch_shapes=[V((rows, mix_width), BF16)] * 6
        + [
            V((mix_width, width), BF16),
            V((tps, width, hid), BF16),
            V((tps, width, hid), BF16),
            V((tps * hid, width), BF16),
            V((width, 2 * shared), BF16),
            V((shared, width), BF16),
            V((rows, mix_width), BF16),
            V((rows, mix_width), F32),
            V((experts, 48, lanes), BF16),
            V((experts, 48, lanes), BF16),
            V((experts, 8, lanes), F32),
            V((experts, 8, lanes), F32),
            V((rows, mix_width), BF16),
        ]
        + [V(slab, BF16)] * 4
        + [
            V((experts * capacity, width), BF16),
            V((experts * capacity, width), F32),
            V((experts * capacity, 3 * hid), BF16),
            V((tokens, width), BF16),
            V((tps, tokens, width), BF16),
            V((tps, mixer_rows, width), BF16),
            V((tps, tokens, width), BF16),
            V((2, mixer_rows // 2, width), BF16),
            V((2, tokens // 2, width), BF16),
            V((tps, mixer_rows, width), BF16),
            V((tps, tokens, width), BF16),
            dma((13,)),
            dma((5,)),
        ]
        + [dma((experts,))] * 8
        + [dma((16,)), dma((16,)), dma((12,)), dma((12,))],
        compiler_params=pltpu.CompilerParams(
            collective_id=0, has_side_effects=True, vmem_limit_bytes=62 * 1024 * 1024
        ),
        name="everything",
    )(
        query_vectors,
        attend_lookup_vectors,
        attend_content_vectors,
        forget_speed_dependent,
        amend_speed_dependent,
        result_switch_preactivation,
        feature_forget_baseline.reshape(1, -1),
        amend_speed_baseline.reshape(1, -1),
        sudden_forget_extra.T,
        group_scaling_factor.reshape(1, -1),
        result_mapping_matrix,
        specialist_tokens_activations,
        specialist_scaling_factor.reshape(1, -1),
        selected_specialists.T,
        selection_mixing_factors.T,
        dispatched_switch_matrix[0],
        dispatched_raising_matrix[0],
        dispatched_lowering_matrix[0],
        common_switch_matrix,
        common_raising_matrix,
        common_lowering_matrix,
    )


def solution(mesh):
    rows = P(("grp", "ep"), "tp")
    tokens = P(("grp", "ep", "tp"), None)
    placed = (
        (rows,) * 6
        + (P("tp"), P("tp"), rows, P("tp"), P("tp", None), tokens, P(), tokens, tokens)
        + (P("ep", None, "tp"), P("ep", None, "tp"), P("ep", "tp", None))
        + (P(None, "tp"), P(None, "tp"), P("tp", None))
    )
    return jax.shard_map(
        on_device, mesh=mesh, in_specs=placed, out_specs=(tokens, tokens), check_vma=False
    )
```

```python
import functools

import jax
import jax.numpy as jnp
from jax import lax
from jax.experimental import pallas as pl
from jax.experimental.pallas import tpu as pltpu
from jax.sharding import PartitionSpec as P

F32 = jnp.float32
BF16 = jnp.bfloat16
SPAN = 64
MESH = pl.DeviceIdType.MESH


def dot(a, b):
    return jnp.dot(a, b, preferred_element_type=F32)


def dot_nt(a, b):
    return lax.dot_general(a, b, (((1,), (1,)), ((), ())), preferred_element_type=F32)


def dot_tn(a, b):
    return lax.dot_general(a, b, (((0,), (0,)), ((), ())), preferred_element_type=F32)


def split(x, parts):
    out = []
    for _ in range(parts - 1):
        out.append(x.astype(BF16))
        x = x - out[-1].astype(F32)
    out.append(x.astype(BF16))
    return out


def iota(shape, dim):
    return lax.broadcasted_iota(jnp.int32, shape, dim)


def local_mixer(
    pair, q_ref, k_ref, v_ref, f_ref, a_ref, fb_ref, ab_ref, x_ref, omap_ref, oloc_ref, pay_ref
):
    rows = q_ref.shape[0]
    groups = x_ref.shape[0]
    half = q_ref.shape[1] // groups
    lanes = 2 * half
    spans = rows // SPAN
    here = pl.ds(pl.multiple_of(pair * lanes, lanes), lanes)
    low = iota((SPAN, lanes), 1) < half
    col = jnp.where(low, iota((SPAN, lanes), 1), iota((SPAN, lanes), 1) - half)
    row = iota((SPAN, lanes), 0)
    strict = row > col
    inclusive = row >= col
    tri = (iota((SPAN, SPAN), 0) >= iota((SPAN, SPAN), 1)).astype(BF16)
    tri3 = jnp.concatenate([tri] * 3, axis=1)
    same = ((iota((lanes, lanes), 0) < half) == (iota((lanes, lanes), 1) < half)).astype(BF16)
    same2 = jnp.concatenate([same] * 2, axis=0)
    spread = (
        iota((groups, lanes), 0) == 2 * pair + (iota((groups, lanes), 1) >= half).astype(jnp.int32)
    ).astype(F32)
    spread3 = jnp.concatenate([spread] * 3, axis=0).astype(BF16)
    below = iota((lanes, lanes), 0) < half
    left = iota((lanes, lanes), 1) < half

    def stack(x):
        return jnp.concatenate([jnp.where(low, x, 0.0), jnp.where(low, 0.0, x)], axis=0).astype(
            BF16
        )

    fb = fb_ref[:, here]
    ab = ab_ref[:, here]
    parts = [part.astype(F32) for part in split(x_ref[...], 3)]
    extra = dot_tn(jnp.concatenate(parts, axis=0).astype(BF16), spread3)

    spans_in = []
    for c in range(spans):
        at = slice(c * SPAN, (c + 1) * SPAN)
        decay = -jnp.exp(fb + f_ref[at, here].astype(F32)) + extra[at, :]
        rate = jax.nn.sigmoid(ab + a_ref[at, here].astype(F32))
        key = k_ref[at, here].astype(F32)
        sq = dot(jnp.concatenate(split(key * key, 2), axis=1), same2)
        unit = key * lax.rsqrt(sq + 1e-06)
        cum = dot(tri3, jnp.concatenate(split(decay, 3), axis=0))
        mid = cum[SPAN // 2 : SPAN // 2 + 1, :]
        last = cum[SPAN - 1 : SPAN, :]
        left_erase = -unit * jnp.exp(cum - decay - mid)
        left_read = q_ref[at, here].astype(F32) * jnp.exp(cum - mid)
        right = jnp.exp(mid - cum) * rate
        right_erase = unit * right
        right_write = key * right
        grow = jnp.exp(mid)
        tail = jnp.exp(last - mid)
        lefts = jnp.concatenate([left_erase, left_read], axis=0).astype(BF16)
        rights = jnp.concatenate([stack(right_erase), stack(right_write)], axis=0)
        pairs = dot_nt(lefts, rights)
        a_mat = jnp.where(strict, pairs[:SPAN, :lanes], 0.0)
        erase_write = jnp.where(strict, pairs[:SPAN, lanes:], 0.0)
        read_erase = jnp.where(inclusive, pairs[SPAN:, :lanes], 0.0)
        read_write = jnp.where(inclusive, pairs[SPAN:, lanes:], 0.0)
        value = v_ref[at, here].astype(F32)
        writes = dot(
            jnp.concatenate([erase_write, read_write], axis=0).astype(BF16), stack(value)
        )
        ends = jnp.concatenate([right_erase * tail, right_write * tail], axis=0).astype(BF16)
        spans_in.append(
            dict(
                a=a_mat,
                first=stack(left_erase * grow),
                read=left_read * grow,
                re=read_erase.astype(BF16),
                ew=stack(writes[:SPAN]),
                rw=writes[SPAN:],
                ends=ends,
                value=v_ref[at, here],
                last=jnp.exp(last),
            )
        )

    eye = (row == col).astype(F32)
    block = 1
    inverse = None
    while block < SPAN:
        in_block = (row // (2 * block) == col // (2 * block)) & (
            (row // block) % 2 == 1
        ) & ((col // block) % 2 == 0)
        steps = [jnp.where(in_block, s["a"], 0.0) for s in spans_in]
        if inverse is None:
            inverse = [eye + step for step in steps]
        else:
            inner = [
                dot(step.astype(BF16), stack(x)) for step, x in zip(steps, inverse)
            ]
            inverse = [x + dot(x.astype(BF16), stack(y)) for x, y in zip(inverse, inner)]
        block *= 2

    state = jnp.concatenate([eye, jnp.zeros_like(eye)], axis=0)
    for c, s in enumerate(spans_in):
        at = slice(c * SPAN, (c + 1) * SPAN)
        solved = dot(inverse[c].astype(BF16), jnp.concatenate([s["first"], s["ew"]], axis=1))
        w, y = (solved[:, :lanes], solved[:, lanes:])
        seen = dot(s["re"], jnp.concatenate([stack(w), stack(y)], axis=1))
        read = s["read"] + seen[:, :lanes]
        added = s["rw"] + seen[:, lanes:]
        value = s["value"]
        erased = dot_tn(w.astype(BF16), s["ends"][:SPAN])
        erased = jnp.where(below == left, erased, 0.0).astype(BF16)
        offset = dot_tn(jnp.concatenate([y.astype(BF16), value], axis=0), s["ends"])
        offset = jnp.where(low, offset[:half], offset[half:])
        both = jnp.concatenate([stack(state[:SPAN]), stack(state[SPAN:])], axis=0)
        reads = dot_nt(read.astype(BF16), both)
        omap_ref[at, here] = reads[:, :lanes].astype(BF16)
        oloc_ref[at, here] = added + reads[:, lanes:]
        state = (
            state * s["last"]
            + dot(state.astype(BF16), erased)
            + jnp.concatenate([jnp.zeros_like(offset), offset], axis=0)
        )
    jump, offset = (state[:SPAN], state[SPAN:])
    jump_turned = pltpu.roll(jump, half, 1)
    offset_turned = pltpu.roll(offset, half, 1)
    near = low[: SPAN // 2]
    for h in range(2):
        packed = [
            jnp.where(near, (x, turned)[h][: SPAN // 2], (turned, x)[h][SPAN // 2 :])
            for x, turned in ((jump, jump_turned), (offset, offset_turned))
        ]
        pay_ref[2 * pair + h] = jnp.concatenate(packed, axis=0).astype(BF16)


def fold_step(state, arrived):
    lanes = state.shape[1]
    half = lanes // 2
    low = iota(state.shape, 1) < half
    block = arrived.astype(F32)
    rows = state.shape[0]
    jump, offset = (block[:rows], block[rows:])
    turned = pltpu.roll(jump, half, 1)
    spread = jnp.concatenate(
        [
            jnp.where(low, jump, 0.0),
            jnp.where(low, turned, 0.0),
            jnp.where(low, 0.0, turned),
            jnp.where(low, 0.0, jump),
        ],
        axis=0,
    ).astype(BF16)
    parts = [part.astype(F32) for part in split(state, 2)]
    moved = dot(jnp.concatenate(parts, axis=0).astype(BF16), spread)
    return moved[:rows] + moved[rows:] + offset


def finish_mixer(pair, omap_ref, oloc_ref, state_ref, gate_ref, gain_ref, out_ref):
    lanes = state_ref.shape[2]
    half = lanes // 2
    here = pl.ds(pl.multiple_of(pair * lanes, lanes), lanes)
    low = iota(state_ref.shape[1:], 1) < half
    tiles = []
    for h in range(2):
        block = state_ref[2 * pair + h]
        turned = pltpu.roll(block, half, 1)
        if h == 0:
            tiles += [jnp.where(low, block, 0.0), jnp.where(low, turned, 0.0)]
        else:
            tiles += [jnp.where(low, 0.0, turned), jnp.where(low, 0.0, block)]
    state = jnp.concatenate(tiles, axis=0).astype(BF16)
    same = jnp.where(
        (iota((lanes, lanes), 0) < half) == (iota((lanes, lanes), 1) < half), 1.0 / half, 0.0
    ).astype(BF16)
    same2 = jnp.concatenate([same] * 2, axis=0)
    head_out = oloc_ref[:, here] + dot_nt(omap_ref[:, here], state)
    mean = dot(jnp.concatenate(split(head_out, 2), axis=1), same2)
    centered = head_out - mean
    var = dot(jnp.concatenate(split(centered * centered, 2), axis=1), same2)
    normed = centered * lax.rsqrt(var + 0.00064) * gain_ref[:, here]
    out_ref[:, here] = (normed * jax.nn.sigmoid(gate_ref[:, here].astype(F32))).astype(BF16)


def slot_hits(ids, experts, capacity):
    tokens = ids.shape[1]
    ids = ids.astype(F32)
    expert = iota((experts, tokens), 0).astype(F32)
    hot = [(expert == ids[j : j + 1]).astype(F32) for j in range(2)]
    earlier = (iota((tokens, tokens), 0) < iota((tokens, tokens), 1)).astype(F32).astype(BF16)
    before = dot((hot[0] + hot[1]).astype(BF16), earlier)
    place = [
        ids[j : j + 1] * capacity + jnp.sum(hot[j] * before, axis=0, keepdims=True)
        for j in range(2)
    ]
    at = iota((16 * experts, tokens), 0)
    base = (capacity * (at // 16) + at % 4).astype(F32)
    quarter = (at // 4) % 4
    groups = [[base + 4 * g == place[j] for j in range(2)] for g in range(capacity // 4)]
    return groups, quarter


def everything(
    capacity,
    q_in,
    k_in,
    v_in,
    f_in,
    a_in,
    g_in,
    fb_ref,
    ab_ref,
    x_ref,
    gain_ref,
    wout_in,
    tok_ref,
    scale_ref,
    ids_ref,
    mix_ref,
    gate_in,
    up_in,
    down_in,
    cgate_in,
    cup_in,
    cdown_in,
    attend_ref,
    moe_ref,
    q_ref,
    k_ref,
    v_ref,
    f_ref,
    a_ref,
    g_ref,
    wout_ref,
    wg_ref,
    wu_ref,
    wd_ref,
    cgu_ref,
    cd_ref,
    omap_ref,
    oloc_ref,
    pay_ref,
    arrived,
    sent,
    states,
    mixed_ref,
    out_buf,
    in_buf,
    ret_buf,
    back_buf,
    xbuf,
    yacc,
    hbuf,
    normed_own,
    ngather,
    part_a,
    part_b,
    relay_a,
    relay_b,
    sums_a,
    sums_b,
    load_sem,
    own_sem,
    out_send,
    out_recv,
    pay_send,
    pay_recv,
    home_send,
    home_recv,
    ret_send,
    ret_recv,
    ring_send,
    ring_recv,
    rs_send,
    rs_recv,
):
    experts = out_buf.shape[0]
    tps = ngather.shape[0]
    tokens, width = tok_ref.shape
    quarter_width = width // 4
    groups = capacity // 4
    pairs = omap_ref.shape[1] // sent.shape[2]
    ep = lax.axis_index("ep")
    tp = lax.axis_index("tp")
    right, left, across = (lax.rem(tp + 1, tps), lax.rem(tp + 3, tps), lax.rem(tp + 2, tps))
    paired = lax.axis_size("grp") % 2 == 0
    grp = lax.axis_index("grp")
    side = lax.rem(grp, 2)
    partner = grp + 1 - 2 * side
    heads = pay_ref.shape[0]
    stride = experts // heads
    my_head = ep // stride
    folds = lax.rem(ep, stride) == 0

    barrier = pltpu.get_barrier_semaphore()

    def greet(d, carry):
        pl.semaphore_signal(
            barrier, inc=1, device_id={"ep": lax.rem(ep + d, experts)}, device_id_type=MESH
        )
        return carry

    lax.fori_loop(1, experts, greet, 0)
    for near in (right, left):
        pl.semaphore_signal(barrier, inc=1, device_id={"tp": near}, device_id_type=MESH)
    if paired:
        pl.semaphore_signal(barrier, inc=1, device_id={"grp": partner}, device_id_type=MESH)

    half_lanes = cgate_in.shape[1]
    hid = gate_in.shape[1]
    loads = [
        pltpu.make_async_copy(a, b, load_sem.at[i])
        for i, (a, b) in enumerate(
            [
                (q_in, q_ref),
                (k_in, k_ref),
                (v_in, v_ref),
                (f_in, f_ref),
                (a_in, a_ref),
                (g_in, g_ref),
                (wout_in, wout_ref),
                (gate_in, wg_ref.at[0]),
                (up_in, wu_ref.at[0]),
                (down_in, wd_ref.at[pl.ds(0, hid)]),
                (cgate_in, cgu_ref.at[:, pl.ds(0, half_lanes)]),
                (cup_in, cgu_ref.at[:, pl.ds(half_lanes, half_lanes)]),
                (cdown_in, cd_ref),
            ]
        )
    ]
    for load in loads:
        load.start()

    def remote(src, dst, send, recv, axis, to):
        return pltpu.make_async_remote_copy(
            src_ref=src,
            dst_ref=dst,
            send_sem=send,
            recv_sem=recv,
            device_id={axis: to},
            device_id_type=MESH,
        )

    floats = tok_ref[...].astype(F32)
    normed = (
        floats
        * lax.rsqrt(jnp.mean(floats * floats, -1, keepdims=True) + 1e-06)
        * scale_ref[...]
    ).astype(BF16)
    normed_own[...] = normed
    hits, quarter = slot_hits(ids_ref[...], experts, capacity)
    stacked = jnp.concatenate(
        [normed[:, c * quarter_width : (c + 1) * quarter_width] for c in range(4)], axis=0
    )
    for g in range(groups):
        either = hits[g][0] | hits[g][1]
        placing = jnp.concatenate(
            [(either & (quarter == c)).astype(F32).astype(BF16) for c in range(4)], axis=1
        )
        out_buf[:, :, g * quarter_width : (g + 1) * quarter_width] = (
            dot(placing, stacked).astype(BF16).reshape(experts, 16, quarter_width)
        )

    pl.semaphore_wait(barrier, experts - 1 + 2 + int(paired))

    def peer(d):
        return lax.rem(ep + d, experts)

    def outward(d):
        to = peer(d)
        return remote(out_buf.at[to], in_buf.at[ep], out_send.at[d], out_recv.at[ep], "ep", to)

    def inward(d):
        e = peer(d)
        return remote(out_buf.at[e], in_buf.at[e], out_send.at[d], out_recv.at[e], "ep", e)

    def spray(make, first, last):
        def go(i, carry):
            d = experts // 2 - i
            make(d).start()
            make(experts - d).start()
            return carry

        if first == 0:
            make(experts // 2).start()
        lax.fori_loop(max(first, 1), last, go, 0)

    def drain(make, recv):
        def go(d, carry):
            if recv:
                make(d).wait_recv()
            else:
                make(d).wait_send()
            return carry

        lax.fori_loop(1, experts, go, 0)

    spray(outward, 0, experts // 2)

    class Ring:
        def __init__(self, index, own, slot, pair_left, pair_right):
            n = own.shape[0]
            mine = pl.ds(pl.multiple_of(side * (n // 2), n // 2), n // 2)
            other = pl.ds(pl.multiple_of((1 - side) * (n // 2), n // 2), n // 2)
            whole = pl.ds(0, n)
            s = [ring_send.at[6 * index + i] for i in range(6)]
            r = [ring_recv.at[6 * index + i] for i in range(6)]
            self.near, self.far, self.pair, self.paired_in = ([], [], [], [])
            for i, (to, half, rest, pair) in enumerate(
                [
                    (right, mine, other, paired and pair_left),
                    (left, other, mine, paired and pair_right),
                ]
            ):
                part = half if pair else whole
                self.near.append(
                    remote(own.at[part], slot(i + 1, part), s[i], r[i], "tp", to)
                )
                self.far.append(
                    remote(slot(i + 1, half), slot(3, half), s[2 + i], r[2 + i], "tp", to)
                )
                self.pair.append(
                    pair
                    and (
                        remote(
                            slot(i + 1, half), slot(i + 1, half), s[4 + i], r[4 + i], "grp", partner
                        ),
                        remote(
                            slot(i + 1, rest), slot(i + 1, rest), s[4 + i], r[4 + i], "grp", partner
                        ),
                    )
                )

        def start(self):
            for copy in self.near:
                copy.start()

        def forward(self):
            for copy, onward, pair in zip(self.near, self.far, self.pair):
                copy.wait_recv()
                onward.start()
                if pair:
                    pair[0].start()

        def beside(self):
            for pair in self.pair:
                if pair:
                    pair[1].wait_recv()

        def arrive(self):
            for copy in self.far:
                copy.wait_recv()

        def finish(self):
            for copy in self.near + self.far:
                copy.wait_send()
            for pair in self.pair:
                if pair:
                    pair[0].wait_send()

    def down_slot(base):
        def slot(s, rows):
            return wd_ref.at[pl.ds(pl.multiple_of(s * hid + base + rows.start, hid // 4), rows.size)]

        return slot

    gate_ring = Ring(0, gate_in, lambda s, rows: wg_ref.at[s, rows], True, True)
    up_ring = Ring(1, up_in, lambda s, rows: wu_ref.at[s, rows], True, True)
    down_rings = [
        Ring(2, down_in.at[pl.ds(0, hid // 2)], down_slot(0), True, False),
        Ring(3, down_in.at[pl.ds(hid // 2, hid // 2)], down_slot(hid // 2), False, True),
    ]
    normed_ring = Ring(4, normed_own, lambda s, rows: ngather.at[s, rows], False, False)
    weight_rings = (gate_ring, up_ring, *down_rings)
    for ring in weight_rings:
        ring.start()

    own_out = pltpu.make_async_copy(out_buf.at[ep], in_buf.at[ep], own_sem.at[0])
    own_out.start()
    own_normed = pltpu.make_async_copy(normed_own, ngather.at[0], own_sem.at[1])
    own_normed.start()

    for load in loads[:5]:
        load.wait()

    def mix(pair, carry):
        @pl.when(pair == pairs // 2)
        def _():
            gate_ring.forward()

        local_mixer(
            pair,
            q_ref,
            k_ref,
            v_ref,
            f_ref,
            a_ref,
            fb_ref,
            ab_ref,
            x_ref,
            omap_ref,
            oloc_ref,
            pay_ref,
        )
        return carry

    lax.fori_loop(0, pairs, mix, 0)

    def pay_out(h):
        return remote(
            pay_ref.at[h], arrived.at[ep], pay_send.at[h], pay_recv.at[ep], "ep", stride * h
        )

    def pay_in(e):
        return remote(pay_ref.at[0], arrived.at[e], pay_send.at[0], pay_recv.at[e], "ep", e)

    def others(act):
        for h in range(heads):
            pl.when(ep != stride * h)(functools.partial(act, h))

    others(lambda h: pay_out(h).start())
    own_pay = pltpu.make_async_copy(pay_ref.at[my_head], arrived.at[ep], own_sem.at[2])

    @pl.when(folds)
    def _():
        own_pay.start()

    for ring in weight_rings[1:]:
        ring.forward()
    normed_ring.start()

    own_out.wait()
    drain(inward, True)
    block_rows = 4 * experts
    at_row = iota((block_rows, 16 * experts), 0)
    at_col = iota((block_rows, 16 * experts), 1)
    for c in range(4):
        pick = (at_col == 16 * (at_row // 4) + 4 * c + at_row % 4).astype(F32).astype(BF16)
        for g in range(groups):
            block = in_buf[:, :, g * quarter_width : (g + 1) * quarter_width].reshape(
                16 * experts, quarter_width
            )
            xbuf[
                g * block_rows : (g + 1) * block_rows,
                c * quarter_width : (c + 1) * quarter_width,
            ] = dot(pick, block).astype(BF16)

    for load in loads[7:10]:
        load.wait()

    def hidden(s):
        rows = xbuf[...]
        return (jax.nn.silu(dot(rows, wg_ref[s])) * dot(rows, wu_ref[s])).astype(BF16)

    gate_ring.beside()
    up_ring.beside()
    for s in range(3):
        hbuf[:, s * hid : (s + 1) * hid] = hidden(s)
    for ring in down_rings:
        ring.beside()
    yacc[...] = dot(hbuf[...], wd_ref[: 3 * hid])

    for ring in weight_rings:
        ring.arrive()
    total = yacc[...] + dot(hidden(3), wd_ref[3 * hid :])
    yacc[...] = total
    at_row = iota((16 * experts, block_rows), 0)
    at_col = iota((16 * experts, block_rows), 1)
    put = jnp.concatenate(
        [
            (at_row == 16 * (at_col // 4) + 4 * c + at_col % 4).astype(F32).astype(BF16)
            for c in range(4)
        ],
        axis=1,
    )
    for g in range(groups):
        rows = yacc[g * block_rows : (g + 1) * block_rows, :].astype(BF16)
        rows = jnp.concatenate(
            [rows[:, c * quarter_width : (c + 1) * quarter_width] for c in range(4)], axis=0
        )
        ret_buf[:, :, g * quarter_width : (g + 1) * quarter_width] = (
            dot(put, rows).astype(BF16).reshape(experts, 16, quarter_width)
        )

    def ret_out(d):
        to = peer(d)
        return remote(ret_buf.at[to], back_buf.at[ep], ret_send.at[d], ret_recv.at[ep], "ep", to)

    def ret_in(d):
        e = peer(d)
        return remote(ret_buf.at[e], back_buf.at[e], ret_send.at[d], ret_recv.at[e], "ep", e)

    spray(ret_out, 0, experts // 8)
    def homeward(e):
        return remote(
            sent.at[e], states.at[my_head], home_send.at[e], home_recv.at[my_head], "ep", e
        )

    def home(h):
        return remote(sent.at[0], states.at[h], home_send.at[0], home_recv.at[h], "ep", stride * h)

    own_state = pltpu.make_async_copy(sent.at[ep], states.at[my_head], own_sem.at[3])

    def step(e, state):
        sent[e] = state

        @pl.when(e != ep)
        def _():
            pay_in(e).wait_recv()

        @pl.when((e > 0) & (e - 1 != ep))
        def _():
            homeward(e - 1).start()

        return fold_step(state, arrived[e])

    @pl.when(folds)
    def _():
        own_pay.wait()
        lax.fori_loop(0, experts, step, jnp.zeros(sent.shape[1:], F32))

        @pl.when(ep != experts - 1)
        def _():
            homeward(experts - 1).start()

        own_state.start()
        own_state.wait()

    spray(ret_out, experts // 8, experts // 2)
    own_ret = pltpu.make_async_copy(ret_buf.at[ep], back_buf.at[ep], own_sem.at[4])
    own_ret.start()

    normed_ring.forward()

    class Scatter:
        def __init__(self, index, part, relay, sums):
            n = part.shape[1]
            top, bottom = (pl.ds(0, n // 2), pl.ds(n // 2, n // 2))
            s = [rs_send.at[6 * index + i] for i in range(6)]
            r = [rs_recv.at[6 * index + i] for i in range(6)]
            self.part, self.sums = (part, sums)
            self.near = [
                remote(part.at[3, top], relay.at[0], s[0], r[0], "tp", right),
                remote(part.at[3, bottom], relay.at[1], s[1], r[1], "tp", left),
                remote(part.at[2], sums.at[1], s[2], r[2], "tp", right),
                remote(part.at[1], sums.at[2], s[3], r[3], "tp", left),
            ]
            self.far = [
                remote(relay.at[0], sums.at[3, top], s[4], r[4], "tp", right),
                remote(relay.at[1], sums.at[3, bottom], s[5], r[5], "tp", left),
            ]

        def start(self):
            for copy in self.near:
                copy.start()

        def forward(self):
            for copy, onward in zip(self.near[:2], self.far):
                copy.wait_recv()
                onward.start()

        def total(self):
            for copy in self.near[2:] + self.far:
                copy.wait_recv()
            out = self.part[0].astype(F32)
            for s in range(1, 4):
                out = out + self.sums[s].astype(F32)
            return out

        def finish(self):
            for copy in self.near + self.far:
                copy.wait_send()

    scatter_a = Scatter(0, part_a, relay_a, sums_a)
    scatter_b = Scatter(1, part_b, relay_b, sums_b)

    own_normed.wait()
    for load in loads[10:13]:
        load.wait()
    normed_ring.arrive()
    both = dot(ngather[...].reshape(tps * tokens, width), cgu_ref[...])
    inner = (jax.nn.silu(both[:, :half_lanes]) * both[:, half_lanes:]).astype(BF16)
    for s in range(4):
        part_b[s] = dot(inner[s * tokens : (s + 1) * tokens], cd_ref[...]).astype(BF16)
    scatter_b.start()

    others(lambda h: home(h).wait_recv())
    for load in loads[5:7]:
        load.wait()

    def finish(pair, carry):
        finish_mixer(pair, omap_ref, oloc_ref, states, g_ref, gain_ref, mixed_ref)
        return carry

    lax.fori_loop(0, pairs, finish, 0)
    mixer_rows = part_a.shape[1]
    for s, owner in enumerate((tp, left, right, across)):
        mine = pl.ds(pl.multiple_of(owner * mixer_rows, mixer_rows), mixer_rows)
        part_a[s] = dot(mixed_ref[mine, :], wout_ref[...]).astype(BF16)
    scatter_b.forward()
    scatter_a.start()
    scatter_a.forward()
    yacc[:tokens, :] = scatter_b.total()
    attend_ref[...] = scatter_a.total().astype(BF16)

    hits, quarter = slot_hits(ids_ref[...], experts, capacity)
    own_ret.wait()
    drain(ret_in, True)
    for c in range(4):
        block = yacc[:tokens, c * quarter_width : (c + 1) * quarter_width]
        for g in range(groups):
            weight = jnp.where(hits[g][0], mix_ref[0:1, :], 0.0) + jnp.where(
                hits[g][1], mix_ref[1:2, :], 0.0
            )
            weight = jnp.where(quarter == c, weight, 0.0)
            values = back_buf[:, :, g * quarter_width : (g + 1) * quarter_width].reshape(
                16 * experts, quarter_width
            )
            for part in split(weight, 2):
                block = block + dot_tn(part, values)
        moe_ref[:, c * quarter_width : (c + 1) * quarter_width] = block.astype(BF16)

    drain(outward, False)
    drain(ret_out, False)
    others(lambda h: pay_out(h).wait_send())

    def homegoing(d, carry):
        homeward(peer(d)).wait_send()
        return carry

    @pl.when(folds)
    def _():
        lax.fori_loop(1, experts, homegoing, 0)

    for item in weight_rings + (normed_ring, scatter_a, scatter_b):
        item.finish()


def on_device(
    query_vectors,
    attend_lookup_vectors,
    attend_content_vectors,
    forget_speed_dependent,
    amend_speed_dependent,
    result_switch_preactivation,
    feature_forget_baseline,
    amend_speed_baseline,
    sudden_forget_extra,
    group_scaling_factor,
    result_mapping_matrix,
    specialist_tokens_activations,
    specialist_scaling_factor,
    selected_specialists,
    selection_mixing_factors,
    dispatched_switch_matrix,
    dispatched_raising_matrix,
    dispatched_lowering_matrix,
    common_switch_matrix,
    common_raising_matrix,
    common_lowering_matrix,
):
    tokens, top_count = selected_specialists.shape
    width = specialist_tokens_activations.shape[1]
    rows, mix_width = query_vectors.shape
    groups = sudden_forget_extra.shape[1]
    lanes = 2 * (mix_width // groups)
    experts = lax.axis_size("ep")
    tps = lax.axis_size("tp")
    capacity = 3 * tokens * top_count // (2 * experts)
    hid = dispatched_switch_matrix.shape[2]
    shared = common_switch_matrix.shape[1]
    slab = (experts, 16, capacity * width // 16)
    vmem = pl.BlockSpec(memory_space=pltpu.VMEM)
    hbm = pl.BlockSpec(memory_space=pl.ANY)
    V = pltpu.VMEM
    dma = pltpu.SemaphoreType.DMA
    mixer_rows = rows // tps
    return pl.pallas_call(
        functools.partial(everything, capacity),
        in_specs=[hbm] * 6 + [vmem] * 4 + [hbm] + [vmem] * 4 + [hbm] * 6,
        out_specs=(vmem, vmem),
        out_shape=(
            jax.ShapeDtypeStruct((mixer_rows, width), BF16),
            jax.ShapeDtypeStruct((tokens, width), BF16),
        ),
        scratch_shapes=[V((rows, mix_width), BF16)] * 6
        + [
            V((mix_width, width), BF16),
            V((tps, width, hid), BF16),
            V((tps, width, hid), BF16),
            V((tps * hid, width), BF16),
            V((width, 2 * shared), BF16),
            V((shared, width), BF16),
            V((rows, mix_width), BF16),
            V((rows, mix_width), F32),
            V((groups, lanes // 2, lanes), BF16),
            V((experts, lanes // 2, lanes), BF16),
            V((experts, lanes // 4, lanes), F32),
            V((groups, lanes // 4, lanes), F32),
            V((rows, mix_width), BF16),
        ]
        + [V(slab, BF16)] * 4
        + [
            V((experts * capacity, width), BF16),
            V((experts * capacity, width), F32),
            V((experts * capacity, 3 * hid), BF16),
            V((tokens, width), BF16),
            V((tps, tokens, width), BF16),
            V((tps, mixer_rows, width), BF16),
            V((tps, tokens, width), BF16),
            V((2, mixer_rows // 2, width), BF16),
            V((2, tokens // 2, width), BF16),
            V((tps, mixer_rows, width), BF16),
            V((tps, tokens, width), BF16),
            dma((13,)),
            dma((5,)),
        ]
        + [dma((experts,))] * 8
        + [dma((30,)), dma((30,)), dma((12,)), dma((12,))],
        compiler_params=pltpu.CompilerParams(
            collective_id=0, has_side_effects=True, vmem_limit_bytes=62 * 1024 * 1024
        ),
        name="everything",
    )(
        query_vectors,
        attend_lookup_vectors,
        attend_content_vectors,
        forget_speed_dependent,
        amend_speed_dependent,
        result_switch_preactivation,
        feature_forget_baseline.reshape(1, -1),
        amend_speed_baseline.reshape(1, -1),
        sudden_forget_extra.T,
        group_scaling_factor.reshape(1, -1),
        result_mapping_matrix,
        specialist_tokens_activations,
        specialist_scaling_factor.reshape(1, -1),
        selected_specialists.T,
        selection_mixing_factors.T,
        dispatched_switch_matrix[0],
        dispatched_raising_matrix[0],
        dispatched_lowering_matrix[0],
        common_switch_matrix,
        common_raising_matrix,
        common_lowering_matrix,
    )


def solution(mesh):
    rows = P(("grp", "ep"), "tp")
    tokens = P(("grp", "ep", "tp"), None)
    placed = (
        (rows,) * 6
        + (P("tp"), P("tp"), rows, P("tp"), P("tp", None), tokens, P(), tokens, tokens)
        + (P("ep", None, "tp"), P("ep", None, "tp"), P("ep", "tp", None))
        + (P(None, "tp"), P(None, "tp"), P("tp", None))
    )
    return jax.shard_map(
        on_device, mesh=mesh, in_specs=placed, out_specs=(tokens, tokens), check_vma=False
    )
```

```python
import functools

import jax
import jax.numpy as jnp
from jax import lax
from jax.experimental import pallas as pl
from jax.experimental.pallas import tpu as pltpu
from jax.sharding import PartitionSpec as P

F32 = jnp.float32
BF16 = jnp.bfloat16
SPAN = 64
MESH = pl.DeviceIdType.MESH


def dot(a, b):
    return jnp.dot(a, b, preferred_element_type=F32)


def dot_nt(a, b):
    return lax.dot_general(a, b, (((1,), (1,)), ((), ())), preferred_element_type=F32)


def dot_tn(a, b):
    return lax.dot_general(a, b, (((0,), (0,)), ((), ())), preferred_element_type=F32)


def split(x, parts):
    out = []
    for _ in range(parts - 1):
        out.append(x.astype(BF16))
        x = x - out[-1].astype(F32)
    out.append(x.astype(BF16))
    return out


def iota(shape, dim):
    return lax.broadcasted_iota(jnp.int32, shape, dim)


def local_mixer(
    pair, q_ref, k_ref, v_ref, f_ref, a_ref, fb_ref, ab_ref, x_ref, omap_ref, oloc_ref, pay_ref
):
    rows = q_ref.shape[0]
    groups = x_ref.shape[0]
    half = q_ref.shape[1] // groups
    lanes = 2 * half
    spans = rows // SPAN
    here = pl.ds(pl.multiple_of(pair * lanes, lanes), lanes)
    low = iota((SPAN, lanes), 1) < half
    col = jnp.where(low, iota((SPAN, lanes), 1), iota((SPAN, lanes), 1) - half)
    row = iota((SPAN, lanes), 0)
    strict = row > col
    inclusive = row >= col
    tri = (iota((SPAN, SPAN), 0) >= iota((SPAN, SPAN), 1)).astype(BF16)
    tri3 = jnp.concatenate([tri] * 3, axis=1)
    same = ((iota((lanes, lanes), 0) < half) == (iota((lanes, lanes), 1) < half)).astype(BF16)
    same2 = jnp.concatenate([same] * 2, axis=0)
    spread = (
        iota((groups, lanes), 0) == 2 * pair + (iota((groups, lanes), 1) >= half).astype(jnp.int32)
    ).astype(F32)
    spread3 = jnp.concatenate([spread] * 3, axis=0).astype(BF16)
    below = iota((lanes, lanes), 0) < half
    left = iota((lanes, lanes), 1) < half

    def stack(x):
        return jnp.concatenate([jnp.where(low, x, 0.0), jnp.where(low, 0.0, x)], axis=0).astype(
            BF16
        )

    fb = fb_ref[:, here]
    ab = ab_ref[:, here]
    parts = [part.astype(F32) for part in split(x_ref[...], 3)]
    extra = dot_tn(jnp.concatenate(parts, axis=0).astype(BF16), spread3)

    spans_in = []
    for c in range(spans):
        at = slice(c * SPAN, (c + 1) * SPAN)
        decay = -jnp.exp(fb + f_ref[at, here].astype(F32)) + extra[at, :]
        rate = jax.nn.sigmoid(ab + a_ref[at, here].astype(F32))
        key = k_ref[at, here].astype(F32)
        sq = dot(jnp.concatenate(split(key * key, 2), axis=1), same2)
        unit = key * lax.rsqrt(sq + 1e-06)
        cum = dot(tri3, jnp.concatenate(split(decay, 3), axis=0))
        mid = cum[SPAN // 2 : SPAN // 2 + 1, :]
        last = cum[SPAN - 1 : SPAN, :]
        left_erase = -unit * jnp.exp(cum - decay - mid)
        left_read = q_ref[at, here].astype(F32) * jnp.exp(cum - mid)
        right = jnp.exp(mid - cum) * rate
        right_erase = unit * right
        right_write = key * right
        grow = jnp.exp(mid)
        tail = jnp.exp(last - mid)
        lefts = jnp.concatenate([left_erase, left_read], axis=0).astype(BF16)
        rights = jnp.concatenate([stack(right_erase), stack(right_write)], axis=0)
        pairs = dot_nt(lefts, rights)
        a_mat = jnp.where(strict, pairs[:SPAN, :lanes], 0.0)
        erase_write = jnp.where(strict, pairs[:SPAN, lanes:], 0.0)
        read_erase = jnp.where(inclusive, pairs[SPAN:, :lanes], 0.0)
        read_write = jnp.where(inclusive, pairs[SPAN:, lanes:], 0.0)
        value = v_ref[at, here].astype(F32)
        writes = dot(
            jnp.concatenate([erase_write, read_write], axis=0).astype(BF16), stack(value)
        )
        ends = jnp.concatenate([right_erase * tail, right_write * tail], axis=0).astype(BF16)
        spans_in.append(
            dict(
                a=a_mat,
                first=stack(left_erase * grow),
                read=left_read * grow,
                re=read_erase.astype(BF16),
                ew=stack(writes[:SPAN]),
                rw=writes[SPAN:],
                ends=ends,
                value=v_ref[at, here],
                last=jnp.exp(last),
            )
        )

    eye = (row == col).astype(F32)
    block = 1
    inverse = None
    while block < SPAN:
        in_block = (row // (2 * block) == col // (2 * block)) & (
            (row // block) % 2 == 1
        ) & ((col // block) % 2 == 0)
        steps = [jnp.where(in_block, s["a"], 0.0) for s in spans_in]
        if inverse is None:
            inverse = [eye + step for step in steps]
        else:
            inner = [
                dot(step.astype(BF16), stack(x)) for step, x in zip(steps, inverse)
            ]
            inverse = [x + dot(x.astype(BF16), stack(y)) for x, y in zip(inverse, inner)]
        block *= 2

    state = jnp.concatenate([eye, jnp.zeros_like(eye)], axis=0)
    for c, s in enumerate(spans_in):
        at = slice(c * SPAN, (c + 1) * SPAN)
        solved = dot(inverse[c].astype(BF16), jnp.concatenate([s["first"], s["ew"]], axis=1))
        w, y = (solved[:, :lanes], solved[:, lanes:])
        seen = dot(s["re"], jnp.concatenate([stack(w), stack(y)], axis=1))
        read = s["read"] + seen[:, :lanes]
        added = s["rw"] + seen[:, lanes:]
        value = s["value"]
        erased = dot_tn(w.astype(BF16), s["ends"][:SPAN])
        erased = jnp.where(below == left, erased, 0.0).astype(BF16)
        offset = dot_tn(jnp.concatenate([y.astype(BF16), value], axis=0), s["ends"])
        offset = jnp.where(low, offset[:half], offset[half:])
        both = jnp.concatenate([stack(state[:SPAN]), stack(state[SPAN:])], axis=0)
        reads = dot_nt(read.astype(BF16), both)
        omap_ref[at, here] = reads[:, :lanes].astype(BF16)
        oloc_ref[at, here] = added + reads[:, lanes:]
        state = (
            state * s["last"]
            + dot(state.astype(BF16), erased)
            + jnp.concatenate([jnp.zeros_like(offset), offset], axis=0)
        )
    jump, offset = (state[:SPAN], state[SPAN:])
    jump_turned = pltpu.roll(jump, half, 1)
    offset_turned = pltpu.roll(offset, half, 1)
    near = low[: SPAN // 2]
    for h in range(2):
        packed = [
            jnp.where(near, (x, turned)[h][: SPAN // 2], (turned, x)[h][SPAN // 2 :])
            for x, turned in ((jump, jump_turned), (offset, offset_turned))
        ]
        pay_ref[2 * pair + h] = jnp.concatenate(packed, axis=0).astype(BF16)


def fold_step(state, arrived):
    lanes = state.shape[1]
    half = lanes // 2
    low = iota(state.shape, 1) < half
    block = arrived.astype(F32)
    rows = state.shape[0]
    jump, offset = (block[:rows], block[rows:])
    turned = pltpu.roll(jump, half, 1)
    spread = jnp.concatenate(
        [
            jnp.where(low, jump, 0.0),
            jnp.where(low, turned, 0.0),
            jnp.where(low, 0.0, turned),
            jnp.where(low, 0.0, jump),
        ],
        axis=0,
    ).astype(BF16)
    parts = [part.astype(F32) for part in split(state, 2)]
    moved = dot(jnp.concatenate(parts, axis=0).astype(BF16), spread)
    return moved[:rows] + moved[rows:] + offset


def finish_mixer(pair, omap_ref, oloc_ref, state_ref, gate_ref, gain_ref, out_ref):
    lanes = state_ref.shape[2]
    half = lanes // 2
    here = pl.ds(pl.multiple_of(pair * lanes, lanes), lanes)
    low = iota(state_ref.shape[1:], 1) < half
    tiles = []
    for h in range(2):
        block = state_ref[2 * pair + h]
        turned = pltpu.roll(block, half, 1)
        if h == 0:
            tiles += [jnp.where(low, block, 0.0), jnp.where(low, turned, 0.0)]
        else:
            tiles += [jnp.where(low, 0.0, turned), jnp.where(low, 0.0, block)]
    state = jnp.concatenate(tiles, axis=0).astype(BF16)
    same = jnp.where(
        (iota((lanes, lanes), 0) < half) == (iota((lanes, lanes), 1) < half), 1.0 / half, 0.0
    ).astype(BF16)
    same2 = jnp.concatenate([same] * 2, axis=0)
    head_out = oloc_ref[:, here] + dot_nt(omap_ref[:, here], state)
    mean = dot(jnp.concatenate(split(head_out, 2), axis=1), same2)
    centered = head_out - mean
    var = dot(jnp.concatenate(split(centered * centered, 2), axis=1), same2)
    normed = centered * lax.rsqrt(var + 0.00064) * gain_ref[:, here]
    out_ref[:, here] = (normed * jax.nn.sigmoid(gate_ref[:, here].astype(F32))).astype(BF16)


def slot_hits(ids, experts, capacity):
    tokens = ids.shape[1]
    ids = ids.astype(F32)
    expert = iota((experts, tokens), 0).astype(F32)
    hot = [(expert == ids[j : j + 1]).astype(F32) for j in range(2)]
    earlier = (iota((tokens, tokens), 0) < iota((tokens, tokens), 1)).astype(F32).astype(BF16)
    before = dot((hot[0] + hot[1]).astype(BF16), earlier)
    place = [
        ids[j : j + 1] * capacity + jnp.sum(hot[j] * before, axis=0, keepdims=True)
        for j in range(2)
    ]
    at = iota((16 * experts, tokens), 0)
    base = (capacity * (at // 16) + at % 4).astype(F32)
    quarter = (at // 4) % 4
    groups = [[base + 4 * g == place[j] for j in range(2)] for g in range(capacity // 4)]
    return groups, quarter


def everything(
    capacity,
    q_in,
    k_in,
    v_in,
    f_in,
    a_in,
    g_in,
    fb_ref,
    ab_ref,
    x_ref,
    gain_ref,
    wout_in,
    tok_ref,
    scale_ref,
    ids_ref,
    mix_ref,
    gate_in,
    up_in,
    down_in,
    cgate_in,
    cup_in,
    cdown_in,
    attend_ref,
    moe_ref,
    q_ref,
    k_ref,
    v_ref,
    f_ref,
    a_ref,
    g_ref,
    wout_ref,
    wg_ref,
    wu_ref,
    wd_ref,
    cgu_ref,
    cd_ref,
    omap_ref,
    oloc_ref,
    pay_ref,
    arrived,
    sent,
    states,
    mixed_ref,
    out_buf,
    in_buf,
    ret_buf,
    back_buf,
    xbuf,
    yacc,
    hbuf,
    normed_own,
    ngather,
    part_a,
    part_b,
    relay_a,
    relay_b,
    sums_a,
    sums_b,
    load_sem,
    own_sem,
    out_send,
    out_recv,
    pay_send,
    pay_recv,
    home_send,
    home_recv,
    ret_send,
    ret_recv,
    ring_send,
    ring_recv,
    rs_send,
    rs_recv,
):
    experts = out_buf.shape[0]
    tps = ngather.shape[0]
    tokens, width = tok_ref.shape
    quarter_width = width // 4
    groups = capacity // 4
    pairs = omap_ref.shape[1] // sent.shape[2]
    ep = lax.axis_index("ep")
    tp = lax.axis_index("tp")
    right, left, across = (lax.rem(tp + 1, tps), lax.rem(tp + 3, tps), lax.rem(tp + 2, tps))
    paired = lax.axis_size("grp") % 2 == 0
    grp = lax.axis_index("grp")
    side = lax.rem(grp, 2)
    partner = grp + 1 - 2 * side
    heads = pay_ref.shape[0]
    stride = experts // heads
    my_head = ep // stride
    folds = lax.rem(ep, stride) == 0

    barrier = pltpu.get_barrier_semaphore()

    def greet(d, carry):
        pl.semaphore_signal(
            barrier, inc=1, device_id={"ep": lax.rem(ep + d, experts)}, device_id_type=MESH
        )
        return carry

    lax.fori_loop(1, experts, greet, 0)
    for near in (right, left):
        pl.semaphore_signal(barrier, inc=1, device_id={"tp": near}, device_id_type=MESH)
    if paired:
        pl.semaphore_signal(barrier, inc=1, device_id={"grp": partner}, device_id_type=MESH)

    half_lanes = cgate_in.shape[1]
    hid = gate_in.shape[1]
    loads = [
        pltpu.make_async_copy(a, b, load_sem.at[i])
        for i, (a, b) in enumerate(
            [
                (q_in, q_ref),
                (k_in, k_ref),
                (v_in, v_ref),
                (f_in, f_ref),
                (a_in, a_ref),
                (g_in, g_ref),
                (wout_in, wout_ref),
                (gate_in, wg_ref.at[0]),
                (up_in, wu_ref.at[0]),
                (down_in, wd_ref.at[pl.ds(0, hid)]),
                (cgate_in, cgu_ref.at[:, pl.ds(0, half_lanes)]),
                (cup_in, cgu_ref.at[:, pl.ds(half_lanes, half_lanes)]),
                (cdown_in, cd_ref),
            ]
        )
    ]
    for load in loads:
        load.start()

    def remote(src, dst, send, recv, axis, to):
        return pltpu.make_async_remote_copy(
            src_ref=src,
            dst_ref=dst,
            send_sem=send,
            recv_sem=recv,
            device_id={axis: to},
            device_id_type=MESH,
        )

    floats = tok_ref[...].astype(F32)
    normed = (
        floats
        * lax.rsqrt(jnp.mean(floats * floats, -1, keepdims=True) + 1e-06)
        * scale_ref[...]
    ).astype(BF16)
    normed_own[...] = normed
    hits, quarter = slot_hits(ids_ref[...], experts, capacity)
    stacked = jnp.concatenate(
        [normed[:, c * quarter_width : (c + 1) * quarter_width] for c in range(4)], axis=0
    )
    for g in range(groups):
        either = hits[g][0] | hits[g][1]
        placing = jnp.concatenate(
            [(either & (quarter == c)).astype(F32).astype(BF16) for c in range(4)], axis=1
        )
        out_buf[:, :, g * quarter_width : (g + 1) * quarter_width] = (
            dot(placing, stacked).astype(BF16).reshape(experts, 16, quarter_width)
        )

    pl.semaphore_wait(barrier, experts - 1 + 2 + int(paired))

    def peer(d):
        return lax.rem(ep + d, experts)

    def outward(d):
        to = peer(d)
        return remote(out_buf.at[to], in_buf.at[ep], out_send.at[d], out_recv.at[ep], "ep", to)

    def inward(d):
        e = peer(d)
        return remote(out_buf.at[e], in_buf.at[e], out_send.at[d], out_recv.at[e], "ep", e)

    def spray(make, first, last):
        def go(i, carry):
            d = experts // 2 - i
            make(d).start()
            make(experts - d).start()
            return carry

        if first == 0:
            make(experts // 2).start()
        lax.fori_loop(max(first, 1), last, go, 0)

    def drain(make, recv):
        def go(d, carry):
            if recv:
                make(d).wait_recv()
            else:
                make(d).wait_send()
            return carry

        lax.fori_loop(1, experts, go, 0)

    early = 3 * experts // 16
    spray(outward, 0, early)

    class Ring:
        def __init__(self, index, own, slot, pair_left, pair_right):
            n = own.shape[0]
            mine = pl.ds(pl.multiple_of(side * (n // 2), n // 2), n // 2)
            other = pl.ds(pl.multiple_of((1 - side) * (n // 2), n // 2), n // 2)
            whole = pl.ds(0, n)
            s = [ring_send.at[6 * index + i] for i in range(6)]
            r = [ring_recv.at[6 * index + i] for i in range(6)]
            self.near, self.far, self.pair, self.paired_in = ([], [], [], [])
            for i, (to, half, rest, pair) in enumerate(
                [
                    (right, mine, other, paired and pair_left),
                    (left, other, mine, paired and pair_right),
                ]
            ):
                part = half if pair else whole
                self.near.append(
                    remote(own.at[part], slot(i + 1, part), s[i], r[i], "tp", to)
                )
                self.far.append(
                    remote(slot(i + 1, half), slot(3, half), s[2 + i], r[2 + i], "tp", to)
                )
                self.pair.append(
                    pair
                    and (
                        remote(
                            slot(i + 1, half), slot(i + 1, half), s[4 + i], r[4 + i], "grp", partner
                        ),
                        remote(
                            slot(i + 1, rest), slot(i + 1, rest), s[4 + i], r[4 + i], "grp", partner
                        ),
                    )
                )

        def start(self):
            for copy in self.near:
                copy.start()

        def forward(self):
            for copy, onward, pair in zip(self.near, self.far, self.pair):
                copy.wait_recv()
                onward.start()
                if pair:
                    pair[0].start()

        def beside(self):
            for pair in self.pair:
                if pair:
                    pair[1].wait_recv()

        def arrive(self):
            for copy in self.far:
                copy.wait_recv()

        def finish(self):
            for copy in self.near + self.far:
                copy.wait_send()
            for pair in self.pair:
                if pair:
                    pair[0].wait_send()

    def down_slot(base):
        def slot(s, rows):
            return wd_ref.at[pl.ds(pl.multiple_of(s * hid + base + rows.start, hid // 4), rows.size)]

        return slot

    gate_ring = Ring(0, gate_in, lambda s, rows: wg_ref.at[s, rows], True, True)
    up_ring = Ring(1, up_in, lambda s, rows: wu_ref.at[s, rows], True, True)
    down_rings = [
        Ring(2, down_in.at[pl.ds(0, hid // 2)], down_slot(0), True, False),
        Ring(3, down_in.at[pl.ds(hid // 2, hid // 2)], down_slot(hid // 2), False, True),
    ]
    normed_ring = Ring(4, normed_own, lambda s, rows: ngather.at[s, rows], False, False)
    weight_rings = (gate_ring, up_ring, *down_rings)
    for ring in weight_rings:
        ring.start()

    own_out = pltpu.make_async_copy(out_buf.at[ep], in_buf.at[ep], own_sem.at[0])
    own_out.start()
    own_normed = pltpu.make_async_copy(normed_own, ngather.at[0], own_sem.at[1])
    own_normed.start()

    for load in loads[:5]:
        load.wait()

    def mix(pair, carry):
        @pl.when(pair == pairs // 2)
        def _():
            gate_ring.forward()

        local_mixer(
            pair,
            q_ref,
            k_ref,
            v_ref,
            f_ref,
            a_ref,
            fb_ref,
            ab_ref,
            x_ref,
            omap_ref,
            oloc_ref,
            pay_ref,
        )
        return carry

    lax.fori_loop(0, pairs, mix, 0)

    def pay_out(h):
        return remote(
            pay_ref.at[h], arrived.at[ep], pay_send.at[h], pay_recv.at[ep], "ep", stride * h
        )

    def pay_in(e):
        return remote(pay_ref.at[0], arrived.at[e], pay_send.at[0], pay_recv.at[e], "ep", e)

    def others(act):
        for h in range(heads):
            pl.when(ep != stride * h)(functools.partial(act, h))

    others(lambda h: pay_out(h).start())
    own_pay = pltpu.make_async_copy(pay_ref.at[my_head], arrived.at[ep], own_sem.at[2])

    @pl.when(folds)
    def _():
        own_pay.start()

    spray(outward, early, experts // 2)
    for ring in weight_rings[1:]:
        ring.forward()
    normed_ring.start()

    def homeward(e):
        return remote(
            sent.at[e], states.at[my_head], home_send.at[e], home_recv.at[my_head], "ep", e
        )

    def home(h):
        return remote(sent.at[0], states.at[h], home_send.at[0], home_recv.at[h], "ep", stride * h)

    own_state = pltpu.make_async_copy(sent.at[ep], states.at[my_head], own_sem.at[3])

    def step(e, state):
        sent[e] = state

        @pl.when(e != ep)
        def _():
            pay_in(e).wait_recv()

        @pl.when((e > 0) & (e - 1 != ep))
        def _():
            homeward(e - 1).start()

        return fold_step(state, arrived[e])

    @pl.when(folds)
    def _():
        own_pay.wait()
        lax.fori_loop(0, experts, step, jnp.zeros(sent.shape[1:], F32))

        @pl.when(ep != experts - 1)
        def _():
            homeward(experts - 1).start()

        own_state.start()
        own_state.wait()

    own_out.wait()
    drain(inward, True)
    block_rows = 4 * experts
    at_row = iota((block_rows, 16 * experts), 0)
    at_col = iota((block_rows, 16 * experts), 1)
    for c in range(4):
        pick = (at_col == 16 * (at_row // 4) + 4 * c + at_row % 4).astype(F32).astype(BF16)
        for g in range(groups):
            block = in_buf[:, :, g * quarter_width : (g + 1) * quarter_width].reshape(
                16 * experts, quarter_width
            )
            xbuf[
                g * block_rows : (g + 1) * block_rows,
                c * quarter_width : (c + 1) * quarter_width,
            ] = dot(pick, block).astype(BF16)

    for load in loads[7:10]:
        load.wait()

    def hidden(s):
        rows = xbuf[...]
        return (jax.nn.silu(dot(rows, wg_ref[s])) * dot(rows, wu_ref[s])).astype(BF16)

    gate_ring.beside()
    up_ring.beside()
    for s in range(3):
        hbuf[:, s * hid : (s + 1) * hid] = hidden(s)
    for ring in down_rings:
        ring.beside()
    yacc[...] = dot(hbuf[...], wd_ref[: 3 * hid])

    for ring in weight_rings:
        ring.arrive()
    total = yacc[...] + dot(hidden(3), wd_ref[3 * hid :])
    yacc[...] = total
    at_row = iota((16 * experts, block_rows), 0)
    at_col = iota((16 * experts, block_rows), 1)
    put = jnp.concatenate(
        [
            (at_row == 16 * (at_col // 4) + 4 * c + at_col % 4).astype(F32).astype(BF16)
            for c in range(4)
        ],
        axis=1,
    )
    for g in range(groups):
        rows = yacc[g * block_rows : (g + 1) * block_rows, :].astype(BF16)
        rows = jnp.concatenate(
            [rows[:, c * quarter_width : (c + 1) * quarter_width] for c in range(4)], axis=0
        )
        ret_buf[:, :, g * quarter_width : (g + 1) * quarter_width] = (
            dot(put, rows).astype(BF16).reshape(experts, 16, quarter_width)
        )

    def ret_out(d):
        to = peer(d)
        return remote(ret_buf.at[to], back_buf.at[ep], ret_send.at[d], ret_recv.at[ep], "ep", to)

    def ret_in(d):
        e = peer(d)
        return remote(ret_buf.at[e], back_buf.at[e], ret_send.at[d], ret_recv.at[e], "ep", e)

    spray(ret_out, 0, experts // 2)
    own_ret = pltpu.make_async_copy(ret_buf.at[ep], back_buf.at[ep], own_sem.at[4])
    own_ret.start()

    class Scatter:
        def __init__(self, index, part, relay, sums):
            n = part.shape[1]
            top, bottom = (pl.ds(0, n // 2), pl.ds(n // 2, n // 2))
            s = [rs_send.at[6 * index + i] for i in range(6)]
            r = [rs_recv.at[6 * index + i] for i in range(6)]
            self.part, self.sums = (part, sums)
            self.near = [
                remote(part.at[3, top], relay.at[0], s[0], r[0], "tp", right),
                remote(part.at[3, bottom], relay.at[1], s[1], r[1], "tp", left),
                remote(part.at[2], sums.at[1], s[2], r[2], "tp", right),
                remote(part.at[1], sums.at[2], s[3], r[3], "tp", left),
            ]
            self.far = [
                remote(relay.at[0], sums.at[3, top], s[4], r[4], "tp", right),
                remote(relay.at[1], sums.at[3, bottom], s[5], r[5], "tp", left),
            ]

        def start(self):
            for copy in self.near:
                copy.start()

        def forward(self):
            for copy, onward in zip(self.near[:2], self.far):
                copy.wait_recv()
                onward.start()

        def total(self):
            for copy in self.near[2:] + self.far:
                copy.wait_recv()
            out = self.part[0].astype(F32)
            for s in range(1, 4):
                out = out + self.sums[s].astype(F32)
            return out

        def finish(self):
            for copy in self.near + self.far:
                copy.wait_send()

    scatter_a = Scatter(0, part_a, relay_a, sums_a)
    scatter_b = Scatter(1, part_b, relay_b, sums_b)

    others(lambda h: home(h).wait_recv())
    for load in loads[5:7]:
        load.wait()

    def finish(pair, carry):
        finish_mixer(pair, omap_ref, oloc_ref, states, g_ref, gain_ref, mixed_ref)
        return carry

    lax.fori_loop(0, pairs, finish, 0)
    mixer_rows = part_a.shape[1]
    for s, owner in enumerate((tp, left, right, across)):
        mine = pl.ds(pl.multiple_of(owner * mixer_rows, mixer_rows), mixer_rows)
        part_a[s] = dot(mixed_ref[mine, :], wout_ref[...]).astype(BF16)
    normed_ring.forward()
    scatter_a.start()

    own_normed.wait()
    for load in loads[10:13]:
        load.wait()
    normed_ring.arrive()
    scatter_a.forward()
    both = dot(ngather[...].reshape(tps * tokens, width), cgu_ref[...])
    inner = (jax.nn.silu(both[:, :half_lanes]) * both[:, half_lanes:]).astype(BF16)
    for s in range(4):
        part_b[s] = dot(inner[s * tokens : (s + 1) * tokens], cd_ref[...]).astype(BF16)
    scatter_b.start()
    scatter_b.forward()
    attend_ref[...] = scatter_a.total().astype(BF16)
    yacc[:tokens, :] = scatter_b.total()

    hits, quarter = slot_hits(ids_ref[...], experts, capacity)
    own_ret.wait()
    drain(ret_in, True)
    for c in range(4):
        block = yacc[:tokens, c * quarter_width : (c + 1) * quarter_width]
        for g in range(groups):
            weight = jnp.where(hits[g][0], mix_ref[0:1, :], 0.0) + jnp.where(
                hits[g][1], mix_ref[1:2, :], 0.0
            )
            weight = jnp.where(quarter == c, weight, 0.0)
            values = back_buf[:, :, g * quarter_width : (g + 1) * quarter_width].reshape(
                16 * experts, quarter_width
            )
            for part in split(weight, 2):
                block = block + dot_tn(part, values)
        moe_ref[:, c * quarter_width : (c + 1) * quarter_width] = block.astype(BF16)

    drain(outward, False)
    drain(ret_out, False)
    others(lambda h: pay_out(h).wait_send())

    def homegoing(d, carry):
        homeward(peer(d)).wait_send()
        return carry

    @pl.when(folds)
    def _():
        lax.fori_loop(1, experts, homegoing, 0)

    for item in weight_rings + (normed_ring, scatter_a, scatter_b):
        item.finish()


def on_device(
    query_vectors,
    attend_lookup_vectors,
    attend_content_vectors,
    forget_speed_dependent,
    amend_speed_dependent,
    result_switch_preactivation,
    feature_forget_baseline,
    amend_speed_baseline,
    sudden_forget_extra,
    group_scaling_factor,
    result_mapping_matrix,
    specialist_tokens_activations,
    specialist_scaling_factor,
    selected_specialists,
    selection_mixing_factors,
    dispatched_switch_matrix,
    dispatched_raising_matrix,
    dispatched_lowering_matrix,
    common_switch_matrix,
    common_raising_matrix,
    common_lowering_matrix,
):
    tokens, top_count = selected_specialists.shape
    width = specialist_tokens_activations.shape[1]
    rows, mix_width = query_vectors.shape
    groups = sudden_forget_extra.shape[1]
    lanes = 2 * (mix_width // groups)
    experts = lax.axis_size("ep")
    tps = lax.axis_size("tp")
    capacity = 3 * tokens * top_count // (2 * experts)
    hid = dispatched_switch_matrix.shape[2]
    shared = common_switch_matrix.shape[1]
    slab = (experts, 16, capacity * width // 16)
    vmem = pl.BlockSpec(memory_space=pltpu.VMEM)
    hbm = pl.BlockSpec(memory_space=pl.ANY)
    V = pltpu.VMEM
    dma = pltpu.SemaphoreType.DMA
    mixer_rows = rows // tps
    return pl.pallas_call(
        functools.partial(everything, capacity),
        in_specs=[hbm] * 6 + [vmem] * 4 + [hbm] + [vmem] * 4 + [hbm] * 6,
        out_specs=(vmem, vmem),
        out_shape=(
            jax.ShapeDtypeStruct((mixer_rows, width), BF16),
            jax.ShapeDtypeStruct((tokens, width), BF16),
        ),
        scratch_shapes=[V((rows, mix_width), BF16)] * 6
        + [
            V((mix_width, width), BF16),
            V((tps, width, hid), BF16),
            V((tps, width, hid), BF16),
            V((tps * hid, width), BF16),
            V((width, 2 * shared), BF16),
            V((shared, width), BF16),
            V((rows, mix_width), BF16),
            V((rows, mix_width), F32),
            V((groups, lanes // 2, lanes), BF16),
            V((experts, lanes // 2, lanes), BF16),
            V((experts, lanes // 4, lanes), F32),
            V((groups, lanes // 4, lanes), F32),
            V((rows, mix_width), BF16),
        ]
        + [V(slab, BF16)] * 4
        + [
            V((experts * capacity, width), BF16),
            V((experts * capacity, width), F32),
            V((experts * capacity, 3 * hid), BF16),
            V((tokens, width), BF16),
            V((tps, tokens, width), BF16),
            V((tps, mixer_rows, width), BF16),
            V((tps, tokens, width), BF16),
            V((2, mixer_rows // 2, width), BF16),
            V((2, tokens // 2, width), BF16),
            V((tps, mixer_rows, width), BF16),
            V((tps, tokens, width), BF16),
            dma((13,)),
            dma((5,)),
        ]
        + [dma((experts,))] * 8
        + [dma((30,)), dma((30,)), dma((12,)), dma((12,))],
        compiler_params=pltpu.CompilerParams(
            collective_id=0, has_side_effects=True, vmem_limit_bytes=52 * 1024 * 1024
        ),
        name="everything",
    )(
        query_vectors,
        attend_lookup_vectors,
        attend_content_vectors,
        forget_speed_dependent,
        amend_speed_dependent,
        result_switch_preactivation,
        feature_forget_baseline.reshape(1, -1),
        amend_speed_baseline.reshape(1, -1),
        sudden_forget_extra.T,
        group_scaling_factor.reshape(1, -1),
        result_mapping_matrix,
        specialist_tokens_activations,
        specialist_scaling_factor.reshape(1, -1),
        selected_specialists.T,
        selection_mixing_factors.T,
        dispatched_switch_matrix[0],
        dispatched_raising_matrix[0],
        dispatched_lowering_matrix[0],
        common_switch_matrix,
        common_raising_matrix,
        common_lowering_matrix,
    )


def solution(mesh):
    rows = P(("grp", "ep"), "tp")
    tokens = P(("grp", "ep", "tp"), None)
    placed = (
        (rows,) * 6
        + (P("tp"), P("tp"), rows, P("tp"), P("tp", None), tokens, P(), tokens, tokens)
        + (P("ep", None, "tp"), P("ep", None, "tp"), P("ep", "tp", None))
        + (P(None, "tp"), P(None, "tp"), P("tp", None))
    )
    return jax.shard_map(
        on_device, mesh=mesh, in_specs=placed, out_specs=(tokens, tokens), check_vma=False
    )
```

```python
import functools

import jax
import jax.numpy as jnp
from jax import lax
from jax.experimental import pallas as pl
from jax.experimental.pallas import tpu as pltpu
from jax.sharding import PartitionSpec as P

F32 = jnp.float32
BF16 = jnp.bfloat16
SPAN = 64
MESH = pl.DeviceIdType.MESH


def dot(a, b):
    return jnp.dot(a, b, preferred_element_type=F32)


def dot_nt(a, b):
    return lax.dot_general(a, b, (((1,), (1,)), ((), ())), preferred_element_type=F32)


def dot_tn(a, b):
    return lax.dot_general(a, b, (((0,), (0,)), ((), ())), preferred_element_type=F32)


def split(x, parts):
    out = []
    for _ in range(parts - 1):
        out.append(x.astype(BF16))
        x = x - out[-1].astype(F32)
    out.append(x.astype(BF16))
    return out


def iota(shape, dim):
    return lax.broadcasted_iota(jnp.int32, shape, dim)


def local_mixer(
    pair, q_ref, k_ref, v_ref, f_ref, a_ref, fb_ref, ab_ref, x_ref, omap_ref, oloc_ref, pay_ref
):
    rows = q_ref.shape[0]
    groups = x_ref.shape[0]
    half = q_ref.shape[1] // groups
    lanes = 2 * half
    spans = rows // SPAN
    here = pl.ds(pl.multiple_of(pair * lanes, lanes), lanes)
    low = iota((SPAN, lanes), 1) < half
    col = jnp.where(low, iota((SPAN, lanes), 1), iota((SPAN, lanes), 1) - half)
    row = iota((SPAN, lanes), 0)
    strict = row > col
    inclusive = row >= col
    tri = (iota((SPAN, SPAN), 0) >= iota((SPAN, SPAN), 1)).astype(BF16)
    tri3 = jnp.concatenate([tri] * 3, axis=1)
    same = ((iota((lanes, lanes), 0) < half) == (iota((lanes, lanes), 1) < half)).astype(BF16)
    same2 = jnp.concatenate([same] * 2, axis=0)
    spread = (
        iota((groups, lanes), 0) == 2 * pair + (iota((groups, lanes), 1) >= half).astype(jnp.int32)
    ).astype(F32)
    spread3 = jnp.concatenate([spread] * 3, axis=0).astype(BF16)
    below = iota((lanes, lanes), 0) < half
    left = iota((lanes, lanes), 1) < half

    def stack(x):
        return jnp.concatenate([jnp.where(low, x, 0.0), jnp.where(low, 0.0, x)], axis=0).astype(
            BF16
        )

    fb = fb_ref[:, here]
    ab = ab_ref[:, here]
    parts = [part.astype(F32) for part in split(x_ref[...], 3)]
    extra = dot_tn(jnp.concatenate(parts, axis=0).astype(BF16), spread3)

    spans_in = []
    for c in range(spans):
        at = slice(c * SPAN, (c + 1) * SPAN)
        decay = -jnp.exp(fb + f_ref[at, here].astype(F32)) + extra[at, :]
        rate = jax.nn.sigmoid(ab + a_ref[at, here].astype(F32))
        key = k_ref[at, here].astype(F32)
        sq = dot(jnp.concatenate(split(key * key, 2), axis=1), same2)
        unit = key * lax.rsqrt(sq + 1e-06)
        cum = dot(tri3, jnp.concatenate(split(decay, 3), axis=0))
        mid = cum[SPAN // 2 : SPAN // 2 + 1, :]
        last = cum[SPAN - 1 : SPAN, :]
        left_erase = -unit * jnp.exp(cum - decay - mid)
        left_read = q_ref[at, here].astype(F32) * jnp.exp(cum - mid)
        right = jnp.exp(mid - cum) * rate
        right_erase = unit * right
        right_write = key * right
        grow = jnp.exp(mid)
        tail = jnp.exp(last - mid)
        lefts = jnp.concatenate([left_erase, left_read], axis=0).astype(BF16)
        rights = jnp.concatenate([stack(right_erase), stack(right_write)], axis=0)
        pairs = dot_nt(lefts, rights)
        a_mat = jnp.where(strict, pairs[:SPAN, :lanes], 0.0)
        erase_write = jnp.where(strict, pairs[:SPAN, lanes:], 0.0)
        read_erase = jnp.where(inclusive, pairs[SPAN:, :lanes], 0.0)
        read_write = jnp.where(inclusive, pairs[SPAN:, lanes:], 0.0)
        value = v_ref[at, here].astype(F32)
        writes = dot(
            jnp.concatenate([erase_write, read_write], axis=0).astype(BF16), stack(value)
        )
        ends = jnp.concatenate([right_erase * tail, right_write * tail], axis=0).astype(BF16)
        spans_in.append(
            dict(
                a=a_mat,
                first=stack(left_erase * grow),
                read=left_read * grow,
                re=read_erase.astype(BF16),
                ew=stack(writes[:SPAN]),
                rw=writes[SPAN:],
                ends=ends,
                value=v_ref[at, here],
                last=jnp.exp(last),
            )
        )

    eye = (row == col).astype(F32)
    block = 1
    inverse = None
    while block < SPAN:
        in_block = (row // (2 * block) == col // (2 * block)) & (
            (row // block) % 2 == 1
        ) & ((col // block) % 2 == 0)
        steps = [jnp.where(in_block, s["a"], 0.0) for s in spans_in]
        if inverse is None:
            inverse = [eye + step for step in steps]
        else:
            inner = [
                dot(step.astype(BF16), stack(x)) for step, x in zip(steps, inverse)
            ]
            inverse = [x + dot(x.astype(BF16), stack(y)) for x, y in zip(inverse, inner)]
        block *= 2

    state = jnp.concatenate([eye, jnp.zeros_like(eye)], axis=0)
    for c, s in enumerate(spans_in):
        at = slice(c * SPAN, (c + 1) * SPAN)
        solved = dot(inverse[c].astype(BF16), jnp.concatenate([s["first"], s["ew"]], axis=1))
        w, y = (solved[:, :lanes], solved[:, lanes:])
        seen = dot(s["re"], jnp.concatenate([stack(w), stack(y)], axis=1))
        read = s["read"] + seen[:, :lanes]
        added = s["rw"] + seen[:, lanes:]
        value = s["value"]
        erased = dot_tn(w.astype(BF16), s["ends"][:SPAN])
        erased = jnp.where(below == left, erased, 0.0).astype(BF16)
        offset = dot_tn(jnp.concatenate([y.astype(BF16), value], axis=0), s["ends"])
        offset = jnp.where(low, offset[:half], offset[half:])
        both = jnp.concatenate([stack(state[:SPAN]), stack(state[SPAN:])], axis=0)
        reads = dot_nt(read.astype(BF16), both)
        omap_ref[at, here] = reads[:, :lanes].astype(BF16)
        oloc_ref[at, here] = added + reads[:, lanes:]
        state = (
            state * s["last"]
            + dot(state.astype(BF16), erased)
            + jnp.concatenate([jnp.zeros_like(offset), offset], axis=0)
        )
    jump, offset = (state[:SPAN], state[SPAN:])
    jump_turned = pltpu.roll(jump, half, 1)
    offset_turned = pltpu.roll(offset, half, 1)
    near = low[: SPAN // 2]
    for h in range(2):
        packed = [
            jnp.where(near, (x, turned)[h][: SPAN // 2], (turned, x)[h][SPAN // 2 :])
            for x, turned in ((jump, jump_turned), (offset, offset_turned))
        ]
        pay_ref[2 * pair + h] = jnp.concatenate(packed, axis=0).astype(BF16)


def fold_step(state, arrived):
    lanes = state.shape[1]
    half = lanes // 2
    low = iota(state.shape, 1) < half
    block = arrived.astype(F32)
    rows = state.shape[0]
    jump, offset = (block[:rows], block[rows:])
    turned = pltpu.roll(jump, half, 1)
    spread = jnp.concatenate(
        [
            jnp.where(low, jump, 0.0),
            jnp.where(low, turned, 0.0),
            jnp.where(low, 0.0, turned),
            jnp.where(low, 0.0, jump),
        ],
        axis=0,
    ).astype(BF16)
    parts = [part.astype(F32) for part in split(state, 2)]
    moved = dot(jnp.concatenate(parts, axis=0).astype(BF16), spread)
    return moved[:rows] + moved[rows:] + offset


def finish_mixer(pair, omap_ref, oloc_ref, state_ref, gate_ref, gain_ref, out_ref):
    lanes = state_ref.shape[2]
    half = lanes // 2
    here = pl.ds(pl.multiple_of(pair * lanes, lanes), lanes)
    low = iota(state_ref.shape[1:], 1) < half
    tiles = []
    for h in range(2):
        block = state_ref[2 * pair + h].astype(F32)
        turned = pltpu.roll(block, half, 1)
        if h == 0:
            tiles += [jnp.where(low, block, 0.0), jnp.where(low, turned, 0.0)]
        else:
            tiles += [jnp.where(low, 0.0, turned), jnp.where(low, 0.0, block)]
    state = jnp.concatenate(tiles, axis=0).astype(BF16)
    same = jnp.where(
        (iota((lanes, lanes), 0) < half) == (iota((lanes, lanes), 1) < half), 1.0 / half, 0.0
    ).astype(BF16)
    same2 = jnp.concatenate([same] * 2, axis=0)
    head_out = oloc_ref[:, here] + dot_nt(omap_ref[:, here], state)
    mean = dot(jnp.concatenate(split(head_out, 2), axis=1), same2)
    centered = head_out - mean
    var = dot(jnp.concatenate(split(centered * centered, 2), axis=1), same2)
    normed = centered * lax.rsqrt(var + 0.00064) * gain_ref[:, here]
    out_ref[:, here] = (normed * jax.nn.sigmoid(gate_ref[:, here].astype(F32))).astype(BF16)


def slot_hits(ids, experts, capacity):
    tokens = ids.shape[1]
    ids = ids.astype(F32)
    expert = iota((experts, tokens), 0).astype(F32)
    hot = [(expert == ids[j : j + 1]).astype(F32) for j in range(2)]
    earlier = (iota((tokens, tokens), 0) < iota((tokens, tokens), 1)).astype(F32).astype(BF16)
    before = dot((hot[0] + hot[1]).astype(BF16), earlier)
    place = [
        ids[j : j + 1] * capacity + jnp.sum(hot[j] * before, axis=0, keepdims=True)
        for j in range(2)
    ]
    at = iota((16 * experts, tokens), 0)
    base = (capacity * (at // 16) + at % 4).astype(F32)
    quarter = (at // 4) % 4
    groups = [[base + 4 * g == place[j] for j in range(2)] for g in range(capacity // 4)]
    return groups, quarter


def everything(
    capacity,
    q_in,
    k_in,
    v_in,
    f_in,
    a_in,
    g_in,
    fb_in,
    ab_in,
    x_in,
    gain_in,
    wout_in,
    tok_in,
    scale_in,
    ids_in,
    mix_in,
    gate_in,
    up_in,
    down_in,
    cgate_in,
    cup_in,
    cdown_in,
    attend_ref,
    moe_ref,
    q_ref,
    k_ref,
    v_ref,
    f_ref,
    a_ref,
    g_ref,
    wout_ref,
    wg_ref,
    wu_ref,
    wd_ref,
    cgu_ref,
    cd_ref,
    omap_ref,
    oloc_ref,
    pay_ref,
    arrived,
    sent,
    states,
    mixed_ref,
    out_buf,
    in_buf,
    ret_buf,
    back_buf,
    xbuf,
    yacc,
    hbuf,
    normed_own,
    ngather,
    part_a,
    part_b,
    relay_a,
    relay_b,
    sums_a,
    sums_b,
    tok_ref,
    scale_ref,
    ids_ref,
    fb_ref,
    ab_ref,
    x_ref,
    gain_ref,
    mix_ref,
    load_sem,
    own_sem,
    out_send,
    out_recv,
    pay_send,
    pay_recv,
    home_send,
    home_recv,
    ret_send,
    ret_recv,
    ring_send,
    ring_recv,
    rs_send,
    rs_recv,
):
    experts = out_buf.shape[0]
    tps = ngather.shape[0]
    tokens, width = tok_ref.shape
    quarter_width = width // 4
    groups = capacity // 4
    pairs = omap_ref.shape[1] // sent.shape[2]
    ep = lax.axis_index("ep")
    tp = lax.axis_index("tp")
    right, left, across = (lax.rem(tp + 1, tps), lax.rem(tp + 3, tps), lax.rem(tp + 2, tps))
    paired = lax.axis_size("grp") % 2 == 0
    grp = lax.axis_index("grp")
    side = lax.rem(grp, 2)
    partner = grp + 1 - 2 * side
    heads = pay_ref.shape[0]
    stride = experts // heads
    my_head = ep // stride
    folds = lax.rem(ep, stride) == 0

    barrier = pltpu.get_barrier_semaphore()

    def greet(d, carry):
        pl.semaphore_signal(
            barrier, inc=1, device_id={"ep": lax.rem(ep + d, experts)}, device_id_type=MESH
        )
        return carry

    lax.fori_loop(1, experts, greet, 0)
    for near in (right, left):
        pl.semaphore_signal(barrier, inc=1, device_id={"tp": near}, device_id_type=MESH)
    if paired:
        pl.semaphore_signal(barrier, inc=1, device_id={"grp": partner}, device_id_type=MESH)

    half_lanes = cgate_in.shape[1]
    hid = gate_in.shape[1]
    loads = [
        pltpu.make_async_copy(a, b, load_sem.at[i])
        for i, (a, b) in enumerate(
            [
                (q_in, q_ref),
                (k_in, k_ref),
                (v_in, v_ref),
                (f_in, f_ref),
                (a_in, a_ref),
                (g_in, g_ref),
                (wout_in, wout_ref),
                (gate_in, wg_ref.at[0]),
                (up_in, wu_ref.at[0]),
                (down_in, wd_ref.at[pl.ds(0, hid)]),
                (cgate_in, cgu_ref.at[:, pl.ds(0, half_lanes)]),
                (cup_in, cgu_ref.at[:, pl.ds(half_lanes, half_lanes)]),
                (cdown_in, cd_ref),
                (tok_in, tok_ref),
                (scale_in, scale_ref),
                (ids_in, ids_ref),
                (fb_in, fb_ref),
                (ab_in, ab_ref),
                (x_in, x_ref),
                (gain_in, gain_ref),
                (mix_in, mix_ref),
            ]
        )
    ]
    for load in loads[13:] + loads[:13]:
        load.start()

    def remote(src, dst, send, recv, axis, to):
        return pltpu.make_async_remote_copy(
            src_ref=src,
            dst_ref=dst,
            send_sem=send,
            recv_sem=recv,
            device_id={axis: to},
            device_id_type=MESH,
        )

    for load in loads[13:16]:
        load.wait()
    floats = tok_ref[...].astype(F32)
    normed = (
        floats
        * lax.rsqrt(jnp.mean(floats * floats, -1, keepdims=True) + 1e-06)
        * scale_ref[...]
    ).astype(BF16)
    normed_own[...] = normed
    from_here = ids_ref[...] - ep
    from_here = jnp.where(from_here < 0, from_here + experts, from_here)
    hits, quarter = slot_hits(from_here, experts, capacity)
    stacked = jnp.concatenate(
        [normed[:, c * quarter_width : (c + 1) * quarter_width] for c in range(4)], axis=0
    )
    for g in range(groups):
        either = hits[g][0] | hits[g][1]
        placing = jnp.concatenate(
            [(either & (quarter == c)).astype(F32).astype(BF16) for c in range(4)], axis=1
        )
        out_buf[:, :, g * quarter_width : (g + 1) * quarter_width] = (
            dot(placing, stacked).astype(BF16).reshape(experts, 16, quarter_width)
        )

    pl.semaphore_wait(barrier, experts - 1 + 2 + int(paired))

    def peer(d):
        return lax.rem(ep + d, experts)

    def outward(d):
        there = experts - d
        return remote(
            out_buf.at[d], in_buf.at[there], out_send.at[d], out_recv.at[there], "ep", peer(d)
        )

    def inward(d):
        return remote(out_buf.at[d], in_buf.at[d], out_send.at[d], out_recv.at[d], "ep", peer(d))

    def spray(make, first, last):
        def go(i, carry):
            d = experts // 2 - i
            make(d).start()
            make(experts - d).start()
            return carry

        if first == 0:
            make(experts // 2).start()
        lax.fori_loop(max(first, 1), last, go, 0)

    far_from, far_to = (experts // 4, 3 * experts // 4)

    def drain(make, recv, first=1, last=experts):
        def go(d, carry):
            if recv:
                make(d).wait_recv()
            else:
                make(d).wait_send()
            return carry

        lax.fori_loop(first, last, go, 0)

    def far_slots(ref, g):
        return ref[far_from:far_to, :, g * quarter_width : (g + 1) * quarter_width].reshape(
            8 * experts, quarter_width
        )

    def near_slots(ref, g):
        here = slice(g * quarter_width, (g + 1) * quarter_width)
        return jnp.concatenate([ref[:far_from, :, here], ref[far_to:, :, here]], axis=0).reshape(
            8 * experts, quarter_width
        )

    early = 3 * experts // 16
    spray(outward, 0, early)

    class Ring:
        def __init__(self, index, own, slot, pair_left, pair_right):
            n = own.shape[0]
            mine = pl.ds(pl.multiple_of(side * (n // 2), n // 2), n // 2)
            other = pl.ds(pl.multiple_of((1 - side) * (n // 2), n // 2), n // 2)
            whole = pl.ds(0, n)
            s = [ring_send.at[6 * index + i] for i in range(6)]
            r = [ring_recv.at[6 * index + i] for i in range(6)]
            self.near, self.far, self.pair, self.paired_in = ([], [], [], [])
            for i, (to, half, rest, pair) in enumerate(
                [
                    (right, mine, other, paired and pair_left),
                    (left, other, mine, paired and pair_right),
                ]
            ):
                part = half if pair else whole
                self.near.append(
                    remote(own.at[part], slot(i + 1, part), s[i], r[i], "tp", to)
                )
                self.far.append(
                    remote(slot(i + 1, half), slot(3, half), s[2 + i], r[2 + i], "tp", to)
                )
                self.pair.append(
                    pair
                    and (
                        remote(
                            slot(i + 1, half), slot(i + 1, half), s[4 + i], r[4 + i], "grp", partner
                        ),
                        remote(
                            slot(i + 1, rest), slot(i + 1, rest), s[4 + i], r[4 + i], "grp", partner
                        ),
                    )
                )

        def start(self):
            for copy in self.near:
                copy.start()

        def forward(self):
            for copy, onward, pair in zip(self.near, self.far, self.pair):
                copy.wait_recv()
                onward.start()
                if pair:
                    pair[0].start()

        def beside(self):
            for pair in self.pair:
                if pair:
                    pair[1].wait_recv()

        def arrive(self):
            for copy in self.far:
                copy.wait_recv()

        def finish(self):
            for copy in self.near + self.far:
                copy.wait_send()
            for pair in self.pair:
                if pair:
                    pair[0].wait_send()

    def down_slot(base):
        def slot(s, rows):
            return wd_ref.at[pl.ds(pl.multiple_of(s * hid + base + rows.start, hid // 4), rows.size)]

        return slot

    gate_ring = Ring(0, gate_in, lambda s, rows: wg_ref.at[s, rows], True, True)
    up_ring = Ring(1, up_in, lambda s, rows: wu_ref.at[s, rows], True, True)
    down_rings = [
        Ring(2, down_in.at[pl.ds(0, hid // 2)], down_slot(0), True, False),
        Ring(3, down_in.at[pl.ds(hid // 2, hid // 2)], down_slot(hid // 2), False, True),
    ]
    normed_ring = Ring(4, normed_own, lambda s, rows: ngather.at[s, rows], False, False)
    weight_rings = (gate_ring, up_ring, *down_rings)
    for ring in weight_rings:
        ring.start()

    own_out = pltpu.make_async_copy(out_buf.at[0], in_buf.at[0], own_sem.at[0])
    own_out.start()
    own_normed = pltpu.make_async_copy(normed_own, ngather.at[0], own_sem.at[1])
    own_normed.start()

    for load in loads[:5] + loads[16:19]:
        load.wait()

    def mix(pair, carry):
        @pl.when(pair == pairs // 2)
        def _():
            gate_ring.forward()

        local_mixer(
            pair,
            q_ref,
            k_ref,
            v_ref,
            f_ref,
            a_ref,
            fb_ref,
            ab_ref,
            x_ref,
            omap_ref,
            oloc_ref,
            pay_ref,
        )
        return carry

    lax.fori_loop(0, pairs, mix, 0)

    def pay_out(h):
        return remote(
            pay_ref.at[h], arrived.at[ep], pay_send.at[h], pay_recv.at[ep], "ep", stride * h
        )

    def pay_in(e):
        return remote(pay_ref.at[0], arrived.at[e], pay_send.at[0], pay_recv.at[e], "ep", e)

    def others(act):
        for h in range(heads):
            pl.when(ep != stride * h)(functools.partial(act, h))

    others(lambda h: pay_out(h).start())
    own_pay = pltpu.make_async_copy(pay_ref.at[my_head], arrived.at[ep], own_sem.at[2])

    @pl.when(folds)
    def _():
        own_pay.start()

    spray(outward, early, experts // 2)
    for ring in weight_rings[1:]:
        ring.forward()
    normed_ring.start()

    def homeward(e):
        return remote(
            sent.at[e], states.at[my_head], home_send.at[e], home_recv.at[my_head], "ep", e
        )

    def home(h):
        return remote(sent.at[0], states.at[h], home_send.at[0], home_recv.at[h], "ep", stride * h)

    own_state = pltpu.make_async_copy(sent.at[ep], states.at[my_head], own_sem.at[3])

    def step(e, state):
        sent[e] = state.astype(BF16)

        @pl.when(e != ep)
        def _():
            pay_in(e).wait_recv()

        @pl.when((e > 0) & (e - 1 != ep))
        def _():
            homeward(e - 1).start()

        return fold_step(state, arrived[e])

    @pl.when(folds)
    def _():
        own_pay.wait()
        lax.fori_loop(0, experts, step, jnp.zeros(sent.shape[1:], F32))

        @pl.when(ep != experts - 1)
        def _():
            homeward(experts - 1).start()

        own_state.start()
        own_state.wait()

    half_rows = 2 * experts
    many = groups * half_rows
    at_row = iota((half_rows, 8 * experts), 0)
    at_col = iota((half_rows, 8 * experts), 1)
    picks = [
        (at_col == 16 * (at_row // 4) + 4 * c + at_row % 4).astype(F32).astype(BF16)
        for c in range(4)
    ]

    def unpack(slots, base):
        for g in range(groups):
            block = slots(in_buf, g)
            for c in range(4):
                xbuf[
                    base + g * half_rows : base + (g + 1) * half_rows,
                    c * quarter_width : (c + 1) * quarter_width,
                ] = dot(picks[c], block).astype(BF16)

    def hidden(base, s):
        rows = xbuf[base : base + many, :]
        return (jax.nn.silu(dot(rows, wg_ref[s])) * dot(rows, wu_ref[s])).astype(BF16)

    def lift(base):
        for s in range(3):
            hbuf[base : base + many, s * hid : (s + 1) * hid] = hidden(base, s)

    def lower(base):
        yacc[base : base + many, :] = dot(hbuf[base : base + many, :], wd_ref[: 3 * hid])

    at_row = iota((8 * experts, half_rows), 0)
    at_col = iota((8 * experts, half_rows), 1)
    put = jnp.concatenate(
        [
            (at_row == 16 * (at_col // 4) + 4 * c + at_col % 4).astype(F32).astype(BF16)
            for c in range(4)
        ],
        axis=1,
    )

    def complete(base, store):
        total = yacc[base : base + many, :] + dot(hidden(base, 3), wd_ref[3 * hid :])
        for g in range(groups):
            rows = total[g * half_rows : (g + 1) * half_rows].astype(BF16)
            rows = jnp.concatenate(
                [rows[:, c * quarter_width : (c + 1) * quarter_width] for c in range(4)], axis=0
            )
            block = dot(put, rows).astype(BF16).reshape(experts // 2, 16, quarter_width)
            store(slice(g * quarter_width, (g + 1) * quarter_width), block)

    def store_far(here, block):
        ret_buf[far_from:far_to, :, here] = block

    def store_near(here, block):
        ret_buf[:far_from, :, here] = block[:far_from]
        ret_buf[far_to:, :, here] = block[far_from:]

    def ret_out(d):
        there = experts - d
        return remote(
            ret_buf.at[d], back_buf.at[there], ret_send.at[d], ret_recv.at[there], "ep", peer(d)
        )

    def ret_in(d):
        return remote(ret_buf.at[d], back_buf.at[d], ret_send.at[d], ret_recv.at[d], "ep", peer(d))

    drain(inward, True, far_from, far_to)
    unpack(far_slots, 0)
    for load in loads[7:10]:
        load.wait()
    gate_ring.beside()
    up_ring.beside()
    lift(0)
    for ring in down_rings:
        ring.beside()
    lower(0)
    own_out.wait()
    drain(inward, True, 1, far_from)
    drain(inward, True, far_to, experts)
    unpack(near_slots, many)
    lift(many)
    lower(many)
    for ring in weight_rings:
        ring.arrive()
    complete(0, store_far)
    spray(ret_out, 0, experts // 4)
    complete(many, store_near)
    spray(ret_out, experts // 4, experts // 2)
    own_ret = pltpu.make_async_copy(ret_buf.at[0], back_buf.at[0], own_sem.at[4])
    own_ret.start()

    class Scatter:
        def __init__(self, index, part, relay, sums):
            n = part.shape[1]
            top, bottom = (pl.ds(0, n // 2), pl.ds(n // 2, n // 2))
            s = [rs_send.at[6 * index + i] for i in range(6)]
            r = [rs_recv.at[6 * index + i] for i in range(6)]
            self.part, self.sums = (part, sums)
            self.near = [
                remote(part.at[3, top], relay.at[0], s[0], r[0], "tp", right),
                remote(part.at[3, bottom], relay.at[1], s[1], r[1], "tp", left),
                remote(part.at[2], sums.at[1], s[2], r[2], "tp", right),
                remote(part.at[1], sums.at[2], s[3], r[3], "tp", left),
            ]
            self.far = [
                remote(relay.at[0], sums.at[3, top], s[4], r[4], "tp", right),
                remote(relay.at[1], sums.at[3, bottom], s[5], r[5], "tp", left),
            ]

        def start(self):
            for copy in self.near:
                copy.start()

        def forward(self):
            for copy, onward in zip(self.near[:2], self.far):
                copy.wait_recv()
                onward.start()

        def total(self):
            for copy in self.near[2:] + self.far:
                copy.wait_recv()
            out = self.part[0].astype(F32)
            for s in range(1, 4):
                out = out + self.sums[s].astype(F32)
            return out

        def finish(self):
            for copy in self.near + self.far:
                copy.wait_send()

    scatter_a = Scatter(0, part_a, relay_a, sums_a)
    scatter_b = Scatter(1, part_b, relay_b, sums_b)

    others(lambda h: home(h).wait_recv())
    for load in loads[5:7] + loads[19:20]:
        load.wait()

    def finish(pair, carry):
        finish_mixer(pair, omap_ref, oloc_ref, states, g_ref, gain_ref, mixed_ref)
        return carry

    lax.fori_loop(0, pairs, finish, 0)
    mixer_rows = part_a.shape[1]
    for s, owner in enumerate((tp, left, right, across)):
        mine = pl.ds(pl.multiple_of(owner * mixer_rows, mixer_rows), mixer_rows)
        part_a[s] = dot(mixed_ref[mine, :], wout_ref[...]).astype(BF16)
    normed_ring.forward()
    scatter_a.start()

    own_normed.wait()
    for load in loads[10:13]:
        load.wait()
    normed_ring.arrive()
    scatter_a.forward()
    both = dot(ngather[...].reshape(tps * tokens, width), cgu_ref[...])
    inner = (jax.nn.silu(both[:, :half_lanes]) * both[:, half_lanes:]).astype(BF16)
    for s in range(4):
        part_b[s] = dot(inner[s * tokens : (s + 1) * tokens], cd_ref[...]).astype(BF16)
    scatter_b.start()
    scatter_b.forward()
    attend_ref[...] = scatter_a.total().astype(BF16)
    yacc[:tokens, :] = scatter_b.total()

    from_here = ids_ref[...] - ep
    from_here = jnp.where(from_here < 0, from_here + experts, from_here)
    hits, quarter = slot_hits(from_here, experts, capacity)
    for load in loads[20:]:
        load.wait()

    def weigh(g, c):
        weight = jnp.where(hits[g][0], mix_ref[0:1, :], 0.0) + jnp.where(
            hits[g][1], mix_ref[1:2, :], 0.0
        )
        return split(jnp.where(quarter == c, weight, 0.0), 2)

    far = slice(16 * far_from, 16 * far_to)

    def gather(slots, take):
        for c in range(4):
            here = slice(c * quarter_width, (c + 1) * quarter_width)
            block = yacc[:tokens, here]
            for g in range(groups):
                values = slots(back_buf, g)
                for part in weigh(g, c):
                    block = block + dot_tn(take(part), values)
            yacc[:tokens, here] = block

    drain(ret_in, True, far_from, far_to)
    gather(far_slots, lambda part: part[far])
    own_ret.wait()
    drain(ret_in, True, 1, far_from)
    drain(ret_in, True, far_to, experts)
    gather(
        near_slots,
        lambda part: jnp.concatenate([part[: far.start], part[far.stop :]], axis=0),
    )
    moe_ref[...] = yacc[:tokens, :].astype(BF16)

    drain(outward, False)
    drain(ret_out, False)
    others(lambda h: pay_out(h).wait_send())

    def homegoing(d, carry):
        homeward(peer(d)).wait_send()
        return carry

    @pl.when(folds)
    def _():
        lax.fori_loop(1, experts, homegoing, 0)

    for item in weight_rings + (normed_ring, scatter_a, scatter_b):
        item.finish()


def on_device(
    query_vectors,
    attend_lookup_vectors,
    attend_content_vectors,
    forget_speed_dependent,
    amend_speed_dependent,
    result_switch_preactivation,
    feature_forget_baseline,
    amend_speed_baseline,
    sudden_forget_extra,
    group_scaling_factor,
    result_mapping_matrix,
    specialist_tokens_activations,
    specialist_scaling_factor,
    selected_specialists,
    selection_mixing_factors,
    dispatched_switch_matrix,
    dispatched_raising_matrix,
    dispatched_lowering_matrix,
    common_switch_matrix,
    common_raising_matrix,
    common_lowering_matrix,
):
    tokens, top_count = selected_specialists.shape
    width = specialist_tokens_activations.shape[1]
    rows, mix_width = query_vectors.shape
    groups = sudden_forget_extra.shape[1]
    lanes = 2 * (mix_width // groups)
    experts = lax.axis_size("ep")
    tps = lax.axis_size("tp")
    capacity = 3 * tokens * top_count // (2 * experts)
    hid = dispatched_switch_matrix.shape[2]
    shared = common_switch_matrix.shape[1]
    slab = (experts, 16, capacity * width // 16)
    vmem = pl.BlockSpec(memory_space=pltpu.VMEM)
    hbm = pl.BlockSpec(memory_space=pltpu.HBM)
    V = pltpu.VMEM
    dma = pltpu.SemaphoreType.DMA
    mixer_rows = rows // tps
    return pl.pallas_call(
        functools.partial(everything, capacity),
        in_specs=[hbm] * 21,
        out_specs=(vmem, vmem),
        out_shape=(
            jax.ShapeDtypeStruct((mixer_rows, width), BF16),
            jax.ShapeDtypeStruct((tokens, width), BF16),
        ),
        scratch_shapes=[V((rows, mix_width), BF16)] * 6
        + [
            V((mix_width, width), BF16),
            V((tps, width, hid), BF16),
            V((tps, width, hid), BF16),
            V((tps * hid, width), BF16),
            V((width, 2 * shared), BF16),
            V((shared, width), BF16),
            V((rows, mix_width), BF16),
            V((rows, mix_width), F32),
            V((groups, lanes // 2, lanes), BF16),
            V((experts, lanes // 2, lanes), BF16),
            V((experts, lanes // 4, lanes), BF16),
            V((groups, lanes // 4, lanes), BF16),
            V((rows, mix_width), BF16),
        ]
        + [V(slab, BF16)] * 4
        + [
            V((experts * capacity, width), BF16),
            V((experts * capacity, width), F32),
            V((experts * capacity, 3 * hid), BF16),
            V((tokens, width), BF16),
            V((tps, tokens, width), BF16),
            V((tps, mixer_rows, width), BF16),
            V((tps, tokens, width), BF16),
            V((2, mixer_rows // 2, width), BF16),
            V((2, tokens // 2, width), BF16),
            V((tps, mixer_rows, width), BF16),
            V((tps, tokens, width), BF16),
            V((tokens, width), BF16),
            V((1, width), F32),
            V((top_count, tokens), jnp.int32),
            V((1, mix_width), F32),
            V((1, mix_width), F32),
            V((groups, rows), F32),
            V((1, mix_width), F32),
            V((top_count, tokens), F32),
            dma((21,)),
            dma((5,)),
        ]
        + [dma((experts,))] * 8
        + [dma((30,)), dma((30,)), dma((12,)), dma((12,))],
        compiler_params=pltpu.CompilerParams(
            collective_id=0, has_side_effects=True, vmem_limit_bytes=60 * 1024 * 1024
        ),
        name="everything",
    )(
        query_vectors,
        attend_lookup_vectors,
        attend_content_vectors,
        forget_speed_dependent,
        amend_speed_dependent,
        result_switch_preactivation,
        feature_forget_baseline.reshape(1, -1),
        amend_speed_baseline.reshape(1, -1),
        sudden_forget_extra.T,
        group_scaling_factor.reshape(1, -1),
        result_mapping_matrix,
        specialist_tokens_activations,
        specialist_scaling_factor.reshape(1, -1),
        selected_specialists.T,
        selection_mixing_factors.T,
        dispatched_switch_matrix[0],
        dispatched_raising_matrix[0],
        dispatched_lowering_matrix[0],
        common_switch_matrix,
        common_raising_matrix,
        common_lowering_matrix,
    )


def solution(mesh):
    rows = P(("grp", "ep"), "tp")
    tokens = P(("grp", "ep", "tp"), None)
    placed = (
        (rows,) * 6
        + (P("tp"), P("tp"), rows, P("tp"), P("tp", None), tokens, P(), tokens, tokens)
        + (P("ep", None, "tp"), P("ep", None, "tp"), P("ep", "tp", None))
        + (P(None, "tp"), P(None, "tp"), P("tp", None))
    )
    return jax.shard_map(
        on_device, mesh=mesh, in_specs=placed, out_specs=(tokens, tokens), check_vma=False
    )
```

```python
import functools

import jax
import jax.numpy as jnp
from jax import lax
from jax.experimental import pallas as pl
from jax.experimental.pallas import tpu as pltpu
from jax.sharding import PartitionSpec as P

F32 = jnp.float32
BF16 = jnp.bfloat16
SPAN = 64
MESH = pl.DeviceIdType.MESH


def dot(a, b):
    return jnp.dot(a, b, preferred_element_type=F32)


def dot_nt(a, b):
    return lax.dot_general(a, b, (((1,), (1,)), ((), ())), preferred_element_type=F32)


def dot_tn(a, b):
    return lax.dot_general(a, b, (((0,), (0,)), ((), ())), preferred_element_type=F32)


def split(x, parts):
    out = []
    for _ in range(parts - 1):
        out.append(x.astype(BF16))
        x = x - out[-1].astype(F32)
    out.append(x.astype(BF16))
    return out


def iota(shape, dim):
    return lax.broadcasted_iota(jnp.int32, shape, dim)


def local_mixer(
    pair, q_ref, k_ref, v_ref, f_ref, a_ref, fb_ref, ab_ref, x_ref, omap_ref, oloc_ref, pay_ref
):
    rows = q_ref.shape[0]
    groups = x_ref.shape[0]
    half = q_ref.shape[1] // groups
    lanes = 2 * half
    spans = rows // SPAN
    here = pl.ds(pl.multiple_of(pair * lanes, lanes), lanes)
    low = iota((SPAN, lanes), 1) < half
    col = jnp.where(low, iota((SPAN, lanes), 1), iota((SPAN, lanes), 1) - half)
    row = iota((SPAN, lanes), 0)
    strict = row > col
    inclusive = row >= col
    tri = (iota((SPAN, SPAN), 0) >= iota((SPAN, SPAN), 1)).astype(BF16)
    tri3 = jnp.concatenate([tri] * 3, axis=1)
    same = ((iota((lanes, lanes), 0) < half) == (iota((lanes, lanes), 1) < half)).astype(BF16)
    same2 = jnp.concatenate([same] * 2, axis=0)
    spread = (
        iota((groups, lanes), 0) == 2 * pair + (iota((groups, lanes), 1) >= half).astype(jnp.int32)
    ).astype(F32)
    spread3 = jnp.concatenate([spread] * 3, axis=0).astype(BF16)
    below = iota((lanes, lanes), 0) < half
    left = iota((lanes, lanes), 1) < half

    def stack(x):
        return jnp.concatenate([jnp.where(low, x, 0.0), jnp.where(low, 0.0, x)], axis=0).astype(
            BF16
        )

    fb = fb_ref[:, here]
    ab = ab_ref[:, here]
    parts = [part.astype(F32) for part in split(x_ref[...], 3)]
    extra = dot_tn(jnp.concatenate(parts, axis=0).astype(BF16), spread3)

    spans_in = []
    for c in range(spans):
        at = slice(c * SPAN, (c + 1) * SPAN)
        decay = -jnp.exp(fb + f_ref[at, here].astype(F32)) + extra[at, :]
        rate = jax.nn.sigmoid(ab + a_ref[at, here].astype(F32))
        key = k_ref[at, here].astype(F32)
        sq = dot(jnp.concatenate(split(key * key, 2), axis=1), same2)
        unit = key * lax.rsqrt(sq + 1e-06)
        cum = dot(tri3, jnp.concatenate(split(decay, 3), axis=0))
        mid = cum[SPAN // 2 : SPAN // 2 + 1, :]
        last = cum[SPAN - 1 : SPAN, :]
        left_erase = -unit * jnp.exp(cum - decay - mid)
        left_read = q_ref[at, here].astype(F32) * jnp.exp(cum - mid)
        right = jnp.exp(mid - cum) * rate
        right_erase = unit * right
        right_write = key * right
        grow = jnp.exp(mid)
        tail = jnp.exp(last - mid)
        lefts = jnp.concatenate([left_erase, left_read], axis=0).astype(BF16)
        rights = jnp.concatenate([stack(right_erase), stack(right_write)], axis=0)
        pairs = dot_nt(lefts, rights)
        a_mat = jnp.where(strict, pairs[:SPAN, :lanes], 0.0)
        erase_write = jnp.where(strict, pairs[:SPAN, lanes:], 0.0)
        read_erase = jnp.where(inclusive, pairs[SPAN:, :lanes], 0.0)
        read_write = jnp.where(inclusive, pairs[SPAN:, lanes:], 0.0)
        value = v_ref[at, here].astype(F32)
        writes = dot(
            jnp.concatenate([erase_write, read_write], axis=0).astype(BF16), stack(value)
        )
        ends = jnp.concatenate([right_erase * tail, right_write * tail], axis=0).astype(BF16)
        spans_in.append(
            dict(
                a=a_mat,
                first=stack(left_erase * grow),
                read=left_read * grow,
                re=read_erase.astype(BF16),
                ew=stack(writes[:SPAN]),
                rw=writes[SPAN:],
                ends=ends,
                value=v_ref[at, here],
                last=jnp.exp(last),
            )
        )

    eye = (row == col).astype(F32)
    block = 1
    inverse = None
    while block < SPAN:
        in_block = (row // (2 * block) == col // (2 * block)) & (
            (row // block) % 2 == 1
        ) & ((col // block) % 2 == 0)
        steps = [jnp.where(in_block, s["a"], 0.0) for s in spans_in]
        if inverse is None:
            inverse = [eye + step for step in steps]
        else:
            inner = [
                dot(step.astype(BF16), stack(x)) for step, x in zip(steps, inverse)
            ]
            inverse = [x + dot(x.astype(BF16), stack(y)) for x, y in zip(inverse, inner)]
        block *= 2

    state = jnp.concatenate([eye, jnp.zeros_like(eye)], axis=0)
    for c, s in enumerate(spans_in):
        at = slice(c * SPAN, (c + 1) * SPAN)
        solved = dot(inverse[c].astype(BF16), jnp.concatenate([s["first"], s["ew"]], axis=1))
        w, y = (solved[:, :lanes], solved[:, lanes:])
        seen = dot(s["re"], jnp.concatenate([stack(w), stack(y)], axis=1))
        read = s["read"] + seen[:, :lanes]
        added = s["rw"] + seen[:, lanes:]
        value = s["value"]
        erased = dot_tn(w.astype(BF16), s["ends"][:SPAN])
        erased = jnp.where(below == left, erased, 0.0).astype(BF16)
        offset = dot_tn(jnp.concatenate([y.astype(BF16), value], axis=0), s["ends"])
        offset = jnp.where(low, offset[:half], offset[half:])
        both = jnp.concatenate([stack(state[:SPAN]), stack(state[SPAN:])], axis=0)
        reads = dot_nt(read.astype(BF16), both)
        omap_ref[at, here] = reads[:, :lanes].astype(BF16)
        oloc_ref[at, here] = added + reads[:, lanes:]
        state = (
            state * s["last"]
            + dot(state.astype(BF16), erased)
            + jnp.concatenate([jnp.zeros_like(offset), offset], axis=0)
        )
    jump, offset = (state[:SPAN], state[SPAN:])
    jump_turned = pltpu.roll(jump, half, 1)
    offset_turned = pltpu.roll(offset, half, 1)
    near = low[: SPAN // 2]
    for h in range(2):
        packed = [
            jnp.where(near, (x, turned)[h][: SPAN // 2], (turned, x)[h][SPAN // 2 :])
            for x, turned in ((jump, jump_turned), (offset, offset_turned))
        ]
        pay_ref[2 * pair + h] = jnp.concatenate(packed, axis=0).astype(BF16)


def fold_step(state, arrived):
    lanes = state.shape[1]
    half = lanes // 2
    low = iota(state.shape, 1) < half
    block = arrived.astype(F32)
    rows = state.shape[0]
    jump, offset = (block[:rows], block[rows:])
    turned = pltpu.roll(jump, half, 1)
    spread = jnp.concatenate(
        [
            jnp.where(low, jump, 0.0),
            jnp.where(low, turned, 0.0),
            jnp.where(low, 0.0, turned),
            jnp.where(low, 0.0, jump),
        ],
        axis=0,
    ).astype(BF16)
    parts = [part.astype(F32) for part in split(state, 2)]
    moved = dot(jnp.concatenate(parts, axis=0).astype(BF16), spread)
    return moved[:rows] + moved[rows:] + offset


def finish_mixer(pair, omap_ref, oloc_ref, state_ref, gate_ref, gain_ref, out_ref):
    lanes = state_ref.shape[2]
    half = lanes // 2
    here = pl.ds(pl.multiple_of(pair * lanes, lanes), lanes)
    low = iota(state_ref.shape[1:], 1) < half
    tiles = []
    for h in range(2):
        block = state_ref[2 * pair + h].astype(F32)
        turned = pltpu.roll(block, half, 1)
        if h == 0:
            tiles += [jnp.where(low, block, 0.0), jnp.where(low, turned, 0.0)]
        else:
            tiles += [jnp.where(low, 0.0, turned), jnp.where(low, 0.0, block)]
    state = jnp.concatenate(tiles, axis=0).astype(BF16)
    same = jnp.where(
        (iota((lanes, lanes), 0) < half) == (iota((lanes, lanes), 1) < half), 1.0 / half, 0.0
    ).astype(BF16)
    same2 = jnp.concatenate([same] * 2, axis=0)
    head_out = oloc_ref[:, here] + dot_nt(omap_ref[:, here], state)
    mean = dot(jnp.concatenate(split(head_out, 2), axis=1), same2)
    centered = head_out - mean
    var = dot(jnp.concatenate(split(centered * centered, 2), axis=1), same2)
    normed = centered * lax.rsqrt(var + 0.00064) * gain_ref[:, here]
    out_ref[:, here] = (normed * jax.nn.sigmoid(gate_ref[:, here].astype(F32))).astype(BF16)


def slot_hits(ids, experts, capacity):
    tokens = ids.shape[1]
    ids = ids.astype(F32)
    expert = iota((experts, tokens), 0).astype(F32)
    hot = [(expert == ids[j : j + 1]).astype(F32) for j in range(2)]
    earlier = (iota((tokens, tokens), 0) < iota((tokens, tokens), 1)).astype(F32).astype(BF16)
    before = dot((hot[0] + hot[1]).astype(BF16), earlier)
    place = [
        ids[j : j + 1] * capacity + jnp.sum(hot[j] * before, axis=0, keepdims=True)
        for j in range(2)
    ]
    at = iota((16 * experts, tokens), 0)
    base = (capacity * (at // 16) + at % 4).astype(F32)
    quarter = (at // 4) % 4
    groups = [[base + 4 * g == place[j] for j in range(2)] for g in range(capacity // 4)]
    return groups, quarter


def everything(
    capacity,
    q_in,
    k_in,
    v_in,
    f_in,
    a_in,
    g_in,
    fb_in,
    ab_in,
    x_in,
    gain_in,
    wout_in,
    tok_in,
    scale_in,
    ids_in,
    mix_in,
    gate_in,
    up_in,
    down_in,
    cgate_in,
    cup_in,
    cdown_in,
    attend_ref,
    moe_ref,
    q_ref,
    k_ref,
    v_ref,
    f_ref,
    a_ref,
    g_ref,
    wout_ref,
    wg_ref,
    wu_ref,
    wd_ref,
    cgu_ref,
    cd_ref,
    omap_ref,
    oloc_ref,
    pay_ref,
    arrived,
    sent,
    states,
    mixed_ref,
    out_buf,
    in_buf,
    ret_buf,
    back_buf,
    xbuf,
    yacc,
    hbuf,
    normed_own,
    ngather,
    part_a,
    part_b,
    relay_a,
    relay_b,
    sums_a,
    sums_b,
    tok_ref,
    scale_ref,
    ids_ref,
    fb_ref,
    ab_ref,
    x_ref,
    gain_ref,
    mix_ref,
    load_sem,
    own_sem,
    out_send,
    out_recv,
    pay_send,
    pay_recv,
    home_send,
    home_recv,
    ret_send,
    ret_recv,
    ring_send,
    ring_recv,
    rs_send,
    rs_recv,
):
    experts = out_buf.shape[0]
    tps = ngather.shape[0]
    tokens, width = tok_ref.shape
    quarter_width = width // 4
    groups = capacity // 4
    pairs = omap_ref.shape[1] // sent.shape[2]
    ep = lax.axis_index("ep")
    tp = lax.axis_index("tp")
    right, left, across = (lax.rem(tp + 1, tps), lax.rem(tp + 3, tps), lax.rem(tp + 2, tps))
    paired = lax.axis_size("grp") % 2 == 0
    grp = lax.axis_index("grp")
    side = lax.rem(grp, 2)
    partner = grp + 1 - 2 * side
    heads = pay_ref.shape[0]
    stride = experts // heads
    my_head = ep // stride
    folds = lax.rem(ep, stride) == 0

    barrier = pltpu.get_barrier_semaphore()

    def greet(d, carry):
        pl.semaphore_signal(
            barrier, inc=1, device_id={"ep": lax.rem(ep + d, experts)}, device_id_type=MESH
        )
        return carry

    lax.fori_loop(1, experts, greet, 0)
    for near in (right, left):
        pl.semaphore_signal(barrier, inc=1, device_id={"tp": near}, device_id_type=MESH)
    if paired:
        pl.semaphore_signal(barrier, inc=1, device_id={"grp": partner}, device_id_type=MESH)

    half_lanes = cgate_in.shape[1]
    hid = gate_in.shape[1]
    loads = [
        pltpu.make_async_copy(a, b, load_sem.at[i])
        for i, (a, b) in enumerate(
            [
                (q_in, q_ref),
                (k_in, k_ref),
                (v_in, v_ref),
                (f_in, f_ref),
                (a_in, a_ref),
                (g_in, g_ref),
                (wout_in, wout_ref),
                (gate_in, wg_ref.at[0]),
                (up_in, wu_ref.at[0]),
                (down_in, wd_ref.at[pl.ds(0, hid)]),
                (cgate_in, cgu_ref.at[:, pl.ds(0, half_lanes)]),
                (cup_in, cgu_ref.at[:, pl.ds(half_lanes, half_lanes)]),
                (cdown_in, cd_ref),
                (tok_in, tok_ref),
                (scale_in, scale_ref),
                (ids_in, ids_ref),
                (fb_in, fb_ref),
                (ab_in, ab_ref),
                (x_in, x_ref),
                (gain_in, gain_ref),
                (mix_in, mix_ref),
            ]
        )
    ]
    for load in loads[13:] + loads[:13]:
        load.start()

    def remote(src, dst, send, recv, axis, to):
        return pltpu.make_async_remote_copy(
            src_ref=src,
            dst_ref=dst,
            send_sem=send,
            recv_sem=recv,
            device_id={axis: to},
            device_id_type=MESH,
        )

    for load in loads[13:16]:
        load.wait()
    floats = tok_ref[...].astype(F32)
    normed = (
        floats
        * lax.rsqrt(jnp.mean(floats * floats, -1, keepdims=True) + 1e-06)
        * scale_ref[...]
    ).astype(BF16)
    normed_own[...] = normed
    from_here = ids_ref[...] - ep
    from_here = jnp.where(from_here < 0, from_here + experts, from_here)
    hits, quarter = slot_hits(from_here, experts, capacity)
    stacked = jnp.concatenate(
        [normed[:, c * quarter_width : (c + 1) * quarter_width] for c in range(4)], axis=0
    )
    for g in range(groups):
        either = hits[g][0] | hits[g][1]
        placing = jnp.concatenate(
            [(either & (quarter == c)).astype(F32).astype(BF16) for c in range(4)], axis=1
        )
        out_buf[:, :, g * quarter_width : (g + 1) * quarter_width] = (
            dot(placing, stacked).astype(BF16).reshape(experts, 16, quarter_width)
        )

    pl.semaphore_wait(barrier, experts - 1 + 2 + int(paired))

    def peer(d):
        return lax.rem(ep + d, experts)

    def outward(d):
        there = experts - d
        return remote(
            out_buf.at[d], in_buf.at[there], out_send.at[d], out_recv.at[there], "ep", peer(d)
        )

    def inward(d):
        return remote(out_buf.at[d], in_buf.at[d], out_send.at[d], out_recv.at[d], "ep", peer(d))

    def spray(make, first, last):
        def go(i, carry):
            d = experts // 2 - i
            make(d).start()
            make(experts - d).start()
            return carry

        if first == 0:
            make(experts // 2).start()
        lax.fori_loop(max(first, 1), last, go, 0)

    far_from, far_to = (experts // 4, 3 * experts // 4)

    def drain(make, recv, first=1, last=experts):
        def go(d, carry):
            if recv:
                make(d).wait_recv()
            else:
                make(d).wait_send()
            return carry

        lax.fori_loop(first, last, go, 0)

    def far_slots(ref, g):
        return ref[far_from:far_to, :, g * quarter_width : (g + 1) * quarter_width].reshape(
            8 * experts, quarter_width
        )

    def near_slots(ref, g):
        here = slice(g * quarter_width, (g + 1) * quarter_width)
        return jnp.concatenate([ref[:far_from, :, here], ref[far_to:, :, here]], axis=0).reshape(
            8 * experts, quarter_width
        )

    early = 3 * experts // 16
    spray(outward, 0, early)

    class Ring:
        def __init__(self, index, own, slot, pair_left, pair_right):
            n = own.shape[0]
            mine = pl.ds(pl.multiple_of(side * (n // 2), n // 2), n // 2)
            other = pl.ds(pl.multiple_of((1 - side) * (n // 2), n // 2), n // 2)
            whole = pl.ds(0, n)
            s = [ring_send.at[6 * index + i] for i in range(6)]
            r = [ring_recv.at[6 * index + i] for i in range(6)]
            self.near, self.far, self.pair, self.paired_in = ([], [], [], [])
            for i, (to, half, rest, pair) in enumerate(
                [
                    (right, mine, other, paired and pair_left),
                    (left, other, mine, paired and pair_right),
                ]
            ):
                part = half if pair else whole
                self.near.append(
                    remote(own.at[part], slot(i + 1, part), s[i], r[i], "tp", to)
                )
                self.far.append(
                    remote(slot(i + 1, half), slot(3, half), s[2 + i], r[2 + i], "tp", to)
                )
                self.pair.append(
                    pair
                    and (
                        remote(
                            slot(i + 1, half), slot(i + 1, half), s[4 + i], r[4 + i], "grp", partner
                        ),
                        remote(
                            slot(i + 1, rest), slot(i + 1, rest), s[4 + i], r[4 + i], "grp", partner
                        ),
                    )
                )

        def start(self):
            for copy in self.near:
                copy.start()

        def forward(self):
            for copy, onward, pair in zip(self.near, self.far, self.pair):
                copy.wait_recv()
                onward.start()
                if pair:
                    pair[0].start()

        def beside(self):
            for pair in self.pair:
                if pair:
                    pair[1].wait_recv()

        def arrive(self):
            for copy in self.far:
                copy.wait_recv()

        def finish(self):
            for copy in self.near + self.far:
                copy.wait_send()
            for pair in self.pair:
                if pair:
                    pair[0].wait_send()

    def down_slot(base):
        def slot(s, rows):
            return wd_ref.at[pl.ds(pl.multiple_of(s * hid + base + rows.start, hid // 4), rows.size)]

        return slot

    gate_ring = Ring(0, gate_in, lambda s, rows: wg_ref.at[s, rows], True, True)
    up_ring = Ring(1, up_in, lambda s, rows: wu_ref.at[s, rows], True, True)
    down_rings = [
        Ring(2, down_in.at[pl.ds(0, hid // 2)], down_slot(0), True, False),
        Ring(3, down_in.at[pl.ds(hid // 2, hid // 2)], down_slot(hid // 2), False, True),
    ]
    normed_ring = Ring(4, normed_own, lambda s, rows: ngather.at[s, rows], False, False)
    weight_rings = (gate_ring, up_ring, *down_rings)
    for ring in weight_rings:
        ring.start()

    own_out = pltpu.make_async_copy(out_buf.at[0], in_buf.at[0], own_sem.at[0])
    own_out.start()
    own_normed = pltpu.make_async_copy(normed_own, ngather.at[0], own_sem.at[1])
    own_normed.start()

    for load in loads[:5] + loads[16:19]:
        load.wait()

    def mix(pair, carry):
        @pl.when(pair == pairs // 2)
        def _():
            gate_ring.forward()

        local_mixer(
            pair,
            q_ref,
            k_ref,
            v_ref,
            f_ref,
            a_ref,
            fb_ref,
            ab_ref,
            x_ref,
            omap_ref,
            oloc_ref,
            pay_ref,
        )
        return carry

    lax.fori_loop(0, pairs, mix, 0)

    def pay_out(h):
        return remote(
            pay_ref.at[h], arrived.at[ep], pay_send.at[h], pay_recv.at[ep], "ep", stride * h
        )

    def pay_in(e):
        return remote(pay_ref.at[0], arrived.at[e], pay_send.at[0], pay_recv.at[e], "ep", e)

    def others(act):
        for h in range(heads):
            pl.when(ep != stride * h)(functools.partial(act, h))

    others(lambda h: pay_out(h).start())
    own_pay = pltpu.make_async_copy(pay_ref.at[my_head], arrived.at[ep], own_sem.at[2])

    @pl.when(folds)
    def _():
        own_pay.start()

    spray(outward, early, experts // 2)
    for ring in weight_rings[1:]:
        ring.forward()
    normed_ring.start()

    def homeward(e):
        return remote(
            sent.at[e], states.at[my_head], home_send.at[e], home_recv.at[my_head], "ep", e
        )

    def home(h):
        return remote(sent.at[0], states.at[h], home_send.at[0], home_recv.at[h], "ep", stride * h)

    own_state = pltpu.make_async_copy(sent.at[ep], states.at[my_head], own_sem.at[3])

    def step(e, state):
        sent[e] = state.astype(BF16)

        @pl.when(e != ep)
        def _():
            pay_in(e).wait_recv()

        @pl.when((e > 0) & (e - 1 != ep))
        def _():
            homeward(e - 1).start()

        return fold_step(state, arrived[e])

    @pl.when(folds)
    def _():
        own_pay.wait()
        lax.fori_loop(0, experts, step, jnp.zeros(sent.shape[1:], F32))

        @pl.when(ep != experts - 1)
        def _():
            homeward(experts - 1).start()

        own_state.start()
        own_state.wait()

    half_rows = 2 * experts
    many = groups * half_rows
    at_row = iota((half_rows, 8 * experts), 0)
    at_col = iota((half_rows, 8 * experts), 1)
    picks = [
        (at_col == 16 * (at_row // 4) + 4 * c + at_row % 4).astype(F32).astype(BF16)
        for c in range(4)
    ]

    def unpack(slots, base):
        for g in range(groups):
            block = slots(in_buf, g)
            for c in range(4):
                xbuf[
                    base + g * half_rows : base + (g + 1) * half_rows,
                    c * quarter_width : (c + 1) * quarter_width,
                ] = dot(picks[c], block).astype(BF16)

    def hidden(base, s):
        rows = xbuf[base : base + many, :]
        return (jax.nn.silu(dot(rows, wg_ref[s])) * dot(rows, wu_ref[s])).astype(BF16)

    def lift(base):
        for s in range(3):
            hbuf[base : base + many, s * hid : (s + 1) * hid] = hidden(base, s)

    def lower(base):
        yacc[base : base + many, :] = dot(hbuf[base : base + many, :], wd_ref[: 3 * hid])

    at_row = iota((8 * experts, half_rows), 0)
    at_col = iota((8 * experts, half_rows), 1)
    put = jnp.concatenate(
        [
            (at_row == 16 * (at_col // 4) + 4 * c + at_col % 4).astype(F32).astype(BF16)
            for c in range(4)
        ],
        axis=1,
    )

    def complete(base, store):
        total = yacc[base : base + many, :] + dot(hidden(base, 3), wd_ref[3 * hid :])
        for g in range(groups):
            rows = total[g * half_rows : (g + 1) * half_rows].astype(BF16)
            rows = jnp.concatenate(
                [rows[:, c * quarter_width : (c + 1) * quarter_width] for c in range(4)], axis=0
            )
            block = dot(put, rows).astype(BF16).reshape(experts // 2, 16, quarter_width)
            store(slice(g * quarter_width, (g + 1) * quarter_width), block)

    def store_far(here, block):
        ret_buf[far_from:far_to, :, here] = block

    def store_near(here, block):
        ret_buf[:far_from, :, here] = block[:far_from]
        ret_buf[far_to:, :, here] = block[far_from:]

    def ret_out(d):
        there = experts - d
        return remote(
            ret_buf.at[d], back_buf.at[there], ret_send.at[d], ret_recv.at[there], "ep", peer(d)
        )

    def ret_in(d):
        return remote(ret_buf.at[d], back_buf.at[d], ret_send.at[d], ret_recv.at[d], "ep", peer(d))

    drain(inward, True, far_from, far_to)
    unpack(far_slots, 0)
    for load in loads[7:10]:
        load.wait()
    gate_ring.beside()
    up_ring.beside()
    lift(0)
    for ring in down_rings:
        ring.beside()
    lower(0)
    for ring in weight_rings:
        ring.arrive()
    complete(0, store_far)
    spray(ret_out, 0, experts // 4)
    own_out.wait()
    drain(inward, True, 1, far_from)
    drain(inward, True, far_to, experts)
    unpack(near_slots, many)
    lift(many)
    lower(many)
    complete(many, store_near)
    spray(ret_out, experts // 4, experts // 2)
    own_ret = pltpu.make_async_copy(ret_buf.at[0], back_buf.at[0], own_sem.at[4])
    own_ret.start()

    class Scatter:
        def __init__(self, index, part, relay, sums):
            n = part.shape[1]
            top, bottom = (pl.ds(0, n // 2), pl.ds(n // 2, n // 2))
            s = [rs_send.at[6 * index + i] for i in range(6)]
            r = [rs_recv.at[6 * index + i] for i in range(6)]
            self.part, self.sums = (part, sums)
            self.near = [
                remote(part.at[3, top], relay.at[0], s[0], r[0], "tp", right),
                remote(part.at[3, bottom], relay.at[1], s[1], r[1], "tp", left),
                remote(part.at[2], sums.at[1], s[2], r[2], "tp", right),
                remote(part.at[1], sums.at[2], s[3], r[3], "tp", left),
            ]
            self.far = [
                remote(relay.at[0], sums.at[3, top], s[4], r[4], "tp", right),
                remote(relay.at[1], sums.at[3, bottom], s[5], r[5], "tp", left),
            ]

        def start(self):
            for copy in self.near:
                copy.start()

        def forward(self):
            for copy, onward in zip(self.near[:2], self.far):
                copy.wait_recv()
                onward.start()

        def total(self):
            for copy in self.near[2:] + self.far:
                copy.wait_recv()
            out = self.part[0].astype(F32)
            for s in range(1, 4):
                out = out + self.sums[s].astype(F32)
            return out

        def finish(self):
            for copy in self.near + self.far:
                copy.wait_send()

    scatter_a = Scatter(0, part_a, relay_a, sums_a)
    scatter_b = Scatter(1, part_b, relay_b, sums_b)

    others(lambda h: home(h).wait_recv())
    for load in loads[5:7] + loads[19:20]:
        load.wait()

    def finish(pair, carry):
        finish_mixer(pair, omap_ref, oloc_ref, states, g_ref, gain_ref, mixed_ref)
        return carry

    lax.fori_loop(0, pairs, finish, 0)
    mixer_rows = part_a.shape[1]
    for s, owner in enumerate((tp, left, right, across)):
        mine = pl.ds(pl.multiple_of(owner * mixer_rows, mixer_rows), mixer_rows)
        part_a[s] = dot(mixed_ref[mine, :], wout_ref[...]).astype(BF16)
    normed_ring.forward()
    scatter_a.start()

    own_normed.wait()
    for load in loads[10:13]:
        load.wait()
    normed_ring.arrive()
    scatter_a.forward()
    both = dot(ngather[...].reshape(tps * tokens, width), cgu_ref[...])
    inner = (jax.nn.silu(both[:, :half_lanes]) * both[:, half_lanes:]).astype(BF16)
    for s in range(4):
        part_b[s] = dot(inner[s * tokens : (s + 1) * tokens], cd_ref[...]).astype(BF16)
    scatter_b.start()
    scatter_b.forward()
    attend_ref[...] = scatter_a.total().astype(BF16)
    yacc[:tokens, :] = scatter_b.total()

    from_here = ids_ref[...] - ep
    from_here = jnp.where(from_here < 0, from_here + experts, from_here)
    hits, quarter = slot_hits(from_here, experts, capacity)
    for load in loads[20:]:
        load.wait()

    def weigh(g, c):
        weight = jnp.where(hits[g][0], mix_ref[0:1, :], 0.0) + jnp.where(
            hits[g][1], mix_ref[1:2, :], 0.0
        )
        return split(jnp.where(quarter == c, weight, 0.0), 2)

    far = slice(16 * far_from, 16 * far_to)

    def gather(slots, take):
        for c in range(4):
            here = slice(c * quarter_width, (c + 1) * quarter_width)
            block = yacc[:tokens, here]
            for g in range(groups):
                values = slots(back_buf, g)
                for part in weigh(g, c):
                    block = block + dot_tn(take(part), values)
            yacc[:tokens, here] = block

    drain(ret_in, True, far_from, far_to)
    gather(far_slots, lambda part: part[far])
    own_ret.wait()
    drain(ret_in, True, 1, far_from)
    drain(ret_in, True, far_to, experts)
    gather(
        near_slots,
        lambda part: jnp.concatenate([part[: far.start], part[far.stop :]], axis=0),
    )
    moe_ref[...] = yacc[:tokens, :].astype(BF16)

    drain(outward, False)
    drain(ret_out, False)
    others(lambda h: pay_out(h).wait_send())

    def homegoing(d, carry):
        homeward(peer(d)).wait_send()
        return carry

    @pl.when(folds)
    def _():
        lax.fori_loop(1, experts, homegoing, 0)

    for item in weight_rings + (normed_ring, scatter_a, scatter_b):
        item.finish()


def emit(a_in, b_in, a_out, b_out, buf, in_sem, out_sem):
    half = a_in.shape[0] // 2
    moves = []
    for i, (src, dst) in enumerate([(a_in, a_out), (b_in, b_out)]):
        for j in range(2):
            n = 2 * i + j
            at = pl.ds(j * half, half)
            moves.append(
                (
                    pltpu.make_async_copy(src.at[at], buf.at[n], in_sem.at[n]),
                    pltpu.make_async_copy(buf.at[n], dst.at[at], out_sem.at[n]),
                )
            )
    for load, _ in moves:
        load.start()
    for load, store in moves:
        load.wait()
        store.start()
    for _, store in moves:
        store.wait()


def on_device(
    query_vectors,
    attend_lookup_vectors,
    attend_content_vectors,
    forget_speed_dependent,
    amend_speed_dependent,
    result_switch_preactivation,
    feature_forget_baseline,
    amend_speed_baseline,
    sudden_forget_extra,
    group_scaling_factor,
    result_mapping_matrix,
    specialist_tokens_activations,
    specialist_scaling_factor,
    selected_specialists,
    selection_mixing_factors,
    dispatched_switch_matrix,
    dispatched_raising_matrix,
    dispatched_lowering_matrix,
    common_switch_matrix,
    common_raising_matrix,
    common_lowering_matrix,
):
    tokens, top_count = selected_specialists.shape
    width = specialist_tokens_activations.shape[1]
    rows, mix_width = query_vectors.shape
    groups = sudden_forget_extra.shape[1]
    lanes = 2 * (mix_width // groups)
    experts = lax.axis_size("ep")
    tps = lax.axis_size("tp")
    capacity = 3 * tokens * top_count // (2 * experts)
    hid = dispatched_switch_matrix.shape[2]
    shared = common_switch_matrix.shape[1]
    slab = (experts, 16, capacity * width // 16)
    vmem = pl.BlockSpec(memory_space=pltpu.VMEM)
    hbm = pl.BlockSpec(memory_space=pltpu.HBM)
    V = pltpu.VMEM
    dma = pltpu.SemaphoreType.DMA
    mixer_rows = rows // tps
    attend, moe = pl.pallas_call(
        functools.partial(everything, capacity),
        in_specs=[hbm] * 21,
        out_specs=(vmem, vmem),
        out_shape=(
            jax.ShapeDtypeStruct((mixer_rows, width), BF16),
            jax.ShapeDtypeStruct((tokens, width), BF16),
        ),
        scratch_shapes=[V((rows, mix_width), BF16)] * 6
        + [
            V((mix_width, width), BF16),
            V((tps, width, hid), BF16),
            V((tps, width, hid), BF16),
            V((tps * hid, width), BF16),
            V((width, 2 * shared), BF16),
            V((shared, width), BF16),
            V((rows, mix_width), BF16),
            V((rows, mix_width), F32),
            V((groups, lanes // 2, lanes), BF16),
            V((experts, lanes // 2, lanes), BF16),
            V((experts, lanes // 4, lanes), BF16),
            V((groups, lanes // 4, lanes), BF16),
            V((rows, mix_width), BF16),
        ]
        + [V(slab, BF16)] * 4
        + [
            V((experts * capacity, width), BF16),
            V((experts * capacity, width), F32),
            V((experts * capacity, 3 * hid), BF16),
            V((tokens, width), BF16),
            V((tps, tokens, width), BF16),
            V((tps, mixer_rows, width), BF16),
            V((tps, tokens, width), BF16),
            V((2, mixer_rows // 2, width), BF16),
            V((2, tokens // 2, width), BF16),
            V((tps, mixer_rows, width), BF16),
            V((tps, tokens, width), BF16),
            V((tokens, width), BF16),
            V((1, width), F32),
            V((top_count, tokens), jnp.int32),
            V((1, mix_width), F32),
            V((1, mix_width), F32),
            V((groups, rows), F32),
            V((1, mix_width), F32),
            V((top_count, tokens), F32),
            dma((21,)),
            dma((5,)),
        ]
        + [dma((experts,))] * 8
        + [dma((30,)), dma((30,)), dma((12,)), dma((12,))],
        compiler_params=pltpu.CompilerParams(
            collective_id=0, has_side_effects=True, vmem_limit_bytes=60 * 1024 * 1024
        ),
        name="everything",
    )(
        query_vectors,
        attend_lookup_vectors,
        attend_content_vectors,
        forget_speed_dependent,
        amend_speed_dependent,
        result_switch_preactivation,
        feature_forget_baseline.reshape(1, -1),
        amend_speed_baseline.reshape(1, -1),
        sudden_forget_extra.T,
        group_scaling_factor.reshape(1, -1),
        result_mapping_matrix,
        specialist_tokens_activations,
        specialist_scaling_factor.reshape(1, -1),
        selected_specialists.T,
        selection_mixing_factors.T,
        dispatched_switch_matrix[0],
        dispatched_raising_matrix[0],
        dispatched_lowering_matrix[0],
        common_switch_matrix,
        common_raising_matrix,
        common_lowering_matrix,
    )
    return pl.pallas_call(
        emit,
        in_specs=[hbm, hbm],
        out_specs=(hbm, hbm),
        out_shape=(
            jax.ShapeDtypeStruct(attend.shape, BF16),
            jax.ShapeDtypeStruct(moe.shape, BF16),
        ),
        scratch_shapes=[V((4, tokens // 2, width), BF16), dma((4,)), dma((4,))],
        compiler_params=pltpu.CompilerParams(vmem_limit_bytes=60 * 1024 * 1024),
        name="emit",
    )(attend, moe)


def solution(mesh):
    rows = P(("grp", "ep"), "tp")
    tokens = P(("grp", "ep", "tp"), None)
    placed = (
        (rows,) * 6
        + (P("tp"), P("tp"), rows, P("tp"), P("tp", None), tokens, P(), tokens, tokens)
        + (P("ep", None, "tp"), P("ep", None, "tp"), P("ep", "tp", None))
        + (P(None, "tp"), P(None, "tp"), P("tp", None))
    )
    return jax.shard_map(
        on_device, mesh=mesh, in_specs=placed, out_specs=(tokens, tokens), check_vma=False
    )
```

```python
import functools

import jax
import jax.numpy as jnp
from jax import lax
from jax.experimental import pallas as pl
from jax.experimental.pallas import tpu as pltpu
from jax.sharding import PartitionSpec as P

F32 = jnp.float32
BF16 = jnp.bfloat16
SPAN = 64
MESH = pl.DeviceIdType.MESH


def dot(a, b):
    return jnp.dot(a, b, preferred_element_type=F32)


def dot_nt(a, b):
    return lax.dot_general(a, b, (((1,), (1,)), ((), ())), preferred_element_type=F32)


def dot_tn(a, b):
    return lax.dot_general(a, b, (((0,), (0,)), ((), ())), preferred_element_type=F32)


def split(x, parts):
    out = []
    for _ in range(parts - 1):
        out.append(x.astype(BF16))
        x = x - out[-1].astype(F32)
    out.append(x.astype(BF16))
    return out


def iota(shape, dim):
    return lax.broadcasted_iota(jnp.int32, shape, dim)


def local_mixer(
    pair, q_ref, k_ref, v_ref, f_ref, a_ref, fb_ref, ab_ref, x_ref, omap_ref, oloc_ref, pay_ref
):
    rows = q_ref.shape[0]
    groups = x_ref.shape[0]
    half = q_ref.shape[1] // groups
    lanes = 2 * half
    spans = rows // SPAN
    here = pl.ds(pl.multiple_of(pair * lanes, lanes), lanes)
    low = iota((SPAN, lanes), 1) < half
    col = jnp.where(low, iota((SPAN, lanes), 1), iota((SPAN, lanes), 1) - half)
    row = iota((SPAN, lanes), 0)
    strict = row > col
    inclusive = row >= col
    tri = (iota((SPAN, SPAN), 0) >= iota((SPAN, SPAN), 1)).astype(BF16)
    tri3 = jnp.concatenate([tri] * 3, axis=1)
    same = ((iota((lanes, lanes), 0) < half) == (iota((lanes, lanes), 1) < half)).astype(BF16)
    same2 = jnp.concatenate([same] * 2, axis=0)
    spread = (
        iota((groups, lanes), 0) == 2 * pair + (iota((groups, lanes), 1) >= half).astype(jnp.int32)
    ).astype(F32)
    spread3 = jnp.concatenate([spread] * 3, axis=0).astype(BF16)
    below = iota((lanes, lanes), 0) < half
    left = iota((lanes, lanes), 1) < half

    def stack(x):
        return jnp.concatenate([jnp.where(low, x, 0.0), jnp.where(low, 0.0, x)], axis=0).astype(
            BF16
        )

    fb = fb_ref[:, here]
    ab = ab_ref[:, here]
    parts = [part.astype(F32) for part in split(x_ref[...], 3)]
    extra = dot_tn(jnp.concatenate(parts, axis=0).astype(BF16), spread3)

    spans_in = []
    for c in range(spans):
        at = slice(c * SPAN, (c + 1) * SPAN)
        decay = -jnp.exp(fb + f_ref[at, here].astype(F32)) + extra[at, :]
        rate = jax.nn.sigmoid(ab + a_ref[at, here].astype(F32))
        key = k_ref[at, here].astype(F32)
        sq = dot(jnp.concatenate(split(key * key, 2), axis=1), same2)
        unit = key * lax.rsqrt(sq + 1e-06)
        cum = dot(tri3, jnp.concatenate(split(decay, 3), axis=0))
        mid = cum[SPAN // 2 : SPAN // 2 + 1, :]
        last = cum[SPAN - 1 : SPAN, :]
        left_erase = -unit * jnp.exp(cum - decay - mid)
        left_read = q_ref[at, here].astype(F32) * jnp.exp(cum - mid)
        right = jnp.exp(mid - cum) * rate
        right_erase = unit * right
        right_write = key * right
        grow = jnp.exp(mid)
        tail = jnp.exp(last - mid)
        lefts = jnp.concatenate([left_erase, left_read], axis=0).astype(BF16)
        rights = jnp.concatenate([stack(right_erase), stack(right_write)], axis=0)
        pairs = dot_nt(lefts, rights)
        a_mat = jnp.where(strict, pairs[:SPAN, :lanes], 0.0)
        erase_write = jnp.where(strict, pairs[:SPAN, lanes:], 0.0)
        read_erase = jnp.where(inclusive, pairs[SPAN:, :lanes], 0.0)
        read_write = jnp.where(inclusive, pairs[SPAN:, lanes:], 0.0)
        value = v_ref[at, here].astype(F32)
        writes = dot(
            jnp.concatenate([erase_write, read_write], axis=0).astype(BF16), stack(value)
        )
        ends = jnp.concatenate([right_erase * tail, right_write * tail], axis=0).astype(BF16)
        spans_in.append(
            dict(
                a=a_mat,
                first=stack(left_erase * grow),
                read=left_read * grow,
                re=read_erase.astype(BF16),
                ew=stack(writes[:SPAN]),
                rw=writes[SPAN:],
                ends=ends,
                value=v_ref[at, here],
                last=jnp.exp(last),
            )
        )

    eye = (row == col).astype(F32)
    block = 1
    inverse = None
    while block < SPAN:
        in_block = (row // (2 * block) == col // (2 * block)) & (
            (row // block) % 2 == 1
        ) & ((col // block) % 2 == 0)
        steps = [jnp.where(in_block, s["a"], 0.0) for s in spans_in]
        if inverse is None:
            inverse = [eye + step for step in steps]
        else:
            inner = [
                dot(step.astype(BF16), stack(x)) for step, x in zip(steps, inverse)
            ]
            inverse = [x + dot(x.astype(BF16), stack(y)) for x, y in zip(inverse, inner)]
        block *= 2

    state = jnp.concatenate([eye, jnp.zeros_like(eye)], axis=0)
    for c, s in enumerate(spans_in):
        at = slice(c * SPAN, (c + 1) * SPAN)
        solved = dot(inverse[c].astype(BF16), jnp.concatenate([s["first"], s["ew"]], axis=1))
        w, y = (solved[:, :lanes], solved[:, lanes:])
        seen = dot(s["re"], jnp.concatenate([stack(w), stack(y)], axis=1))
        read = s["read"] + seen[:, :lanes]
        added = s["rw"] + seen[:, lanes:]
        value = s["value"]
        erased = dot_tn(w.astype(BF16), s["ends"][:SPAN])
        erased = jnp.where(below == left, erased, 0.0).astype(BF16)
        offset = dot_tn(jnp.concatenate([y.astype(BF16), value], axis=0), s["ends"])
        offset = jnp.where(low, offset[:half], offset[half:])
        both = jnp.concatenate([stack(state[:SPAN]), stack(state[SPAN:])], axis=0)
        reads = dot_nt(read.astype(BF16), both)
        omap_ref[at, here] = reads[:, :lanes].astype(BF16)
        oloc_ref[at, here] = added + reads[:, lanes:]
        state = (
            state * s["last"]
            + dot(state.astype(BF16), erased)
            + jnp.concatenate([jnp.zeros_like(offset), offset], axis=0)
        )
    jump, offset = (state[:SPAN], state[SPAN:])
    jump_turned = pltpu.roll(jump, half, 1)
    offset_turned = pltpu.roll(offset, half, 1)
    near = low[: SPAN // 2]
    for h in range(2):
        packed = [
            jnp.where(near, (x, turned)[h][: SPAN // 2], (turned, x)[h][SPAN // 2 :])
            for x, turned in ((jump, jump_turned), (offset, offset_turned))
        ]
        pay_ref[2 * pair + h] = jnp.concatenate(packed, axis=0).astype(BF16)


def fold_step(state, arrived):
    lanes = state.shape[1]
    half = lanes // 2
    low = iota(state.shape, 1) < half
    block = arrived.astype(F32)
    rows = state.shape[0]
    jump, offset = (block[:rows], block[rows:])
    turned = pltpu.roll(jump, half, 1)
    spread = jnp.concatenate(
        [
            jnp.where(low, jump, 0.0),
            jnp.where(low, turned, 0.0),
            jnp.where(low, 0.0, turned),
            jnp.where(low, 0.0, jump),
        ],
        axis=0,
    ).astype(BF16)
    parts = [part.astype(F32) for part in split(state, 2)]
    moved = dot(jnp.concatenate(parts, axis=0).astype(BF16), spread)
    return moved[:rows] + moved[rows:] + offset


def finish_mixer(pair, omap_ref, oloc_ref, state_ref, gate_ref, gain_ref, out_ref):
    lanes = state_ref.shape[2]
    half = lanes // 2
    here = pl.ds(pl.multiple_of(pair * lanes, lanes), lanes)
    low = iota(state_ref.shape[1:], 1) < half
    tiles = []
    for h in range(2):
        block = state_ref[2 * pair + h].astype(F32)
        turned = pltpu.roll(block, half, 1)
        if h == 0:
            tiles += [jnp.where(low, block, 0.0), jnp.where(low, turned, 0.0)]
        else:
            tiles += [jnp.where(low, 0.0, turned), jnp.where(low, 0.0, block)]
    state = jnp.concatenate(tiles, axis=0).astype(BF16)
    same = jnp.where(
        (iota((lanes, lanes), 0) < half) == (iota((lanes, lanes), 1) < half), 1.0 / half, 0.0
    ).astype(BF16)
    same2 = jnp.concatenate([same] * 2, axis=0)
    head_out = oloc_ref[:, here] + dot_nt(omap_ref[:, here], state)
    mean = dot(jnp.concatenate(split(head_out, 2), axis=1), same2)
    centered = head_out - mean
    var = dot(jnp.concatenate(split(centered * centered, 2), axis=1), same2)
    normed = centered * lax.rsqrt(var + 0.00064) * gain_ref[:, here]
    out_ref[:, here] = (normed * jax.nn.sigmoid(gate_ref[:, here].astype(F32))).astype(BF16)


def slot_hits(ids, experts, capacity):
    tokens = ids.shape[1]
    ids = ids.astype(F32)
    expert = iota((experts, tokens), 0).astype(F32)
    hot = [(expert == ids[j : j + 1]).astype(F32) for j in range(2)]
    earlier = (iota((tokens, tokens), 0) < iota((tokens, tokens), 1)).astype(F32).astype(BF16)
    before = dot((hot[0] + hot[1]).astype(BF16), earlier)
    place = [
        ids[j : j + 1] * capacity + jnp.sum(hot[j] * before, axis=0, keepdims=True)
        for j in range(2)
    ]
    at = iota((16 * experts, tokens), 0)
    base = (capacity * (at // 16) + at % 4).astype(F32)
    quarter = (at // 4) % 4
    groups = [[base + 4 * g == place[j] for j in range(2)] for g in range(capacity // 4)]
    return groups, quarter


def everything(
    capacity,
    q_in,
    k_in,
    v_in,
    f_in,
    a_in,
    g_in,
    fb_in,
    ab_in,
    x_in,
    gain_in,
    wout_in,
    tok_in,
    scale_in,
    ids_in,
    mix_in,
    gate_in,
    up_in,
    down_in,
    cgate_in,
    cup_in,
    cdown_in,
    attend_ref,
    moe_ref,
    q_ref,
    k_ref,
    v_ref,
    f_ref,
    a_ref,
    g_ref,
    wout_ref,
    wg_ref,
    wu_ref,
    wd_ref,
    cgu_ref,
    cd_ref,
    omap_ref,
    oloc_ref,
    pay_ref,
    arrived,
    sent,
    states,
    mixed_ref,
    out_buf,
    in_buf,
    ret_buf,
    back_buf,
    xbuf,
    yacc,
    hbuf,
    normed_own,
    ngather,
    part_a,
    part_b,
    relay_a,
    relay_b,
    sums_a,
    sums_b,
    tok_ref,
    scale_ref,
    ids_ref,
    fb_ref,
    ab_ref,
    x_ref,
    gain_ref,
    mix_ref,
    load_sem,
    own_sem,
    out_send,
    out_recv,
    pay_send,
    pay_recv,
    home_send,
    home_recv,
    ret_send,
    ret_recv,
    ring_send,
    ring_recv,
    rs_send,
    rs_recv,
):
    experts = out_buf.shape[0]
    tps = ngather.shape[0]
    tokens, width = tok_ref.shape
    quarter_width = width // 4
    groups = capacity // 4
    pairs = omap_ref.shape[1] // sent.shape[2]
    ep = lax.axis_index("ep")
    tp = lax.axis_index("tp")
    right, left, across = (lax.rem(tp + 1, tps), lax.rem(tp + 3, tps), lax.rem(tp + 2, tps))
    paired = lax.axis_size("grp") % 2 == 0
    grp = lax.axis_index("grp")
    side = lax.rem(grp, 2)
    partner = grp + 1 - 2 * side
    heads = pay_ref.shape[0]
    stride = experts // heads
    my_head = ep // stride
    folds = lax.rem(ep, stride) == 0

    barrier = pltpu.get_barrier_semaphore()

    def greet(d, carry):
        pl.semaphore_signal(
            barrier, inc=1, device_id={"ep": lax.rem(ep + d, experts)}, device_id_type=MESH
        )
        return carry

    lax.fori_loop(1, experts, greet, 0)
    for near in (right, left):
        pl.semaphore_signal(barrier, inc=1, device_id={"tp": near}, device_id_type=MESH)
    if paired:
        pl.semaphore_signal(barrier, inc=1, device_id={"grp": partner}, device_id_type=MESH)

    half_lanes = cgate_in.shape[1]
    hid = gate_in.shape[1]
    loads = [
        pltpu.make_async_copy(a, b, load_sem.at[i])
        for i, (a, b) in enumerate(
            [
                (q_in, q_ref),
                (k_in, k_ref),
                (v_in, v_ref),
                (f_in, f_ref),
                (a_in, a_ref),
                (g_in, g_ref),
                (wout_in, wout_ref),
                (gate_in, wg_ref.at[0]),
                (up_in, wu_ref.at[0]),
                (down_in, wd_ref.at[pl.ds(0, hid)]),
                (cgate_in, cgu_ref.at[:, pl.ds(0, half_lanes)]),
                (cup_in, cgu_ref.at[:, pl.ds(half_lanes, half_lanes)]),
                (cdown_in, cd_ref),
                (tok_in, tok_ref),
                (scale_in, scale_ref),
                (ids_in, ids_ref),
                (fb_in, fb_ref),
                (ab_in, ab_ref),
                (x_in, x_ref),
                (gain_in, gain_ref),
                (mix_in, mix_ref),
            ]
        )
    ]
    for load in loads[13:] + loads[:13]:
        load.start()

    def remote(src, dst, send, recv, axis, to):
        return pltpu.make_async_remote_copy(
            src_ref=src,
            dst_ref=dst,
            send_sem=send,
            recv_sem=recv,
            device_id={axis: to},
            device_id_type=MESH,
        )

    for load in loads[13:16]:
        load.wait()
    floats = tok_ref[...].astype(F32)
    normed = (
        floats
        * lax.rsqrt(jnp.mean(floats * floats, -1, keepdims=True) + 1e-06)
        * scale_ref[...]
    ).astype(BF16)
    normed_own[...] = normed
    from_here = ids_ref[...] - ep
    from_here = jnp.where(from_here < 0, from_here + experts, from_here)
    hits, quarter = slot_hits(from_here, experts, capacity)
    stacked = jnp.concatenate(
        [normed[:, c * quarter_width : (c + 1) * quarter_width] for c in range(4)], axis=0
    )
    for g in range(groups):
        either = hits[g][0] | hits[g][1]
        placing = jnp.concatenate(
            [(either & (quarter == c)).astype(F32).astype(BF16) for c in range(4)], axis=1
        )
        out_buf[:, :, g * quarter_width : (g + 1) * quarter_width] = (
            dot(placing, stacked).astype(BF16).reshape(experts, 16, quarter_width)
        )

    pl.semaphore_wait(barrier, experts - 1 + 2 + int(paired))

    def peer(d):
        return lax.rem(ep + d, experts)

    def outward(d):
        there = experts - d
        return remote(
            out_buf.at[d], in_buf.at[there], out_send.at[d], out_recv.at[there], "ep", peer(d)
        )

    def inward(d):
        return remote(out_buf.at[d], in_buf.at[d], out_send.at[d], out_recv.at[d], "ep", peer(d))

    def spray(make, first, last):
        def go(i, carry):
            d = experts // 2 - i
            make(d).start()
            make(experts - d).start()
            return carry

        if first == 0:
            make(experts // 2).start()
        lax.fori_loop(max(first, 1), last, go, 0)

    far_from, far_to = (experts // 4, 3 * experts // 4)

    def drain(make, recv, first=1, last=experts):
        def go(d, carry):
            if recv:
                make(d).wait_recv()
            else:
                make(d).wait_send()
            return carry

        lax.fori_loop(first, last, go, 0)

    def far_slots(ref, g):
        return ref[far_from:far_to, :, g * quarter_width : (g + 1) * quarter_width].reshape(
            8 * experts, quarter_width
        )

    def near_slots(ref, g):
        here = slice(g * quarter_width, (g + 1) * quarter_width)
        return jnp.concatenate([ref[:far_from, :, here], ref[far_to:, :, here]], axis=0).reshape(
            8 * experts, quarter_width
        )

    early = 3 * experts // 16
    spray(outward, 0, early)

    class Ring:
        def __init__(self, index, own, slot, pair_left, pair_right):
            n = own.shape[0]
            mine = pl.ds(pl.multiple_of(side * (n // 2), n // 2), n // 2)
            other = pl.ds(pl.multiple_of((1 - side) * (n // 2), n // 2), n // 2)
            whole = pl.ds(0, n)
            s = [ring_send.at[6 * index + i] for i in range(6)]
            r = [ring_recv.at[6 * index + i] for i in range(6)]
            self.near, self.far, self.pair, self.paired_in = ([], [], [], [])
            for i, (to, half, rest, pair) in enumerate(
                [
                    (right, mine, other, paired and pair_left),
                    (left, other, mine, paired and pair_right),
                ]
            ):
                part = half if pair else whole
                self.near.append(
                    remote(own.at[part], slot(i + 1, part), s[i], r[i], "tp", to)
                )
                self.far.append(
                    remote(slot(i + 1, half), slot(3, half), s[2 + i], r[2 + i], "tp", to)
                )
                self.pair.append(
                    pair
                    and (
                        remote(
                            slot(i + 1, half), slot(i + 1, half), s[4 + i], r[4 + i], "grp", partner
                        ),
                        remote(
                            slot(i + 1, rest), slot(i + 1, rest), s[4 + i], r[4 + i], "grp", partner
                        ),
                    )
                )

        def start(self):
            for copy in self.near:
                copy.start()

        def forward(self):
            for copy, onward, pair in zip(self.near, self.far, self.pair):
                copy.wait_recv()
                onward.start()
                if pair:
                    pair[0].start()

        def beside(self):
            for pair in self.pair:
                if pair:
                    pair[1].wait_recv()

        def arrive(self):
            for copy in self.far:
                copy.wait_recv()

        def finish(self):
            for copy in self.near + self.far:
                copy.wait_send()
            for pair in self.pair:
                if pair:
                    pair[0].wait_send()

    def down_slot(base):
        def slot(s, rows):
            return wd_ref.at[pl.ds(pl.multiple_of(s * hid + base + rows.start, hid // 4), rows.size)]

        return slot

    gate_ring = Ring(0, gate_in, lambda s, rows: wg_ref.at[s, rows], True, True)
    up_ring = Ring(1, up_in, lambda s, rows: wu_ref.at[s, rows], True, True)
    down_rings = [
        Ring(2, down_in.at[pl.ds(0, hid // 2)], down_slot(0), True, False),
        Ring(3, down_in.at[pl.ds(hid // 2, hid // 2)], down_slot(hid // 2), False, True),
    ]
    normed_ring = Ring(4, normed_own, lambda s, rows: ngather.at[s, rows], False, False)
    weight_rings = (gate_ring, up_ring, *down_rings)
    for ring in weight_rings:
        ring.start()

    own_out = pltpu.make_async_copy(out_buf.at[0], in_buf.at[0], own_sem.at[0])
    own_out.start()
    own_normed = pltpu.make_async_copy(normed_own, ngather.at[0], own_sem.at[1])
    own_normed.start()

    for load in loads[:5] + loads[16:19]:
        load.wait()

    def mix(pair, carry):
        @pl.when(pair == pairs // 4)
        def _():
            gate_ring.forward()

        local_mixer(
            pair,
            q_ref,
            k_ref,
            v_ref,
            f_ref,
            a_ref,
            fb_ref,
            ab_ref,
            x_ref,
            omap_ref,
            oloc_ref,
            pay_ref,
        )
        return carry

    lax.fori_loop(0, pairs, mix, 0)

    def pay_out(h):
        return remote(
            pay_ref.at[h], arrived.at[ep], pay_send.at[h], pay_recv.at[ep], "ep", stride * h
        )

    def pay_in(e):
        return remote(pay_ref.at[0], arrived.at[e], pay_send.at[0], pay_recv.at[e], "ep", e)

    def others(act):
        for h in range(heads):
            pl.when(ep != stride * h)(functools.partial(act, h))

    others(lambda h: pay_out(h).start())
    own_pay = pltpu.make_async_copy(pay_ref.at[my_head], arrived.at[ep], own_sem.at[2])

    @pl.when(folds)
    def _():
        own_pay.start()

    spray(outward, early, experts // 2)
    for ring in weight_rings[1:]:
        ring.forward()
    normed_ring.start()

    def homeward(e):
        return remote(
            sent.at[e], states.at[my_head], home_send.at[e], home_recv.at[my_head], "ep", e
        )

    def home(h):
        return remote(sent.at[0], states.at[h], home_send.at[0], home_recv.at[h], "ep", stride * h)

    own_state = pltpu.make_async_copy(sent.at[ep], states.at[my_head], own_sem.at[3])

    def step(e, state):
        sent[e] = state.astype(BF16)

        @pl.when(e != ep)
        def _():
            pay_in(e).wait_recv()

        @pl.when((e > 0) & (e - 1 != ep))
        def _():
            homeward(e - 1).start()

        return fold_step(state, arrived[e])

    @pl.when(folds)
    def _():
        own_pay.wait()
        lax.fori_loop(0, experts, step, jnp.zeros(sent.shape[1:], F32))

        @pl.when(ep != experts - 1)
        def _():
            homeward(experts - 1).start()

        own_state.start()
        own_state.wait()

    half_rows = 2 * experts
    many = groups * half_rows
    at_row = iota((half_rows, 8 * experts), 0)
    at_col = iota((half_rows, 8 * experts), 1)
    picks = [
        (at_col == 16 * (at_row // 4) + 4 * c + at_row % 4).astype(F32).astype(BF16)
        for c in range(4)
    ]

    def unpack(slots, base):
        for g in range(groups):
            block = slots(in_buf, g)
            for c in range(4):
                xbuf[
                    base + g * half_rows : base + (g + 1) * half_rows,
                    c * quarter_width : (c + 1) * quarter_width,
                ] = dot(picks[c], block).astype(BF16)

    def hidden(base, s):
        rows = xbuf[base : base + many, :]
        return (jax.nn.silu(dot(rows, wg_ref[s])) * dot(rows, wu_ref[s])).astype(BF16)

    def lift(base):
        for s in range(3):
            hbuf[base : base + many, s * hid : (s + 1) * hid] = hidden(base, s)

    def lower(base):
        yacc[base : base + many, :] = dot(hbuf[base : base + many, :], wd_ref[: 3 * hid])

    at_row = iota((8 * experts, half_rows), 0)
    at_col = iota((8 * experts, half_rows), 1)
    put = jnp.concatenate(
        [
            (at_row == 16 * (at_col // 4) + 4 * c + at_col % 4).astype(F32).astype(BF16)
            for c in range(4)
        ],
        axis=1,
    )

    def complete(base, store):
        total = yacc[base : base + many, :] + dot(hidden(base, 3), wd_ref[3 * hid :])
        for g in range(groups):
            rows = total[g * half_rows : (g + 1) * half_rows].astype(BF16)
            rows = jnp.concatenate(
                [rows[:, c * quarter_width : (c + 1) * quarter_width] for c in range(4)], axis=0
            )
            block = dot(put, rows).astype(BF16).reshape(experts // 2, 16, quarter_width)
            store(slice(g * quarter_width, (g + 1) * quarter_width), block)

    def store_far(here, block):
        ret_buf[far_from:far_to, :, here] = block

    def store_near(here, block):
        ret_buf[:far_from, :, here] = block[:far_from]
        ret_buf[far_to:, :, here] = block[far_from:]

    def ret_out(d):
        there = experts - d
        return remote(
            ret_buf.at[d], back_buf.at[there], ret_send.at[d], ret_recv.at[there], "ep", peer(d)
        )

    def ret_in(d):
        return remote(ret_buf.at[d], back_buf.at[d], ret_send.at[d], ret_recv.at[d], "ep", peer(d))

    drain(inward, True, far_from, far_to)
    unpack(far_slots, 0)
    for load in loads[7:10]:
        load.wait()
    gate_ring.beside()
    up_ring.beside()
    lift(0)
    for ring in down_rings:
        ring.beside()
    lower(0)
    for ring in weight_rings:
        ring.arrive()
    complete(0, store_far)
    spray(ret_out, 0, experts // 4)
    own_out.wait()
    drain(inward, True, 1, far_from)
    drain(inward, True, far_to, experts)
    unpack(near_slots, many)
    lift(many)
    lower(many)
    complete(many, store_near)
    spray(ret_out, experts // 4, experts // 2)
    own_ret = pltpu.make_async_copy(ret_buf.at[0], back_buf.at[0], own_sem.at[4])
    own_ret.start()

    class Scatter:
        def __init__(self, index, part, relay, sums):
            n = part.shape[1]
            top, bottom = (pl.ds(0, n // 2), pl.ds(n // 2, n // 2))
            s = [rs_send.at[6 * index + i] for i in range(6)]
            r = [rs_recv.at[6 * index + i] for i in range(6)]
            self.part, self.sums = (part, sums)
            self.near = [
                remote(part.at[3, top], relay.at[0], s[0], r[0], "tp", right),
                remote(part.at[3, bottom], relay.at[1], s[1], r[1], "tp", left),
                remote(part.at[2], sums.at[1], s[2], r[2], "tp", right),
                remote(part.at[1], sums.at[2], s[3], r[3], "tp", left),
            ]
            self.far = [
                remote(relay.at[0], sums.at[3, top], s[4], r[4], "tp", right),
                remote(relay.at[1], sums.at[3, bottom], s[5], r[5], "tp", left),
            ]

        def start(self):
            for copy in self.near:
                copy.start()

        def forward(self):
            for copy, onward in zip(self.near[:2], self.far):
                copy.wait_recv()
                onward.start()

        def total(self):
            for copy in self.near[2:] + self.far:
                copy.wait_recv()
            out = self.part[0].astype(F32)
            for s in range(1, 4):
                out = out + self.sums[s].astype(F32)
            return out

        def finish(self):
            for copy in self.near + self.far:
                copy.wait_send()

    scatter_a = Scatter(0, part_a, relay_a, sums_a)
    scatter_b = Scatter(1, part_b, relay_b, sums_b)

    others(lambda h: home(h).wait_recv())
    for load in loads[5:7] + loads[19:20]:
        load.wait()

    def finish(pair, carry):
        finish_mixer(pair, omap_ref, oloc_ref, states, g_ref, gain_ref, mixed_ref)
        return carry

    lax.fori_loop(0, pairs, finish, 0)
    mixer_rows = part_a.shape[1]
    for s, owner in enumerate((tp, left, right, across)):
        mine = pl.ds(pl.multiple_of(owner * mixer_rows, mixer_rows), mixer_rows)
        part_a[s] = dot(mixed_ref[mine, :], wout_ref[...]).astype(BF16)
    normed_ring.forward()
    scatter_a.start()

    own_normed.wait()
    for load in loads[10:13]:
        load.wait()
    normed_ring.arrive()
    scatter_a.forward()
    both = dot(ngather[...].reshape(tps * tokens, width), cgu_ref[...])
    inner = (jax.nn.silu(both[:, :half_lanes]) * both[:, half_lanes:]).astype(BF16)
    for s in range(4):
        part_b[s] = dot(inner[s * tokens : (s + 1) * tokens], cd_ref[...]).astype(BF16)
    scatter_b.start()
    scatter_b.forward()
    attend_ref[...] = scatter_a.total().astype(BF16)
    yacc[:tokens, :] = scatter_b.total()

    from_here = ids_ref[...] - ep
    from_here = jnp.where(from_here < 0, from_here + experts, from_here)
    hits, quarter = slot_hits(from_here, experts, capacity)
    for load in loads[20:]:
        load.wait()

    def weigh(g, c):
        weight = jnp.where(hits[g][0], mix_ref[0:1, :], 0.0) + jnp.where(
            hits[g][1], mix_ref[1:2, :], 0.0
        )
        return split(jnp.where(quarter == c, weight, 0.0), 2)

    far = slice(16 * far_from, 16 * far_to)

    def gather(slots, take):
        for c in range(4):
            here = slice(c * quarter_width, (c + 1) * quarter_width)
            block = yacc[:tokens, here]
            for g in range(groups):
                values = slots(back_buf, g)
                for part in weigh(g, c):
                    block = block + dot_tn(take(part), values)
            yacc[:tokens, here] = block

    drain(ret_in, True, far_from, far_to)
    gather(far_slots, lambda part: part[far])
    own_ret.wait()
    drain(ret_in, True, 1, far_from)
    drain(ret_in, True, far_to, experts)
    gather(
        near_slots,
        lambda part: jnp.concatenate([part[: far.start], part[far.stop :]], axis=0),
    )
    moe_ref[...] = yacc[:tokens, :].astype(BF16)

    drain(outward, False)
    drain(ret_out, False)
    others(lambda h: pay_out(h).wait_send())

    def homegoing(d, carry):
        homeward(peer(d)).wait_send()
        return carry

    @pl.when(folds)
    def _():
        lax.fori_loop(1, experts, homegoing, 0)

    for item in weight_rings + (normed_ring, scatter_a, scatter_b):
        item.finish()


def emit(a_in, b_in, a_out, b_out, buf, in_sem, out_sem):
    half = a_in.shape[0] // 2
    moves = []
    for i, (src, dst) in enumerate([(a_in, a_out), (b_in, b_out)]):
        for j in range(2):
            n = 2 * i + j
            at = pl.ds(j * half, half)
            moves.append(
                (
                    pltpu.make_async_copy(src.at[at], buf.at[n], in_sem.at[n]),
                    pltpu.make_async_copy(buf.at[n], dst.at[at], out_sem.at[n]),
                )
            )
    for load, _ in moves:
        load.start()
    for load, store in moves:
        load.wait()
        store.start()
    for _, store in moves:
        store.wait()


def on_device(
    query_vectors,
    attend_lookup_vectors,
    attend_content_vectors,
    forget_speed_dependent,
    amend_speed_dependent,
    result_switch_preactivation,
    feature_forget_baseline,
    amend_speed_baseline,
    sudden_forget_extra,
    group_scaling_factor,
    result_mapping_matrix,
    specialist_tokens_activations,
    specialist_scaling_factor,
    selected_specialists,
    selection_mixing_factors,
    dispatched_switch_matrix,
    dispatched_raising_matrix,
    dispatched_lowering_matrix,
    common_switch_matrix,
    common_raising_matrix,
    common_lowering_matrix,
):
    tokens, top_count = selected_specialists.shape
    width = specialist_tokens_activations.shape[1]
    rows, mix_width = query_vectors.shape
    groups = sudden_forget_extra.shape[1]
    lanes = 2 * (mix_width // groups)
    experts = lax.axis_size("ep")
    tps = lax.axis_size("tp")
    capacity = 3 * tokens * top_count // (2 * experts)
    hid = dispatched_switch_matrix.shape[2]
    shared = common_switch_matrix.shape[1]
    slab = (experts, 16, capacity * width // 16)
    vmem = pl.BlockSpec(memory_space=pltpu.VMEM)
    hbm = pl.BlockSpec(memory_space=pltpu.HBM)
    V = pltpu.VMEM
    dma = pltpu.SemaphoreType.DMA
    mixer_rows = rows // tps
    attend, moe = pl.pallas_call(
        functools.partial(everything, capacity),
        in_specs=[hbm] * 21,
        out_specs=(vmem, vmem),
        out_shape=(
            jax.ShapeDtypeStruct((mixer_rows, width), BF16),
            jax.ShapeDtypeStruct((tokens, width), BF16),
        ),
        scratch_shapes=[V((rows, mix_width), BF16)] * 6
        + [
            V((mix_width, width), BF16),
            V((tps, width, hid), BF16),
            V((tps, width, hid), BF16),
            V((tps * hid, width), BF16),
            V((width, 2 * shared), BF16),
            V((shared, width), BF16),
            V((rows, mix_width), BF16),
            V((rows, mix_width), F32),
            V((groups, lanes // 2, lanes), BF16),
            V((experts, lanes // 2, lanes), BF16),
            V((experts, lanes // 4, lanes), BF16),
            V((groups, lanes // 4, lanes), BF16),
            V((rows, mix_width), BF16),
        ]
        + [V(slab, BF16)] * 4
        + [
            V((experts * capacity, width), BF16),
            V((experts * capacity, width), F32),
            V((experts * capacity, 3 * hid), BF16),
            V((tokens, width), BF16),
            V((tps, tokens, width), BF16),
            V((tps, mixer_rows, width), BF16),
            V((tps, tokens, width), BF16),
            V((2, mixer_rows // 2, width), BF16),
            V((2, tokens // 2, width), BF16),
            V((tps, mixer_rows, width), BF16),
            V((tps, tokens, width), BF16),
            V((tokens, width), BF16),
            V((1, width), F32),
            V((top_count, tokens), jnp.int32),
            V((1, mix_width), F32),
            V((1, mix_width), F32),
            V((groups, rows), F32),
            V((1, mix_width), F32),
            V((top_count, tokens), F32),
            dma((21,)),
            dma((5,)),
        ]
        + [dma((experts,))] * 8
        + [dma((30,)), dma((30,)), dma((12,)), dma((12,))],
        compiler_params=pltpu.CompilerParams(
            collective_id=0, has_side_effects=True, vmem_limit_bytes=60 * 1024 * 1024
        ),
        name="everything",
    )(
        query_vectors,
        attend_lookup_vectors,
        attend_content_vectors,
        forget_speed_dependent,
        amend_speed_dependent,
        result_switch_preactivation,
        feature_forget_baseline.reshape(1, -1),
        amend_speed_baseline.reshape(1, -1),
        sudden_forget_extra.T,
        group_scaling_factor.reshape(1, -1),
        result_mapping_matrix,
        specialist_tokens_activations,
        specialist_scaling_factor.reshape(1, -1),
        selected_specialists.T,
        selection_mixing_factors.T,
        dispatched_switch_matrix[0],
        dispatched_raising_matrix[0],
        dispatched_lowering_matrix[0],
        common_switch_matrix,
        common_raising_matrix,
        common_lowering_matrix,
    )
    return pl.pallas_call(
        emit,
        in_specs=[hbm, hbm],
        out_specs=(hbm, hbm),
        out_shape=(
            jax.ShapeDtypeStruct(attend.shape, BF16),
            jax.ShapeDtypeStruct(moe.shape, BF16),
        ),
        scratch_shapes=[V((4, tokens // 2, width), BF16), dma((4,)), dma((4,))],
        compiler_params=pltpu.CompilerParams(vmem_limit_bytes=60 * 1024 * 1024),
        name="emit",
    )(attend, moe)


def solution(mesh):
    rows = P(("grp", "ep"), "tp")
    tokens = P(("grp", "ep", "tp"), None)
    placed = (
        (rows,) * 6
        + (P("tp"), P("tp"), rows, P("tp"), P("tp", None), tokens, P(), tokens, tokens)
        + (P("ep", None, "tp"), P("ep", None, "tp"), P("ep", "tp", None))
        + (P(None, "tp"), P(None, "tp"), P("tp", None))
    )
    return jax.shard_map(
        on_device, mesh=mesh, in_specs=placed, out_specs=(tokens, tokens), check_vma=False
    )
```
